256 devices in a mesh: sp: 64 (over z, x, core), tp: 4 (over y).
Axes of the slice: x: 4, y: 4, z: 8, core: 2. Of those that a mesh axis runs over, the one named last changes fastest.
Arguments:
- stream: bfloat16 [8192, 2048], P(('sp', 'tp')), may hold values from -2.5 to 2.5
- recurrence_input: bfloat16 [8192, 2, 1024], P('sp', None, 'tp'), may hold values from -6 to 6
- output_gate_input: bfloat16 [8192, 2, 1024], P('sp', None, 'tp'), may hold values from -6 to 6
- convolution_taps: bfloat16 [4, 2, 1024], P(None, None, 'tp'), may hold values from -4 to 4
- first_group_gates: bfloat16 [2, 16, 64, 64], P(None, 'tp'), may hold values from -0.75 to 0.75
- second_group_gates: bfloat16 [2, 8, 128, 128], P(None, 'tp'), may hold values from -0.5 to 0.5
- channel_decay: float32 [2, 1024], P(None, 'tp'), may hold values from 4.7 to 13.6
- position_log_extra: float32 [8192, 2, 1024], P('sp', None, 'tp'), may hold values from -1.4 to 0, as said below
- recurrence_output_weight: bfloat16 [2, 1024, 2048], P(None, 'tp'), may hold values from -0.125 to 0.125
- first_norm_gain: float32 [2048], replicated, may hold values from 0.1 to 1.9
- first_norm_bias: float32 [2048], replicated, may hold values from -1.75 to 1.75
- routed_expert_index: int32 [8192, 4], P('sp'), may hold values from 0 to 63, all different within a row; in each aligned block of 32 rows (0 to 31, 32 to 63, ...) at most 2 rows name the same one
- routed_expert_weight: float32 [8192, 4], P('sp'), may hold values from 0.25 to 1
- routed_gate_weight: bfloat16 [64, 2048, 512], P('sp', None, 'tp'), may hold values from -0.125 to 0.125
- routed_up_weight: bfloat16 [64, 2048, 512], P('sp', None, 'tp'), may hold values from -0.125 to 0.125
- routed_down_weight: bfloat16 [64, 512, 2048], P('sp', 'tp'), may hold values from -0.25 to 0.25
- shared_gate_weight: bfloat16 [2048, 512], replicated, may hold values from -0.125 to 0.125
- shared_up_weight: bfloat16 [2048, 512], replicated, may hold values from -0.125 to 0.125
- shared_down_weight: bfloat16 [512, 2048], replicated, may hold values from -0.25 to 0.25
- second_norm_gain: float32 [2048], replicated, may hold values from 0.1 to 1.9
- second_norm_bias: float32 [2048], replicated, may hold values from -1.75 to 1.75
Outputs:
- result: bfloat16 [8192, 2048], P(('sp', 'tp'))
The draws below stay inside these ranges and needn't reach their ends.
Inputs may be any that keep to these rules, and one draw needn't show every extreme that they name: `routed_expert_index`: each row names 4 different experts. In each aligned block of 32 rows no expert is named more than 2 times, and in some block an expert is named exactly 2 times. `position_log_extra`: every entry is negative.
All inputs are finite; a program needn't handle non-finite values.
Results may differ from the reference program's by a relative error of at most 0.015.
Values may be sent and summed in bfloat16 or wider, within the bound.
No kernel may reach another device: no remote copies, remote signals or barrier semaphores. Data moves between devices by JAX's collectives and lax.ppermute only.
A program may use at most 64 MiB of HBM per device.

```python
import math
import jax
import jax.numpy as jnp
import numpy as np
from jax import lax

D = 2048
D_HALF = 1024
HEAD_SMALL = 64
HEAD_LARGE = 128
HEADS_SMALL = 16
HEADS_LARGE = 8
DQ = 256
CONV = 4
FE = 512
FE_DEV = 128
FS = 512
K = 4
EXPERTS = 64
TOK_DEV = 128
TOK_Q = 32
TOKENS = 8192
CAP_Q = 2
N_TP = 4


def draw_channel_decay(key, part):
    key_flag = jax.random.fold_in(key, 11)
    key_rate = jax.random.fold_in(key, 12)
    fast_limit = 5
    flags = jax.random.randint(key_flag, (2, D_HALF // HEAD_SMALL), 0, 10) < fast_limit
    channel = jnp.arange(D_HALF)
    head_index = jnp.stack([channel // HEAD_SMALL, channel // HEAD_LARGE])
    fast = jnp.take_along_axis(flags, head_index, axis=1)
    spread = jax.random.uniform(key_rate, (2, D_HALF), jnp.float32)
    fast_rate = jnp.exp(jnp.log(0.005) + spread * jnp.log(0.009 / 0.005))
    slow_rate = jnp.exp(jnp.log(1.25e-06) + spread * jnp.log(4.0))
    rate = jnp.where(fast, fast_rate, slow_rate)
    return -jnp.log(jnp.expm1(rate))


def draw_position_log_extra(key, part):
    key_base = jax.random.fold_in(key, 21)
    key_spot = jax.random.fold_in(key, 22)
    key_depth = jax.random.fold_in(key, 23)
    block_count = TOKENS // TOK_DEV
    base = jnp.exp(jax.random.uniform(key_base, (block_count, 1, 2, D_HALF), jnp.float32, jnp.log(5e-06), jnp.log(2e-05)))
    base = jnp.broadcast_to(base, (block_count, TOK_DEV, 2, D_HALF)).reshape(TOKENS, 2, D_HALF)
    spots = jax.random.randint(key_spot, (2,), 0, TOKENS)
    position = jnp.arange(TOKENS)
    hits = jnp.sum((position[:, None] == spots[None, :]).astype(jnp.float32), axis=1)
    depth = jax.random.uniform(key_depth, (2, D_HALF), jnp.float32, 0.22, 0.69)
    return -(base + hits[:, None, None] * depth[None])


def levels(own_key, shape, split, low, top_value):
    level, own = 1.0, jax.random.fold_in(own_key, 6)
    for dim, parts in split:
        heights = jnp.exp(jax.random.uniform(jax.random.fold_in(own, dim), (parts,), jnp.float32, low / len(split), top_value / len(split)))
        level = level * jnp.repeat(heights, shape[dim] // parts).reshape([-1 if axis == dim else 1 for axis in range(len(shape))])
    return level


def deal_out(rng, own, number, rows, count, top, limit, slope):
    sequence = jax.random.permutation(rng, count)
    heavy_load, ordinary = portions_of(count, rows * top, limit, slope, True), portions_of(count, rows * top, limit, slope, False)
    places = jnp.arange(count)

    def named(tallies, rotation):
        used = int((tallies > 0).sum())
        fixed = max(1, used // 4)
        moved = fixed + (places - fixed + rotation * (used - fixed)) % max(1, count - fixed)
        return jnp.zeros((count,), jnp.int32).at[sequence[jnp.where(places < fixed, places, moved)]].set(jnp.asarray(tallies, jnp.int32))

    tallies = jnp.where(number % 4 == 0, named(heavy_load, number // 4), named(ordinary, number - number // 4 - 1))
    mixed = jax.random.permutation(jax.random.fold_in(own, 3), count)
    donor, sink = mixed[0:count // 2 * 2:2], mixed[1:count // 2 * 2:2]
    margin = jnp.minimum(tallies[donor] - 1, limit - tallies[sink]) // 2
    margin = jnp.where((donor == sequence[0]) | (sink == sequence[0]) | (tallies[sink] == 0), 0, jnp.maximum(margin, 0))
    moved = jax.random.randint(jax.random.fold_in(own, 4), (count // 2,), 0, 1 << 20) % (margin + 1)
    tallies = tallies.at[donor].add(-moved).at[sink].add(moved)
    items = jnp.searchsorted(jnp.cumsum(tallies), jnp.arange(rows * top), side="right").astype(jnp.int32)
    table = items.reshape(top, rows).T
    table = table[jax.random.permutation(jax.random.fold_in(own, 1), rows)]
    rotation = jax.random.randint(jax.random.fold_in(own, 2), (rows, 1), 0, top)
    return jnp.take_along_axis(table, (jnp.arange(top)[None, :] + rotation) % top, axis=1)


def portions_of(number_of, total, reach, skew, full):
    portions = [(1 << 20) // math.isqrt(grade ** skew) + 1 for grade in range(1, number_of + 1)]
    largest = reach if full else min(reach, max(-(-total // number_of), total * portions[0] // sum(portions)))
    least = 1 if total - largest >= number_of - 1 else 0
    counts, spare = [largest] + [least] * (number_of - 1), total - largest - least * (number_of - 1)
    while spare > 0:
        movable = [i for i in range(1, number_of) if counts[i] < largest] or [i for i in range(1, number_of) if counts[i] < reach]
        mass, budget = sum([portions[i] for i in movable]), spare
        for i in movable:
            more = min(reach - counts[i], max(1, budget * portions[i] // mass), spare)
            counts[i] = counts[i] + more
            spare = spare - more
    return np.array(counts)


def noise(key, dims, scale, most, pieces=(), held_as=jnp.bfloat16):
    array = jax.random.normal(key, dims, jnp.float32) * scale
    if len(pieces) > 0:
        array = levels(key, dims, pieces, -0.22, 0.18) * array
    return jnp.clip(array, min=-most, max=most).astype(held_as)


def setup_inputs(seed: int = 0) -> dict:
    streams_of = jax.random.split(jax.random.key(seed), 22)
    stream = noise(streams_of[0], (TOKENS, D), 0.4, 2.5, ((0, 256),))
    recurrence_input = noise(streams_of[1], (TOKENS, 2, D_HALF), 1.0, 6.0, ((0, 64), (2, 4)))
    output_gate_input = noise(streams_of[2], (TOKENS, 2, D_HALF), 1.0, 6.0, ((0, 64), (2, 4)))
    convolution_taps = noise(streams_of[3], (CONV, 2, D_HALF), 1.0, 4.0, ((2, 4),))
    first_group_gates = noise(streams_of[4], (2, HEADS_SMALL, HEAD_SMALL, HEAD_SMALL), HEAD_SMALL ** -0.5, 0.75, ((1, 4),))
    second_group_gates = noise(streams_of[5], (2, HEADS_LARGE, HEAD_LARGE, HEAD_LARGE), HEAD_LARGE ** -0.5, 0.5, ((1, 4),))
    channel_decay = draw_channel_decay(jax.random.fold_in(streams_of[21], 71), 0)
    position_log_extra = draw_position_log_extra(jax.random.fold_in(streams_of[21], 71), 0)
    recurrence_output_weight = noise(streams_of[8], (2, D_HALF, D), (2 * D_HALF) ** -0.5, 0.125, ((1, 4),))
    first_norm_gain = jnp.clip(1.0 + 0.18 * jax.random.normal(streams_of[9], (D,), jnp.float32), 0.1, 1.9)
    first_norm_bias = noise(streams_of[10], (D,), 0.3, 1.75, (), jnp.float32)
    routed_expert_index_keys = jax.random.split(jax.random.fold_in(streams_of[11], 1), TOKENS // TOK_Q)
    routed_expert_index_turns = jax.random.permutation(jax.random.fold_in(streams_of[11], 3), TOKENS // TOK_Q)
    routed_expert_index = jax.vmap(lambda own, number: deal_out(jax.random.fold_in(streams_of[11], 2), own, number, TOK_Q, EXPERTS, K, CAP_Q, 1))(routed_expert_index_keys, routed_expert_index_turns).reshape((TOKENS, K))
    routed_expert_weight = jnp.clip(0.25 + 0.75 * jax.random.uniform(streams_of[12], (TOKENS, K), jnp.float32) ** levels(streams_of[12], (TOKENS, K), ((0, 64),), -0.2, 0.2), 0.25, 1.0)
    routed_gate_weight = noise(streams_of[13], (EXPERTS, D, FE), D ** -0.5, 0.125, ((0, 64), (2, 4)))
    routed_up_weight = noise(streams_of[14], (EXPERTS, D, FE), D ** -0.5, 0.125, ((0, 64), (2, 4)))
    routed_down_weight = noise(streams_of[15], (EXPERTS, FE, D), FE ** -0.5, 0.25, ((0, 64), (1, 4)))
    shared_gate_weight = noise(streams_of[16], (D, FS), D ** -0.5, 0.125)
    shared_up_weight = noise(streams_of[17], (D, FS), D ** -0.5, 0.125)
    shared_down_weight = noise(streams_of[18], (FS, D), FS ** -0.5, 0.25)
    second_norm_gain = jnp.clip(1.0 + 0.18 * jax.random.normal(streams_of[19], (D,), jnp.float32), 0.1, 1.9)
    second_norm_bias = noise(streams_of[20], (D,), 0.3, 1.75, (), jnp.float32)
    return {"stream": stream, "recurrence_input": recurrence_input, "output_gate_input": output_gate_input, "convolution_taps": convolution_taps, "first_group_gates": first_group_gates, "second_group_gates": second_group_gates, "channel_decay": channel_decay, "position_log_extra": position_log_extra, "recurrence_output_weight": recurrence_output_weight, "first_norm_gain": first_norm_gain, "first_norm_bias": first_norm_bias, "routed_expert_index": routed_expert_index, "routed_expert_weight": routed_expert_weight, "routed_gate_weight": routed_gate_weight, "routed_up_weight": routed_up_weight, "routed_down_weight": routed_down_weight, "shared_gate_weight": shared_gate_weight, "shared_up_weight": shared_up_weight, "shared_down_weight": shared_down_weight, "second_norm_gain": second_norm_gain, "second_norm_bias": second_norm_bias}


RESIDUAL_SCALE = 8.0 ** 0.25
NORM_EPSILON = 1e-05

def layer_norm(values, gain_vec, bias_vec):
    row_mean = lax.optimization_barrier(jnp.mean(values, axis=-1, keepdims=True))
    spread = lax.optimization_barrier(jnp.mean(jnp.square(values - row_mean), axis=-1, keepdims=True))
    return (values - row_mean) * lax.rsqrt(spread + NORM_EPSILON) * gain_vec + bias_vec

def rounded(values):
    return lax.optimization_barrier(values.astype(jnp.bfloat16)).astype(jnp.float32)

def block_gates(conv_rows, weights, head_size):
    length = conv_rows.shape[0]
    head_rows = conv_rows.reshape(length, -1, head_size).astype(jnp.float32)
    pre_act = jnp.einsum('thc,ghcd->gthd', head_rows, weights.astype(jnp.float32))
    gate_pair = jax.nn.sigmoid(pre_act).reshape(2, length, -1)
    return (gate_pair[0], gate_pair[1])

def chain_link(first_part, second_part):
    return (first_part[0] * second_part[0], second_part[0] * first_part[1] + second_part[1])

def recurrence_result(recurrence_input, output_gate_input, convolution_taps, first_group_gates, second_group_gates, channel_decay, position_log_extra):
    length = recurrence_input.shape[0]
    tap_count = convolution_taps.shape[0]
    padded = jnp.pad(recurrence_input.astype(jnp.float32), ((tap_count - 1, 0), (0, 0), (0, 0)))
    tap_weights = convolution_taps.astype(jnp.float32)
    summed = tap_weights[0] * padded[0:length]
    for offset in range(1, tap_count):
        summed = summed + tap_weights[offset] * padded[offset:offset + length]
    conv_rows = summed.astype(jnp.bfloat16)
    recur_a, input_a = block_gates(conv_rows[:, 0], first_group_gates, first_group_gates.shape[-1])
    recur_b, input_b = block_gates(conv_rows[:, 1], second_group_gates, second_group_gates.shape[-1])
    recurrence_gate = jnp.stack([recur_a, recur_b], axis=1)
    input_gate = jnp.stack([input_a, input_b], axis=1)
    decay_logarithm = -8.0 * recurrence_gate * jax.nn.softplus(-channel_decay) + position_log_extra
    driving = jnp.sqrt(-jnp.expm1(2.0 * decay_logarithm)) * input_gate * conv_rows.astype(jnp.float32)
    states = lax.associative_scan(chain_link, (jnp.exp(decay_logarithm), driving), axis=0)[1]
    return (jax.nn.gelu(output_gate_input.astype(jnp.float32)) * states).astype(jnp.bfloat16)

def reference(stream, recurrence_input, output_gate_input, convolution_taps, first_group_gates, second_group_gates, channel_decay, position_log_extra, recurrence_output_weight, first_norm_gain, first_norm_bias, routed_expert_index, routed_expert_weight, routed_gate_weight, routed_up_weight, routed_down_weight, shared_gate_weight, shared_up_weight, shared_down_weight, second_norm_gain, second_norm_bias):
    branch_output = recurrence_result(recurrence_input, output_gate_input, convolution_taps, first_group_gates, second_group_gates, channel_decay, position_log_extra)
    run_rows = branch_output.reshape(TOKENS, 2, N_TP, DQ)
    run_weights = recurrence_output_weight.reshape(2, N_TP, DQ, D)
    mixed = jnp.zeros((TOKENS, D), jnp.float32)
    for run_index in range(N_TP):
        partial_value = jnp.einsum('tgc,gcd->td', run_rows[:, :, run_index].astype(jnp.float32), run_weights[:, run_index].astype(jnp.float32))
        mixed = mixed + rounded(partial_value)
    normed = layer_norm(RESIDUAL_SCALE * stream.astype(jnp.float32) + mixed, first_norm_gain, first_norm_bias).astype(jnp.bfloat16)
    block_count = TOKENS // TOK_Q
    block_ids = routed_expert_index.reshape(block_count, TOK_Q * K)
    onehot = (block_ids[:, :, None] == jnp.arange(EXPERTS, dtype=jnp.int32)[None, None, :]).astype(jnp.int32)
    slot_ranks = lax.optimization_barrier(jnp.sum((jnp.cumsum(onehot, axis=1) - onehot) * onehot, axis=2)).astype(jnp.int32)
    targets = (block_ids * block_count + jnp.arange(block_count, dtype=jnp.int32)[:, None]) * CAP_Q + slot_ranks
    entries = jnp.arange(TOKENS * K, dtype=jnp.int32).reshape(block_count, TOK_Q * K)
    table = jnp.full((EXPERTS * block_count * CAP_Q,), TOKENS * K, jnp.int32)
    table = table.at[targets.reshape(-1)].set(entries.reshape(-1)).reshape(EXPERTS, block_count * CAP_Q)
    padded_rows = jnp.concatenate([normed, jnp.zeros((1, D), jnp.bfloat16)], axis=0)
    padded_weights = jnp.concatenate([routed_expert_weight.reshape(-1), jnp.zeros((1,), jnp.float32)])

    def expert_step(routed, inputs):
        entry_rows, gate_w, up_w, down_w = inputs
        token_rows = entry_rows // K
        picked = padded_rows[token_rows]
        hidden = (jax.nn.silu(jnp.dot(picked, gate_w, preferred_element_type=jnp.float32)) * jnp.dot(picked, up_w, preferred_element_type=jnp.float32)).astype(jnp.bfloat16)
        summed_out = jnp.zeros((picked.shape[0], D), jnp.float32)
        for run_index in range(N_TP):
            partial_out = jnp.dot(hidden[:, run_index * FE_DEV:(run_index + 1) * FE_DEV], down_w[run_index * FE_DEV:(run_index + 1) * FE_DEV], preferred_element_type=jnp.float32)
            summed_out = summed_out + rounded(partial_out)
        weighted = padded_weights[entry_rows][:, None] * rounded(summed_out)
        return (routed.at[token_rows].add(weighted), None)
    routed = lax.scan(expert_step, jnp.zeros((TOKENS + 1, D), jnp.float32), (table, routed_gate_weight, routed_up_weight, routed_down_weight))[0][:TOKENS]
    shared_hidden = (jax.nn.silu(jnp.dot(normed, shared_gate_weight, preferred_element_type=jnp.float32)) * jnp.dot(normed, shared_up_weight, preferred_element_type=jnp.float32)).astype(jnp.bfloat16)
    shared_out = jnp.dot(shared_hidden, shared_down_weight, preferred_element_type=jnp.float32)
    moe = shared_out + routed
    final = layer_norm(RESIDUAL_SCALE * normed.astype(jnp.float32) + moe, second_norm_gain, second_norm_bias)
    return final.astype(jnp.bfloat16)
```

```python
import jax
import jax.numpy as jnp
from jax import lax
from jax.experimental import pallas as pl
from jax.experimental.pallas import tpu as pltpu
from jax.sharding import PartitionSpec as P

RESIDUAL_SCALE = 8.0**0.25
NORM_EPSILON = 1e-05


def copy_for_each(shard, axis):
    count = lax.axis_size(axis)
    return lax.all_to_all(
        jnp.broadcast_to(shard[None], (count, *shard.shape)), axis, 0, 0, tiled=True
    )


def all_in_one(shard, axis):
    leaves = jax.tree.leaves(shard)
    sequence = sorted(range(len(leaves)), key=lambda k: -leaves[k].size)
    width = (1, *leaves[sequence[0]].shape)[-1]
    lines = [
        jnp.pad(leaves[k].reshape(-1), (0, -leaves[k].size % width)).reshape(-1, width)
        for k in sequence
    ]
    both, at, found = (copy_for_each(jnp.concatenate(lines), axis), 0, {})
    for k, line in zip(sequence, lines):
        slab = both[:, at : at + len(line)].reshape(len(both), -1)
        found[k] = slab[:, : leaves[k].size].reshape(-1, *leaves[k].shape)
        at += len(line)
    numbers = iter(range(len(leaves)))
    return jax.tree.map(lambda _: found[next(numbers)], shard)


def joined_by_halves(pieces, combine):
    while len(jax.tree.leaves(pieces)[0]) > 1:
        pieces = jax.vmap(combine)(
            *(jax.tree.map(lambda part: part[side::2], pieces) for side in (0, 1))
        )
    return jax.tree.map(lambda part: part[0], pieces)


def entering(shard, axis, combine, identity):
    count, mine = (lax.axis_size(axis), lax.axis_index(axis))
    passed = jnp.arange(count) < mine

    def kept(part, zero, own):
        part = jnp.where(
            passed.reshape(-1, *(1 for _ in own.shape)), part, jnp.asarray(zero, own.dtype)
        )
        return part

    pieces = all_in_one(shard, axis)
    return joined_by_halves(jax.tree.map(kept, pieces, identity, shard), combine)


def shifted(shard, axis, by):
    count = lax.axis_size(axis)
    pairs = [(i, i + by) for i in range(count) if 0 <= i + by < count]
    return lax.ppermute(shard, axis, pairs)


def cut_along(shard, dim, count):
    dims = shard.shape
    pieces = shard.reshape(*dims[:dim], count, dims[dim] // count, *dims[dim + 1 :])
    return jnp.moveaxis(pieces, dim, 0)


def summed_on_arrival(shard, axis, dim):
    count = lax.axis_size(axis)
    pieces = lax.all_to_all(cut_along(shard, dim, count), axis, 0, 0, tiled=True)
    return jnp.sum(pieces.astype(jnp.float32), axis=0)


def layer_norm(values, gain_vec, bias_vec):
    row_mean = jnp.mean(values, axis=-1, keepdims=True)
    spread = jnp.mean(jnp.square(values - row_mean), axis=-1, keepdims=True)
    return (values - row_mean) * lax.rsqrt(spread + NORM_EPSILON) * gain_vec + bias_vec


def block_gates(conv_rows, weights, head_size):
    length = conv_rows.shape[0]
    head_rows = conv_rows.reshape(length, -1, head_size)
    pre_act = jnp.einsum("thc,ghcd->gthd", head_rows, weights, preferred_element_type=jnp.float32)
    gate_pair = jax.nn.sigmoid(pre_act).reshape(2, length, -1)
    return (gate_pair[0], gate_pair[1])


def chain_link(first_part, second_part):
    return (first_part[0] * second_part[0], second_part[0] * first_part[1] + second_part[1])


def carried(totals):
    unity = jnp.ones_like(totals[0])
    nought = jnp.zeros_like(totals[1])
    return entering(totals, "sp", chain_link, (unity, nought))[1]


def turned(shard, axis, by):
    count = lax.axis_size(axis)
    return lax.ppermute(shard, axis, [(i, (i + by) % count) for i in range(count)])


def weights_of_expert(gate_w, up_w, down_w):
    near = {(name, by): turned(w, "tp", by) for name, w in (("g", gate_w), ("u", up_w)) for by in (1, -1)}
    near.update({("d", by): turned(down_w, "tp", by) for by in (1, -1)})
    half = down_w.shape[0] // 2
    gate_far = turned(near["g", 1], "tp", 1)
    up_far = turned(near["u", -1], "tp", -1)
    down_far = (turned(near["d", 1][:half], "tp", 1), turned(near["d", -1][half:], "tp", -1))
    gates = [gate_w, near["g", 1], near["g", -1], gate_far]
    ups = [up_w, near["u", 1], near["u", -1], up_far]
    downs = [down_w, near["d", 1], near["d", -1], *down_far]
    return gates, ups, downs


def expert_kernel(rows, g0, g1, g2, g3, u0, u1, u2, u3, d0, d1, d2, d3a, d3b, out):
    picked = rows[...]
    hidden = []
    for gate_w, up_w in ((g0, u0), (g1, u1), (g2, u2), (g3, u3)):
        both = jnp.concatenate([gate_w[...], up_w[...]], axis=1)
        pair = jnp.dot(picked, both, preferred_element_type=jnp.float32)
        width = gate_w.shape[1]
        gated, lifted = pair[:, :width], pair[:, width:]
        hidden.append((gated * jax.nn.sigmoid(gated) * lifted).astype(jnp.bfloat16))
    half = d3a.shape[0]
    acc = jnp.dot(hidden[0], d0[...], preferred_element_type=jnp.float32)
    acc += jnp.dot(hidden[1], d1[...], preferred_element_type=jnp.float32)
    acc += jnp.dot(hidden[2], d2[...], preferred_element_type=jnp.float32)
    acc += jnp.dot(hidden[3], jnp.concatenate([d3a[...], d3b[...]], axis=0), preferred_element_type=jnp.float32)
    out[...] = acc.astype(jnp.bfloat16)


def expert_rows(rows, gates, ups, downs):
    operands = (rows, *gates, *ups, *downs)
    return pl.pallas_call(
        expert_kernel,
        out_shape=jax.ShapeDtypeStruct(rows.shape, jnp.bfloat16),
        in_specs=[pl.BlockSpec(memory_space=pltpu.VMEM) for _ in operands],
        out_specs=pl.BlockSpec(memory_space=pltpu.VMEM),
        name="experts",
    )(*operands)


def shards(
    stream,
    recurrence_input,
    output_gate_input,
    convolution_taps,
    first_group_gates,
    second_group_gates,
    channel_decay,
    position_log_extra,
    recurrence_output_weight,
    first_norm_gain,
    first_norm_bias,
    routed_expert_index,
    routed_expert_weight,
    routed_gate_weight,
    routed_up_weight,
    routed_down_weight,
    shared_gate_weight,
    shared_up_weight,
    shared_down_weight,
    second_norm_gain,
    second_norm_bias,
):
    length = recurrence_input.shape[0]
    tap_count = convolution_taps.shape[0]
    border = shifted(recurrence_input[length - (tap_count - 1) :], "sp", 1)
    padded = jnp.concatenate([border, recurrence_input], axis=0).astype(jnp.float32)
    tap_weights = convolution_taps.astype(jnp.float32)
    summed = tap_weights[0] * padded[0:length]
    for offset in range(1, tap_count):
        summed = summed + tap_weights[offset] * padded[offset : offset + length]
    conv_rows = summed.astype(jnp.bfloat16)
    recur_a, input_a = block_gates(conv_rows[:, 0], first_group_gates, first_group_gates.shape[-1])
    recur_b, input_b = block_gates(
        conv_rows[:, 1], second_group_gates, second_group_gates.shape[-1]
    )
    recurrence_gate = jnp.stack([recur_a, recur_b], axis=1)
    input_gate = jnp.stack([input_a, input_b], axis=1)
    decay_logarithm = -8.0 * recurrence_gate * jax.nn.softplus(-channel_decay) + position_log_extra
    decay_rate = jnp.exp(decay_logarithm)
    driving = (
        jnp.sqrt(-jnp.expm1(2.0 * decay_logarithm)) * input_gate * conv_rows.astype(jnp.float32)
    )
    running = jnp.cumsum(decay_logarithm, axis=0)
    tail_sum = jnp.sum(jnp.exp(running[-1] - running) * driving, axis=0)
    incoming = carried((jnp.exp(running[-1]), tail_sum))
    opening = driving[:1] + decay_rate[:1] * incoming
    started = jnp.concatenate([opening, driving[1:]], axis=0)
    states = lax.associative_scan(chain_link, (decay_rate, started), axis=0)[1]
    branch_output = (jax.nn.gelu(output_gate_input.astype(jnp.float32)) * states).astype(
        jnp.bfloat16
    )
    tp_count = lax.axis_size("tp")
    quarter = length // tp_count
    mixed = summed_on_arrival(
        jnp.einsum(
            "tgc,gcd->td",
            branch_output,
            recurrence_output_weight,
            preferred_element_type=jnp.float32,
        ).astype(jnp.bfloat16),
        "tp",
        0,
    )
    normed = layer_norm(
        RESIDUAL_SCALE * stream.astype(jnp.float32) + mixed, first_norm_gain, first_norm_bias
    ).astype(jnp.bfloat16)
    width = normed.shape[1]
    expert_count = routed_gate_weight.shape[0] * lax.axis_size("sp")
    own_index = lax.axis_index("tp")
    own_ids = lax.dynamic_slice_in_dim(routed_expert_index, own_index * quarter, quarter, 0)
    own_weights = lax.dynamic_slice_in_dim(routed_expert_weight, own_index * quarter, quarter, 0)
    slots = 2
    named = own_ids[None, :, :] == jnp.arange(expert_count, dtype=jnp.int32)[:, None, None]
    weight_of = jnp.sum(jnp.where(named, own_weights[None], 0.0), axis=2)
    names = jnp.any(named, axis=2)
    earlier = jnp.arange(quarter)[:, None] < jnp.arange(quarter)[None, :]
    ranks = jnp.sum((names[:, :, None] & earlier[None]).astype(jnp.int32), axis=1)
    taken = names[:, None, :] & (ranks[:, None, :] == jnp.arange(slots)[None, :, None])
    select = taken.astype(jnp.bfloat16).reshape(expert_count * slots, quarter)
    merge = jnp.where(taken, weight_of[:, None, :], 0.0).reshape(expert_count * slots, quarter)
    outgoing = jnp.dot(select, normed, preferred_element_type=jnp.float32).astype(jnp.bfloat16)
    arrived = lax.all_to_all(
        outgoing.reshape(expert_count, slots, width), "sp", split_axis=0, concat_axis=0, tiled=True
    )
    leaving = expert_rows(
        arrived.reshape(-1, width),
        *weights_of_expert(routed_gate_weight[0], routed_up_weight[0], routed_down_weight[0]),
    )
    returned = lax.all_to_all(
        leaving.reshape(-1, slots, width), "sp", split_axis=0, concat_axis=0, tiled=True
    ).reshape(-1, width)
    routed = lax.dot_general(
        merge,
        returned.astype(jnp.float32),
        (((0,), (0,)), ((), ())),
        precision=lax.Precision.HIGHEST,
        preferred_element_type=jnp.float32,
    )
    shared_hidden = (
        jax.nn.silu(jnp.dot(normed, shared_gate_weight, preferred_element_type=jnp.float32))
        * jnp.dot(normed, shared_up_weight, preferred_element_type=jnp.float32)
    ).astype(jnp.bfloat16)
    shared_out = jnp.dot(shared_hidden, shared_down_weight, preferred_element_type=jnp.float32)
    final = layer_norm(
        RESIDUAL_SCALE * normed.astype(jnp.float32) + (shared_out + routed),
        second_norm_gain,
        second_norm_bias,
    )
    return final.astype(jnp.bfloat16)


def solution(mesh):
    in_specs = (
        P(("sp", "tp"), None),
        P("sp", None, "tp"),
        P("sp", None, "tp"),
        P(None, None, "tp"),
        P(None, "tp", None, None),
        P(None, "tp", None, None),
        P(None, "tp"),
        P("sp", None, "tp"),
        P(None, "tp", None),
        P(),
        P(),
        P("sp", None),
        P("sp", None),
        P("sp", None, "tp"),
        P("sp", None, "tp"),
        P("sp", "tp", None),
        P(),
        P(),
        P(),
        P(),
        P(),
    )
    out_specs = P(("sp", "tp"), None)
    return jax.shard_map(shards, mesh=mesh, in_specs=in_specs, out_specs=out_specs, check_vma=False)
```

```python
import jax
import jax.numpy as jnp
from jax import lax
from jax.experimental import pallas as pl
from jax.experimental.pallas import tpu as pltpu
from jax.sharding import Mesh
from jax.sharding import PartitionSpec as P

RESIDUAL_SCALE = 8.0**0.25
NORM_EPSILON = 1e-05
LANES = 128
SLOTS = 2
BF16, F32 = jnp.bfloat16, jnp.float32
VMEM = pl.BlockSpec(memory_space=pltpu.VMEM)
SMEM = pl.BlockSpec(memory_space=pltpu.SMEM)


def kernel_call(body, out_shape, *operands, scalars=0, scratch=()):
    several = isinstance(out_shape, (list, tuple))
    return pl.pallas_call(
        body,
        out_shape=out_shape,
        in_specs=[SMEM] * scalars + [VMEM] * (len(operands) - scalars),
        out_specs=[VMEM] * len(out_shape) if several else VMEM,
        scratch_shapes=scratch,
    )(*operands)


def dot(a, b):
    return jnp.dot(a, b, preferred_element_type=F32)


def layer_norm(values, gain_vec, bias_vec):
    row_mean = jnp.mean(values, axis=-1, keepdims=True)
    spread = jnp.mean(jnp.square(values - row_mean), axis=-1, keepdims=True)
    return (values - row_mean) * lax.rsqrt(spread + NORM_EPSILON) * gain_vec + bias_vec


def softplus(x):
    u = jnp.exp(-jnp.abs(x))
    s = u / (2.0 + u)
    q = s * s
    series = 1.0 / 17.0
    for k in (15.0, 13.0, 11.0, 9.0, 7.0, 5.0, 3.0, 1.0):
        series = series * q + 1.0 / k
    return jnp.maximum(x, 0.0) + 2.0 * s * series


def expm1(z):
    series = 1.0 + z * (1.0 / 9.0)
    for k in (8.0, 7.0, 6.0, 5.0, 4.0, 3.0, 2.0):
        series = 1.0 + z * (1.0 / k) * series
    return jnp.where(jnp.abs(z) < 0.5, z * series, jnp.exp(z) - 1.0)


def shifted_rows(values, by, row, fill):
    if by < 8:
        return jnp.where(row >= by, pltpu.roll(values, by, 0), fill)
    head = jnp.full((by, values.shape[1]), fill, values.dtype)
    return jnp.concatenate([head, values[: values.shape[0] - by]], axis=0)


def chain_rows(decay, drive):
    row = lax.broadcasted_iota(jnp.int32, decay.shape, 0)
    by = 1
    while by < decay.shape[0]:
        drive = decay * shifted_rows(drive, by, row, 0.0) + drive
        decay = decay * shifted_rows(decay, by, row, 1.0)
        by *= 2
    return decay, drive


def local_kernel(rows, border, taps, small_maps, large_maps, decay_param, extra, decays, states, totals, padded, maps):
    length, half = rows.shape[1], rows.shape[2]
    tap_count = taps.shape[0]
    tap_weights = taps[...].astype(F32)
    rate = -8.0 * softplus(-decay_param[...])
    margin = border.shape[1]
    per_half = half // LANES
    for g, blocks in enumerate((small_maps, large_maps)):
        padded[0:margin] = border[g].astype(F32)
        padded[margin : margin + length] = rows[g].astype(F32)
        start = margin - (tap_count - 1)
        summed = tap_weights[0, g : g + 1] * padded[start : start + length]
        for k in range(1, tap_count):
            summed = summed + tap_weights[k, g : g + 1] * padded[start + k : start + k + length]
        conv_rows = summed.astype(BF16)
        maps[...] = jnp.zeros(maps.shape, BF16)
        head = blocks.shape[-1]
        for m in range(2):
            for h in range(blocks.shape[1]):
                maps[h * head : (h + 1) * head, m * half + h * head : m * half + (h + 1) * head] = blocks[m, h]
        gates = jax.nn.sigmoid(dot(conv_rows, maps[...]))
        log_decay = gates[:, :half] * rate[g : g + 1] + extra[g]
        drive = jnp.sqrt(-expm1(2.0 * log_decay)) * gates[:, half:] * conv_rows.astype(F32)
        decay = jnp.exp(log_decay)
        for c in range(per_half):
            at = slice(c * LANES, (c + 1) * LANES)
            run = g * per_half + c
            product, state = chain_rows(decay[:, at], drive[:, at])
            to = slice(run * LANES, (run + 1) * LANES)
            decays[:, to] = product
            states[:, to] = state
            for j in range(totals.shape[0]):
                totals[j, run : run + 1] = product[length - 1 :]
                totals[j, 2 * per_half + run : 2 * per_half + run + 1] = state[length - 1 :]


def joined(first, second):
    return first[0] * second[0], second[0] * first[1] + second[1]


def before_mine(spans, mine):
    half = spans.shape[1] // 2
    ahead = (jnp.ones((half, LANES), F32), jnp.zeros((half, LANES), F32))
    whole = ahead
    for j in range(spans.shape[0]):
        span = (spans[j, :half], spans[j, half:])
        whole = joined(whole, span)
        passed = j < mine
        ahead = tuple(jnp.where(passed, new, old) for new, old in zip(whole, ahead))
    return ahead, whole


def near_kernel(mine, spans, ahead, totals):
    half = spans.shape[1] // 2
    first, whole = before_mine(spans, mine[0])
    ahead[:half], ahead[half:] = first
    for j in range(totals.shape[0]):
        totals[j, :half], totals[j, half:] = whole


def project_kernel(mine, spans, ahead, decays, states, gate_rows, weight, out):
    half = spans.shape[1] // 2
    far, _ = before_mine(spans, mine[0])
    entering = joined(far, (ahead[:half], ahead[half:]))[1]
    width = gate_rows.shape[2]
    per_half = width // LANES
    acc = None
    for g in range(gate_rows.shape[0]):
        start = jnp.concatenate([entering[g * per_half + c : g * per_half + c + 1] for c in range(per_half)], axis=1)
        at = slice(g * width, (g + 1) * width)
        state = states[:, at] + decays[:, at] * start
        branch = (jax.nn.gelu(gate_rows[g].astype(F32), approximate=True) * state).astype(BF16)
        part = dot(branch, weight[g])
        acc = part if acc is None else acc + part
    out[...] = acc.astype(BF16).reshape(out.shape)


def route_kernel(ids, weights, select, merge):
    slot_count, rows = select.shape[0], ids.shape[1]
    slot = lax.broadcasted_iota(jnp.int32, (slot_count, rows), 0)
    names = jnp.zeros((slot_count, rows), F32)
    weight = jnp.zeros((slot_count, rows), F32)
    for k in range(ids.shape[0]):
        named = ids[k : k + 1] == slot // SLOTS
        names = jnp.where(named, 1.0, names)
        weight = jnp.where(named, weights[k : k + 1], weight)
    earlier = lax.broadcasted_iota(jnp.int32, (rows, rows), 0) < lax.broadcasted_iota(jnp.int32, (rows, rows), 1)
    rank = dot(names.astype(BF16), jnp.where(earlier, 1.0, 0.0).astype(BF16))
    taken = (names > 0.0) & (rank == (slot % SLOTS).astype(F32))
    select[...] = jnp.where(taken, 1.0, 0.0).astype(BF16)[:, : select.shape[1]]
    merge[...] = jnp.where(taken, weight, 0.0).T[: merge.shape[0]]


def mix_kernel(parts, stream, gain, bias, select, normed, outgoing):
    mixed = parts[0].astype(F32)
    for j in range(1, parts.shape[0]):
        mixed = mixed + parts[j].astype(F32)
    rows = layer_norm(RESIDUAL_SCALE * stream[...].astype(F32) + mixed, gain[...], bias[...]).astype(BF16)
    normed[...] = rows
    outgoing[...] = dot(select[...], rows).astype(BF16)


def shared_kernel(normed, gate_w, up_w, down_w, base):
    rows = normed[...]
    gated, lifted = dot(rows, gate_w[...]), dot(rows, up_w[...])
    hidden = (jax.nn.silu(gated) * lifted).astype(BF16)
    base[...] = RESIDUAL_SCALE * rows.astype(F32) + dot(hidden, down_w[...])


def expert_kernel(rows, g0, g1, g2, g3, u0, u1, u2, u3, d0, d1, d2, d3a, d3b, out):
    picked = rows[...]
    hidden = []
    for gate_w, up_w in ((g0, u0), (g1, u1), (g2, u2), (g3, u3)):
        pair = dot(picked, jnp.concatenate([gate_w[...], up_w[...]], axis=1))
        width = gate_w.shape[1]
        hidden.append((jax.nn.silu(pair[:, :width]) * pair[:, width:]).astype(BF16))
    down = jnp.concatenate([d3a[...], d3b[...]], axis=0)
    acc = dot(hidden[0], d0[...]) + dot(hidden[1], d1[...]) + dot(hidden[2], d2[...]) + dot(hidden[3], down)
    out[...] = acc.astype(BF16)


def merge_kernel(merge, returned, base, gain, bias, out):
    rest = merge[...]
    rows = returned[...]
    total = base[...]
    for _ in range(3):
        part = rest.astype(BF16)
        total = total + dot(part, rows)
        rest = rest - part.astype(F32)
    out[...] = layer_norm(total, gain[...], bias[...]).astype(BF16)


def turned(shard, by):
    count = lax.axis_size("tp")
    return lax.ppermute(shard, "tp", [(i, (i + by) % count) for i in range(count)])


def swapped(pieces, axis):
    return lax.all_to_all(pieces, axis, 0, 0, tiled=True)


def shards(
    stream,
    recurrence_input,
    output_gate_input,
    convolution_taps,
    first_group_gates,
    second_group_gates,
    channel_decay,
    position_log_extra,
    recurrence_output_weight,
    first_norm_gain,
    first_norm_bias,
    routed_expert_index,
    routed_expert_weight,
    routed_gate_weight,
    routed_up_weight,
    routed_down_weight,
    shared_gate_weight,
    shared_up_weight,
    shared_down_weight,
    second_norm_gain,
    second_norm_bias,
):
    length, groups, half = recurrence_input.shape
    width = stream.shape[1]
    tp_count, far_count, near_count = (lax.axis_size(a) for a in ("tp", "far", "near"))
    quarter = length // tp_count
    sp_axes = ("far", "near")
    expert_count = routed_gate_weight.shape[0] * far_count * near_count
    slot_count = expert_count * SLOTS
    channels = groups * half

    rows = jnp.transpose(recurrence_input, (1, 0, 2))
    margin = 8
    sp_count = far_count * near_count
    border = lax.ppermute(rows[:, length - margin :], sp_axes, [(i, i + 1) for i in range(sp_count - 1)])

    gate_w, up_w, down_w = routed_gate_weight[0], routed_up_weight[0], routed_down_weight[0]
    gate_left, up_right = turned(gate_w, 1), turned(up_w, -1)
    up_left, gate_right = turned(up_w, 1), turned(gate_w, -1)

    own_index = lax.axis_index("tp")
    own_ids = lax.dynamic_slice_in_dim(routed_expert_index.T, own_index * quarter, quarter, 1)
    own_weights = lax.dynamic_slice_in_dim(routed_expert_weight.T, own_index * quarter, quarter, 1)
    fill = ((0, 0), (0, LANES - quarter))
    select, merge = kernel_call(
        route_kernel,
        [jax.ShapeDtypeStruct((slot_count, quarter), BF16), jax.ShapeDtypeStruct((quarter, slot_count), F32)],
        jnp.pad(own_ids, fill, constant_values=-1),
        jnp.pad(own_weights, fill),
    )

    runs = channels // LANES
    span = jax.ShapeDtypeStruct((2 * runs, LANES), F32)
    decays, states, totals = kernel_call(
        local_kernel,
        [
            jax.ShapeDtypeStruct((length, channels), F32),
            jax.ShapeDtypeStruct((length, channels), F32),
            jax.ShapeDtypeStruct((near_count, 2 * runs, LANES), F32),
        ],
        rows,
        border,
        convolution_taps,
        first_group_gates,
        second_group_gates,
        channel_decay,
        jnp.transpose(position_log_extra, (1, 0, 2)),
        scratch=(pltpu.VMEM((margin + length, half), F32), pltpu.VMEM((half, 2 * half), BF16)),
    )
    near_spans = swapped(totals, "near")
    ahead, totals = kernel_call(
        near_kernel,
        [span, jax.ShapeDtypeStruct((far_count, 2 * runs, LANES), F32)],
        lax.axis_index("near").reshape(1),
        near_spans,
        scalars=1,
    )
    far_spans = swapped(totals, "far")
    parts = kernel_call(
        project_kernel,
        jax.ShapeDtypeStruct((tp_count, quarter, width), BF16),
        lax.axis_index("far").reshape(1),
        far_spans,
        ahead,
        decays,
        states,
        jnp.transpose(output_gate_input, (1, 0, 2)),
        recurrence_output_weight,
        scalars=1,
    )
    parts = swapped(parts, "tp")

    down_left, down_right = turned(down_w, 1), turned(down_w, -1)
    gate_far, up_far = turned(gate_left, 1), turned(up_right, -1)

    normed, outgoing = kernel_call(
        mix_kernel,
        [jax.ShapeDtypeStruct((quarter, width), BF16), jax.ShapeDtypeStruct((slot_count, width), BF16)],
        parts,
        stream,
        first_norm_gain.reshape(1, width),
        first_norm_bias.reshape(1, width),
        select,
    )
    arrived = swapped(outgoing.reshape(expert_count, SLOTS, width), sp_axes)

    cut = down_w.shape[0] // 2
    down_far = turned(down_left[:cut], 1), turned(down_right[cut:], -1)

    base = kernel_call(
        shared_kernel,
        jax.ShapeDtypeStruct((quarter, width), F32),
        normed,
        shared_gate_weight,
        shared_up_weight,
        shared_down_weight,
    )
    leaving = kernel_call(
        expert_kernel,
        jax.ShapeDtypeStruct((slot_count, width), BF16),
        arrived.reshape(slot_count, width),
        *(gate_w, gate_left, gate_right, gate_far),
        *(up_w, up_left, up_right, up_far),
        *(down_w, down_left, down_right, *down_far),
    )
    returned = swapped(leaving.reshape(expert_count, SLOTS, width), sp_axes)
    return kernel_call(
        merge_kernel,
        jax.ShapeDtypeStruct((quarter, width), BF16),
        merge,
        returned.reshape(slot_count, width),
        base,
        second_norm_gain.reshape(1, width),
        second_norm_bias.reshape(1, width),
    )


def solution(mesh):
    near = 8
    shape = (mesh.shape["sp"] // near, near, mesh.shape["tp"])
    fine = Mesh(mesh.devices.reshape(shape), ("far", "near", "tp"))
    sp = ("far", "near")
    in_specs = (
        P((*sp, "tp"), None),
        P(sp, None, "tp"),
        P(sp, None, "tp"),
        P(None, None, "tp"),
        P(None, "tp", None, None),
        P(None, "tp", None, None),
        P(None, "tp"),
        P(sp, None, "tp"),
        P(None, "tp", None),
        P(),
        P(),
        P(sp, None),
        P(sp, None),
        P(sp, None, "tp"),
        P(sp, None, "tp"),
        P(sp, "tp", None),
        P(),
        P(),
        P(),
        P(),
        P(),
    )

    return jax.shard_map(shards, mesh=fine, in_specs=in_specs, out_specs=P((*sp, "tp"), None), check_vma=False)
```

```python
import jax
import jax.numpy as jnp
from jax import lax
from jax.experimental import pallas as pl
from jax.experimental.pallas import tpu as pltpu
from jax.sharding import PartitionSpec as P

RESIDUAL_SCALE = 8.0**0.25
NORM_EPSILON = 1e-05
LANES = 128
SLOTS = 2
BF16, F32 = jnp.bfloat16, jnp.float32
VMEM = pl.BlockSpec(memory_space=pltpu.VMEM)
SMEM = pl.BlockSpec(memory_space=pltpu.SMEM)
ANY = pl.BlockSpec(memory_space=pl.ANY)


def kernel_call(body, out_shape, *operands, scratch=(), limit=16):
    several = isinstance(out_shape, (list, tuple))
    specs, arrays = [], []
    for operand in operands:
        array, place = operand if isinstance(operand, tuple) else (operand, None)
        specs.append({"smem": SMEM, "hbm": ANY}.get(place, VMEM))
        if place != "smem":
            array = pltpu.with_memory_space_constraint(array, pltpu.VMEM if place == "vmem" else pltpu.HBM)
        arrays.append(array)
    return pl.pallas_call(
        body,
        out_shape=out_shape,
        in_specs=specs,
        out_specs=[VMEM] * len(out_shape) if several else VMEM,
        scratch_shapes=scratch,
        compiler_params=pltpu.CompilerParams(vmem_limit_bytes=limit << 20),
    )(*arrays)


def fetched(pairs, sems):
    copies = [pltpu.make_async_copy(source, target, sems.at[k]) for k, (source, target) in enumerate(pairs)]
    for copy in copies:
        copy.start()
    return copies


def dot(a, b):
    return jnp.dot(a, b, preferred_element_type=F32)


def layer_norm(values, gain_vec, bias_vec):
    row_mean = jnp.mean(values, axis=-1, keepdims=True)
    spread = jnp.mean(jnp.square(values - row_mean), axis=-1, keepdims=True)
    return (values - row_mean) * lax.rsqrt(spread + NORM_EPSILON) * gain_vec + bias_vec


def softplus(x):
    u = jnp.exp(-jnp.abs(x))
    s = u / (2.0 + u)
    q = s * s
    series = 1.0 / 17.0
    for k in (15.0, 13.0, 11.0, 9.0, 7.0, 5.0, 3.0, 1.0):
        series = series * q + 1.0 / k
    return jnp.maximum(x, 0.0) + 2.0 * s * series


def expm1(z):
    series = 1.0 + z * (1.0 / 9.0)
    for k in (8.0, 7.0, 6.0, 5.0, 4.0, 3.0, 2.0):
        series = 1.0 + z * (1.0 / k) * series
    return jnp.where(jnp.abs(z) < 0.5, z * series, jnp.exp(z) - 1.0)


def shifted_rows(values, by, row, fill):
    if by < 8:
        return jnp.where(row >= by, pltpu.roll(values, by, 0), fill)
    head = jnp.full((by, values.shape[1]), fill, values.dtype)
    return jnp.concatenate([head, values[: values.shape[0] - by]], axis=0)


def chain_rows(decay, drive):
    row = lax.broadcasted_iota(jnp.int32, decay.shape, 0)
    by = 1
    while by < decay.shape[0]:
        drive = decay * shifted_rows(drive, by, row, 0.0) + drive
        decay = decay * shifted_rows(decay, by, row, 1.0)
        by *= 2
    return decay, drive


def local_kernel(rows, border, taps, small_maps, large_maps, decay_param, extra, decays, states, totals, padded, maps):
    length, half = rows.shape[1], rows.shape[2]
    tap_count = taps.shape[0]
    tap_weights = taps[...].astype(F32)
    rate = -8.0 * softplus(-decay_param[...])
    margin = border.shape[1]
    per_half = half // LANES
    products, ends = [], []
    for g, blocks in enumerate((small_maps, large_maps)):
        padded[0:margin] = border[g].astype(F32)
        padded[margin : margin + length] = rows[g].astype(F32)
        start = margin - (tap_count - 1)
        summed = tap_weights[0, g : g + 1] * padded[start : start + length]
        for k in range(1, tap_count):
            summed = summed + tap_weights[k, g : g + 1] * padded[start + k : start + k + length]
        conv_rows = summed.astype(BF16)
        maps[...] = jnp.zeros(maps.shape, BF16)
        head = blocks.shape[-1]
        for m in range(2):
            for h in range(blocks.shape[1]):
                maps[h * head : (h + 1) * head, m * half + h * head : m * half + (h + 1) * head] = blocks[m, h]
        gates = jax.nn.sigmoid(dot(conv_rows, maps[...]))
        log_decay = gates[:, :half] * rate[g : g + 1] + extra[g]
        drive = jnp.sqrt(-expm1(2.0 * log_decay)) * gates[:, half:] * conv_rows.astype(F32)
        decay = jnp.exp(log_decay)
        for c in range(per_half):
            at = slice(c * LANES, (c + 1) * LANES)
            run = g * per_half + c
            product, state = chain_rows(decay[:, at], drive[:, at])
            to = slice(run * LANES, (run + 1) * LANES)
            decays[:, to] = product
            states[:, to] = state
            products.append(product[length - 1 :])
            ends.append(state[length - 1 :])
    span = jnp.concatenate(products + ends, axis=0)
    for j in range(totals.shape[0]):
        totals[j] = span


def joined(first, second):
    return first[0] * second[0], second[0] * first[1] + second[1]


def before_mine(spans, mine):
    half = spans.shape[1] // 2
    ahead = (jnp.ones((half, LANES), F32), jnp.zeros((half, LANES), F32))
    for j in range(spans.shape[0] - 1):
        new = joined(ahead, (spans[j, :half], spans[j, half:]))
        passed = j < mine
        ahead = tuple(jnp.where(passed, n, old) for n, old in zip(new, ahead))
    return ahead


def project_kernel(mine, spans, decays, states, gate_rows, weight_far, out, weight, sems):
    (copy,) = fetched([(weight_far, weight)], sems)
    entering = before_mine(spans, mine[0])[1]
    width = gate_rows.shape[2]
    per_half = width // LANES
    branches = []
    for g in range(gate_rows.shape[0]):
        start = jnp.concatenate([entering[g * per_half + c : g * per_half + c + 1] for c in range(per_half)], axis=1)
        at = slice(g * width, (g + 1) * width)
        state = states[:, at] + decays[:, at] * start
        branches.append((jax.nn.gelu(gate_rows[g].astype(F32), approximate=True) * state).astype(BF16))
    copy.wait()
    acc = dot(branches[0], weight[0])
    for g in range(1, len(branches)):
        acc = acc + dot(branches[g], weight[g])
    out[...] = acc.astype(BF16).reshape(out.shape)


def route_kernel(ids, weights, select, merge):
    slot_count, rows = select.shape[0], ids.shape[1]
    slot = lax.broadcasted_iota(jnp.int32, (slot_count, rows), 0)
    names = jnp.zeros((slot_count, rows), F32)
    weight = jnp.zeros((slot_count, rows), F32)
    for k in range(ids.shape[0]):
        named = ids[k : k + 1] == slot // SLOTS
        names = jnp.where(named, 1.0, names)
        weight = jnp.where(named, weights[k : k + 1], weight)
    earlier = lax.broadcasted_iota(jnp.int32, (rows, rows), 0) < lax.broadcasted_iota(jnp.int32, (rows, rows), 1)
    rank = dot(names.astype(BF16), jnp.where(earlier, 1.0, 0.0).astype(BF16))
    taken = (names > 0.0) & (rank == (slot % SLOTS).astype(F32))
    select[...] = jnp.where(taken, 1.0, 0.0).astype(BF16)[:, : select.shape[1]]
    merge[...] = jnp.where(taken, weight, 0.0).T[: merge.shape[0]]


def mix_kernel(parts, stream, gain, bias, select, normed, outgoing):
    mixed = parts[0].astype(F32)
    for j in range(1, parts.shape[0]):
        mixed = mixed + parts[j].astype(F32)
    rows = layer_norm(RESIDUAL_SCALE * stream[...].astype(F32) + mixed, gain[...], bias[...]).astype(BF16)
    normed[...] = rows
    outgoing[...] = dot(select[...], rows).astype(BF16).reshape(outgoing.shape)


def shared_kernel(normed, gate_w, up_w, down_w, merge, gain, bias, base, *kept):
    for target, source in zip(kept, (merge, gain, bias)):
        target[...] = source[...]
    rows = normed[...]
    gated, lifted = dot(rows, gate_w[...]), dot(rows, up_w[...])
    hidden = (jax.nn.silu(gated) * lifted).astype(BF16)
    base[...] = RESIDUAL_SCALE * rows.astype(F32) + dot(hidden, down_w[...])


def expert_kernel(rows, g0, g1, g2, g3, u0, u1, u2, u3, d0, d1, d2, d3a, d3b, out, pairs, down, sems):
    width = g0.shape[1]
    moves = []
    for j, (gate_w, up_w) in enumerate(((g0, u0), (g1, u1), (g2, u2), (g3, u3))):
        moves += [(gate_w, pairs.at[j, :, 0:width]), (up_w, pairs.at[j, :, width : 2 * width])]
    at = 0
    for piece in (d0, d1, d2, d3a, d3b):
        moves.append((piece, down.at[at : at + piece.shape[0]]))
        at += piece.shape[0]
    copies = fetched(moves, sems)
    picked = rows[...].reshape(-1, rows.shape[-1])
    hidden = []
    for j in range(pairs.shape[0]):
        copies[2 * j].wait()
        copies[2 * j + 1].wait()
        pair = dot(picked, pairs[j])
        hidden.append((jax.nn.silu(pair[:, :width]) * pair[:, width:]).astype(BF16))
    for copy in copies[2 * pairs.shape[0] :]:
        copy.wait()
    acc = dot(jnp.concatenate(hidden, axis=1), down[...])
    out[...] = acc.astype(BF16).reshape(out.shape)


def merge_kernel(returned, base, merge, gain, bias, out):
    rest = merge[...]
    rows = returned[...].reshape(-1, returned.shape[-1])
    total = base[...]
    for _ in range(3):
        part = rest.astype(BF16)
        total = total + dot(part, rows)
        rest = rest - part.astype(F32)
    out[...] = layer_norm(total, gain[...], bias[...]).astype(BF16)


def turned(shard, by):
    count = lax.axis_size("tp")
    return lax.ppermute(shard, "tp", [(i, (i + by) % count) for i in range(count)])


def swapped(pieces, axis):
    return lax.all_to_all(pieces, axis, 0, 0, tiled=True)


def shards(
    stream,
    recurrence_input,
    output_gate_input,
    convolution_taps,
    first_group_gates,
    second_group_gates,
    channel_decay,
    position_log_extra,
    recurrence_output_weight,
    first_norm_gain,
    first_norm_bias,
    routed_expert_index,
    routed_expert_weight,
    routed_gate_weight,
    routed_up_weight,
    routed_down_weight,
    shared_gate_weight,
    shared_up_weight,
    shared_down_weight,
    second_norm_gain,
    second_norm_bias,
):
    length, groups, half = recurrence_input.shape
    width = stream.shape[1]
    tp_count, sp_count = lax.axis_size("tp"), lax.axis_size("sp")
    quarter = length // tp_count
    expert_count = routed_gate_weight.shape[0] * sp_count
    slot_count = expert_count * SLOTS
    channels = groups * half
    shape, kept = jax.ShapeDtypeStruct, pltpu.VMEM

    rows = jnp.transpose(recurrence_input, (1, 0, 2))
    margin = 8
    border = lax.ppermute(rows[:, length - margin :], "sp", [(i, i + 1) for i in range(sp_count - 1)])

    gate_w, up_w, down_w = routed_gate_weight[0], routed_up_weight[0], routed_down_weight[0]
    gate_left, up_right = turned(gate_w, 1), turned(up_w, -1)
    up_left, gate_right = turned(up_w, 1), turned(gate_w, -1)

    own_index = lax.axis_index("tp")
    own_ids = lax.dynamic_slice_in_dim(routed_expert_index.T, own_index * quarter, quarter, 1)
    own_weights = lax.dynamic_slice_in_dim(routed_expert_weight.T, own_index * quarter, quarter, 1)
    fill = ((0, 0), (0, LANES - quarter))
    select, merge = kernel_call(
        route_kernel,
        [kept((slot_count, quarter), BF16), shape((quarter, slot_count), F32)],
        (jnp.pad(own_ids, fill, constant_values=-1), "vmem"),
        (jnp.pad(own_weights, fill), "vmem"),
    )

    runs = channels // LANES
    decays, states, totals = kernel_call(
        local_kernel,
        [kept((length, channels), F32), kept((length, channels), F32), shape((sp_count, 2 * runs, LANES), F32)],
        (rows, "vmem"),
        (border, "vmem"),
        convolution_taps,
        first_group_gates,
        second_group_gates,
        channel_decay,
        (jnp.transpose(position_log_extra, (1, 0, 2)), "vmem"),
        scratch=(pltpu.VMEM((margin + length, half), F32), pltpu.VMEM((half, 2 * half), BF16)),
    )
    spans = swapped(totals, "sp")
    parts = kernel_call(
        project_kernel,
        shape((tp_count, quarter, width), BF16),
        (lax.axis_index("sp").reshape(1), "smem"),
        (spans, "vmem"),
        (decays, "vmem"),
        (states, "vmem"),
        (jnp.transpose(output_gate_input, (1, 0, 2)), "vmem"),
        (recurrence_output_weight, "hbm"),
        scratch=(pltpu.VMEM(recurrence_output_weight.shape, BF16), pltpu.SemaphoreType.DMA((1,))),
    )
    parts = swapped(parts, "tp")

    down_left, down_right = turned(down_w, 1), turned(down_w, -1)
    gate_far, up_far = turned(gate_left, 1), turned(up_right, -1)

    normed, outgoing = kernel_call(
        mix_kernel,
        [kept((quarter, width), BF16), shape((expert_count, SLOTS, width), BF16)],
        (parts, "vmem"),
        stream,
        first_norm_gain.reshape(1, width),
        first_norm_bias.reshape(1, width),
        (select, "vmem"),
    )
    arrived = swapped(outgoing, "sp")

    cut = down_w.shape[0] // 2
    down_far = turned(down_left[:cut], 1), turned(down_right[cut:], -1)

    last = (merge, second_norm_gain.reshape(1, width), second_norm_bias.reshape(1, width))
    base, *last = kernel_call(
        shared_kernel,
        [kept((quarter, width), F32), *(kept(x.shape, F32) for x in last)],
        (normed, "vmem"),
        shared_gate_weight,
        shared_up_weight,
        shared_down_weight,
        *last,
    )
    weights = (gate_w, gate_left, gate_right, gate_far, up_w, up_left, up_right, up_far, down_w, down_left, down_right, *down_far)
    leaving = kernel_call(
        expert_kernel,
        kept((expert_count, SLOTS, width), BF16),
        (arrived, "vmem"),
        *((w, "hbm") for w in weights),
        scratch=(
            pltpu.VMEM((tp_count, width, 2 * gate_w.shape[1]), BF16),
            pltpu.VMEM((tp_count * down_w.shape[0], width), BF16),
            pltpu.SemaphoreType.DMA((len(weights),)),
        ),
    )
    returned = swapped(leaving, "sp")
    return kernel_call(
        merge_kernel, shape((quarter, width), BF16), (returned, "vmem"), (base, "vmem"), *((x, "vmem") for x in last)
    )


def solution(mesh):
    in_specs = (
        P(("sp", "tp"), None),
        P("sp", None, "tp"),
        P("sp", None, "tp"),
        P(None, None, "tp"),
        P(None, "tp", None, None),
        P(None, "tp", None, None),
        P(None, "tp"),
        P("sp", None, "tp"),
        P(None, "tp", None),
        P(),
        P(),
        P("sp", None),
        P("sp", None),
        P("sp", None, "tp"),
        P("sp", None, "tp"),
        P("sp", "tp", None),
        P(),
        P(),
        P(),
        P(),
        P(),
    )

    return jax.shard_map(shards, mesh=mesh, in_specs=in_specs, out_specs=P(("sp", "tp"), None), check_vma=False)
```

```python
import jax
import jax.numpy as jnp
from jax import lax
from jax.experimental import pallas as pl
from jax.experimental.pallas import tpu as pltpu
from jax.sharding import PartitionSpec as P

RESIDUAL_SCALE = 8.0**0.25
NORM_EPSILON = 1e-05
LANES = 128
SLOTS = 2
BF16, F32 = jnp.bfloat16, jnp.float32
VMEM = pl.BlockSpec(memory_space=pltpu.VMEM)
SMEM = pl.BlockSpec(memory_space=pltpu.SMEM)
ANY = pl.BlockSpec(memory_space=pl.ANY)


def kernel_call(body, out_shape, *operands, scratch=(), limit=16):
    several = isinstance(out_shape, (list, tuple))
    specs, arrays = [], []
    for operand in operands:
        array, place = operand if isinstance(operand, tuple) else (operand, None)
        specs.append({"smem": SMEM, "hbm": ANY}.get(place, VMEM))
        if place != "smem":
            array = pltpu.with_memory_space_constraint(array, pltpu.VMEM if place == "vmem" else pltpu.HBM)
        arrays.append(array)
    return pl.pallas_call(
        body,
        out_shape=out_shape,
        in_specs=specs,
        out_specs=[VMEM] * len(out_shape) if several else VMEM,
        scratch_shapes=scratch,
        compiler_params=pltpu.CompilerParams(vmem_limit_bytes=limit << 20),
    )(*arrays)


def fetched(pairs, sems):
    copies = [pltpu.make_async_copy(source, target, sems.at[k]) for k, (source, target) in enumerate(pairs)]
    for copy in copies:
        copy.start()
    return copies


def dot(a, b):
    return jnp.dot(a, b, preferred_element_type=F32)


def layer_norm(values, gain_vec, bias_vec):
    row_mean = jnp.mean(values, axis=-1, keepdims=True)
    spread = jnp.mean(jnp.square(values - row_mean), axis=-1, keepdims=True)
    return (values - row_mean) * lax.rsqrt(spread + NORM_EPSILON) * gain_vec + bias_vec


def softplus(x):
    u = jnp.exp(-jnp.abs(x))
    s = u / (2.0 + u)
    q = s * s
    series = 1.0 / 17.0
    for k in (15.0, 13.0, 11.0, 9.0, 7.0, 5.0, 3.0, 1.0):
        series = series * q + 1.0 / k
    return jnp.maximum(x, 0.0) + 2.0 * s * series


def expm1(z):
    series = 1.0 + z * (1.0 / 9.0)
    for k in (8.0, 7.0, 6.0, 5.0, 4.0, 3.0, 2.0):
        series = 1.0 + z * (1.0 / k) * series
    return jnp.where(jnp.abs(z) < 0.5, z * series, jnp.exp(z) - 1.0)


def shifted_rows(values, by, row, fill):
    if by < 8:
        return jnp.where(row >= by, pltpu.roll(values, by, 0), fill)
    head = jnp.full((by, values.shape[1]), fill, values.dtype)
    return jnp.concatenate([head, values[: values.shape[0] - by]], axis=0)


def chain_rows(decay, drive):
    row = lax.broadcasted_iota(jnp.int32, decay.shape, 0)
    by = 1
    while by < decay.shape[0]:
        drive = decay * shifted_rows(drive, by, row, 0.0) + drive
        decay = decay * shifted_rows(decay, by, row, 1.0)
        by *= 2
    return decay, drive


def flat(array):
    length, groups, half = array.shape
    return array.reshape(length, groups, half // LANES, LANES).transpose(0, 2, 1, 3).reshape(-1, LANES)


def local_kernel(rows, border, taps, small_maps, large_maps, decay_param, extra, decays, states, totals, padded, maps):
    groups, half = decay_param.shape
    per_half = half // LANES
    step = groups * per_half
    length = rows.shape[0] // step
    tap_count = taps.shape[0]
    tap_weights = taps[...].astype(F32)
    rate = -8.0 * softplus(-decay_param[...])
    margin = border.shape[0]
    padded[0:margin] = border[...].astype(F32)
    padded[margin:] = rows[...].astype(F32)
    logs, ends = [], []
    for g, blocks in enumerate((small_maps, large_maps)):
        conv_runs = []
        for c in range(per_half):
            at = slice(c * LANES, (c + 1) * LANES)
            summed = None
            for k in range(tap_count):
                start = margin - (tap_count - 1 - k) * step + c * groups + g
                term = tap_weights[k, g : g + 1, at] * padded[pl.ds(start, length, stride=step), :]
                summed = term if summed is None else summed + term
            conv_runs.append(summed.astype(BF16))
        conv_rows = jnp.concatenate(conv_runs, axis=1)
        maps[...] = jnp.zeros(maps.shape, BF16)
        head = blocks.shape[-1]
        for m in range(2):
            for h in range(blocks.shape[1]):
                maps[h * head : (h + 1) * head, m * half + h * head : m * half + (h + 1) * head] = blocks[m, h]
        gates = jax.nn.sigmoid(dot(conv_rows, maps[...]))
        for c in range(per_half):
            at = slice(c * LANES, (c + 1) * LANES)
            log_decay = gates[:, at] * rate[g : g + 1, at] + extra[pl.ds(c * groups + g, length, stride=step), :]
            gate = gates[:, half + c * LANES : half + (c + 1) * LANES]
            drive = jnp.sqrt(-expm1(2.0 * log_decay)) * gate * conv_runs[c].astype(F32)
            product, state = chain_rows(jnp.exp(log_decay), drive)
            to = slice((g * per_half + c) * LANES, (g * per_half + c + 1) * LANES)
            decays[:, to] = product
            states[:, to] = state
            logs.append(jnp.sum(log_decay, axis=0, keepdims=True))
            ends.append(state[length - 1 :])
    span = jnp.concatenate(logs + ends, axis=0).astype(BF16)
    for j in range(totals.shape[0]):
        totals[j] = span


def entering_state(spans, mine):
    half = spans.shape[1] // 2
    span = lax.broadcasted_iota(jnp.int32, (spans.shape[0], half, LANES), 0)
    logs = spans[:, :half].astype(F32)
    decays = jnp.where(span < mine, jnp.exp(logs), 1.0)
    ends = jnp.where(span < mine, spans[:, half:].astype(F32), 0.0)
    state = ends[0]
    for j in range(1, spans.shape[0] - 1):
        state = decays[j] * state + ends[j]
    return state


def project_kernel(mine, spans, decays, states, gated, weight_far, out, weight, sems):
    (copy,) = fetched([(weight_far, weight)], sems)
    entering = entering_state(spans, mine[0])
    runs = entering.shape[0]
    branches = []
    for run in range(runs):
        at = slice(run * LANES, (run + 1) * LANES)
        state = states[:, at] + decays[:, at] * entering[run : run + 1]
        branches.append((gated[:, at] * state).astype(BF16))
    copy.wait()
    acc, per_half = None, runs // weight.shape[0]
    for g in range(weight.shape[0]):
        part = dot(jnp.concatenate(branches[g * per_half : (g + 1) * per_half], axis=1), weight[g])
        acc = part if acc is None else acc + part
    out[...] = acc.astype(BF16).reshape(out.shape)


def side_kernel(ids, weights, gate_rows, stream, gain, bias, select, merge, gated, scaled, gain_kept, bias_kept, wide):
    route(ids, weights, select, merge)
    wide[...] = gate_rows[...].astype(F32)
    runs = gated.shape[1] // LANES
    groups = 2
    for run in range(runs):
        g, c = divmod(run, runs // groups)
        values = wide[pl.ds(c * groups + g, gated.shape[0], stride=runs), :]
        gated[:, run * LANES : (run + 1) * LANES] = jax.nn.gelu(values, approximate=True)
    scaled[...] = RESIDUAL_SCALE * stream[...].astype(F32)
    gain_kept[...] = gain[...]
    bias_kept[...] = bias[...]


def route(ids, weights, select, merge):
    slot_count, rows = select.shape[0], ids.shape[1]
    slot = lax.broadcasted_iota(jnp.int32, (slot_count, rows), 0)
    names = jnp.zeros((slot_count, rows), F32)
    weight = jnp.zeros((slot_count, rows), F32)
    for k in range(ids.shape[0]):
        named = ids[k : k + 1] == slot // SLOTS
        names = jnp.where(named, 1.0, names)
        weight = jnp.where(named, weights[k : k + 1], weight)
    earlier = lax.broadcasted_iota(jnp.int32, (rows, rows), 0) < lax.broadcasted_iota(jnp.int32, (rows, rows), 1)
    rank = dot(names.astype(BF16), jnp.where(earlier, 1.0, 0.0).astype(BF16))
    taken = (names > 0.0) & (rank == (slot % SLOTS).astype(F32))
    select[...] = jnp.where(taken, 1.0, 0.0).astype(BF16)[:, : select.shape[1]]
    merge[...] = jnp.where(taken, weight, 0.0).T[: merge.shape[0]]


def mix_kernel(parts, scaled, gain, bias, select, normed, outgoing):
    mixed = parts[0].astype(F32)
    for j in range(1, parts.shape[0]):
        mixed = mixed + parts[j].astype(F32)
    rows = layer_norm(scaled[...] + mixed, gain[...], bias[...]).astype(BF16)
    normed[...] = rows
    outgoing[...] = dot(select[...], rows).astype(BF16).reshape(outgoing.shape)


def shared_kernel(normed, gate_w, up_w, down_w, merge, gain, bias, base, *kept):
    for target, source in zip(kept, (merge, gain, bias)):
        target[...] = source[...]
    rows = normed[...]
    gated, lifted = dot(rows, gate_w[...]), dot(rows, up_w[...])
    hidden = (jax.nn.silu(gated) * lifted).astype(BF16)
    base[...] = RESIDUAL_SCALE * rows.astype(F32) + dot(hidden, down_w[...])


def expert_kernel(rows, gate_own, up_own, left, right, gate_far, up_far, d0, d1, d2, d3a, d3b, out, pairs, down, sems):
    depth, width = gate_own.shape
    near = [(side.at[0:depth], side.at[depth : 2 * depth]) for side in (left, right)]
    moves = []
    for j, (gate_w, up_w) in enumerate([(gate_own, up_own), *near, (gate_far, up_far)]):
        moves += [(gate_w, pairs.at[j, :, 0:width]), (up_w, pairs.at[j, :, width : 2 * width])]
    at = 0
    for piece in (d0, d1, d2, d3a, d3b):
        moves.append((piece, down.at[at : at + piece.shape[0]]))
        at += piece.shape[0]
    copies = fetched(moves, sems)
    picked = rows[...].reshape(-1, rows.shape[-1])
    hidden = []
    for j in range(pairs.shape[0]):
        copies[2 * j].wait()
        copies[2 * j + 1].wait()
        pair = dot(picked, pairs[j])
        hidden.append((jax.nn.silu(pair[:, :width]) * pair[:, width:]).astype(BF16))
    for copy in copies[2 * pairs.shape[0] :]:
        copy.wait()
    acc = dot(jnp.concatenate(hidden, axis=1), down[...])
    out[...] = acc.astype(BF16).reshape(out.shape)


def merge_kernel(returned, base, merge, gain, bias, out):
    rest = merge[...]
    rows = returned[...].reshape(-1, returned.shape[-1])
    total = base[...]
    for _ in range(3):
        part = rest.astype(BF16)
        total = total + dot(part, rows)
        rest = rest - part.astype(F32)
    out[...] = layer_norm(total, gain[...], bias[...]).astype(BF16)


def turned(shard, by):
    count = lax.axis_size("tp")
    return lax.ppermute(shard, "tp", [(i, (i + by) % count) for i in range(count)])


def swapped(pieces, axis):
    return lax.all_to_all(pieces, axis, 0, 0, tiled=True)


def shards(
    stream,
    recurrence_input,
    output_gate_input,
    convolution_taps,
    first_group_gates,
    second_group_gates,
    channel_decay,
    position_log_extra,
    recurrence_output_weight,
    first_norm_gain,
    first_norm_bias,
    routed_expert_index,
    routed_expert_weight,
    routed_gate_weight,
    routed_up_weight,
    routed_down_weight,
    shared_gate_weight,
    shared_up_weight,
    shared_down_weight,
    second_norm_gain,
    second_norm_bias,
):
    length, groups, half = recurrence_input.shape
    width = stream.shape[1]
    tp_count, sp_count = lax.axis_size("tp"), lax.axis_size("sp")
    quarter = length // tp_count
    expert_count = routed_gate_weight.shape[0] * sp_count
    slot_count = expert_count * SLOTS
    channels = groups * half
    shape, kept = jax.ShapeDtypeStruct, pltpu.VMEM

    rows = flat(recurrence_input)
    margin = 16
    border = lax.ppermute(rows[rows.shape[0] - margin :], "sp", [(i, i + 1) for i in range(sp_count - 1)])

    gate_w, up_w, down_w = routed_gate_weight[0], routed_up_weight[0], routed_down_weight[0]
    pair_w = jnp.concatenate([gate_w, up_w], axis=0)
    pair_left, pair_right = turned(pair_w, 1), turned(pair_w, -1)
    down_left, down_right = turned(down_w, 1), turned(down_w, -1)

    runs = channels // LANES
    decays, states, totals = kernel_call(
        local_kernel,
        [kept((length, channels), F32), kept((length, channels), F32), shape((sp_count, 2 * runs, LANES), BF16)],
        rows,
        (border, "vmem"),
        convolution_taps,
        first_group_gates,
        second_group_gates,
        channel_decay,
        flat(position_log_extra),
        scratch=(pltpu.VMEM((margin + rows.shape[0], LANES), F32), pltpu.VMEM((half, 2 * half), BF16)),
    )
    spans = swapped(totals, "sp")

    own_index = lax.axis_index("tp")
    own_ids = lax.dynamic_slice_in_dim(routed_expert_index.T, own_index * quarter, quarter, 1)
    own_weights = lax.dynamic_slice_in_dim(routed_expert_weight.T, own_index * quarter, quarter, 1)
    fill = ((0, 0), (0, LANES - quarter))
    select, merge, gated, *norm_parts = kernel_call(
        side_kernel,
        [
            kept((slot_count, quarter), BF16),
            shape((quarter, slot_count), F32),
            kept((length, channels), F32),
            kept((quarter, width), F32),
            kept((1, width), F32),
            kept((1, width), F32),
        ],
        (jnp.pad(own_ids, fill, constant_values=-1), "vmem"),
        (jnp.pad(own_weights, fill), "vmem"),
        flat(output_gate_input),
        stream,
        first_norm_gain.reshape(1, width),
        first_norm_bias.reshape(1, width),
        scratch=(pltpu.VMEM(rows.shape, F32),),
    )
    parts = kernel_call(
        project_kernel,
        shape((tp_count, quarter, width), BF16),
        (lax.axis_index("sp").reshape(1), "smem"),
        (spans, "vmem"),
        (decays, "vmem"),
        (states, "vmem"),
        (gated, "vmem"),
        (recurrence_output_weight, "hbm"),
        scratch=(pltpu.VMEM(recurrence_output_weight.shape, BF16), pltpu.SemaphoreType.DMA((1,))),
    )
    parts = swapped(parts, "tp")

    depth = gate_w.shape[0]
    gate_far, up_far = turned(pair_left[:depth], 1), turned(pair_right[depth:], -1)

    normed, outgoing = kernel_call(
        mix_kernel,
        [kept((quarter, width), BF16), shape((expert_count, SLOTS, width), BF16)],
        (parts, "vmem"),
        *((x, "vmem") for x in norm_parts),
        (select, "vmem"),
    )
    arrived = swapped(outgoing, "sp")

    cut = down_w.shape[0] // 2
    down_far = turned(down_left[:cut], 1), turned(down_right[cut:], -1)

    last = (merge, second_norm_gain.reshape(1, width), second_norm_bias.reshape(1, width))
    base, *last = kernel_call(
        shared_kernel,
        [kept((quarter, width), F32), *(kept(x.shape, F32) for x in last)],
        (normed, "vmem"),
        shared_gate_weight,
        shared_up_weight,
        shared_down_weight,
        *last,
    )
    weights = (gate_w, up_w, pair_left, pair_right, gate_far, up_far, down_w, down_left, down_right, *down_far)
    leaving = kernel_call(
        expert_kernel,
        kept((expert_count, SLOTS, width), BF16),
        (arrived, "vmem"),
        *((w, "hbm") for w in weights),
        scratch=(
            pltpu.VMEM((tp_count, width, 2 * gate_w.shape[1]), BF16),
            pltpu.VMEM((tp_count * down_w.shape[0], width), BF16),
            pltpu.SemaphoreType.DMA((len(weights) + 2,)),
        ),
    )
    returned = swapped(leaving, "sp")
    return kernel_call(
        merge_kernel, shape((quarter, width), BF16), (returned, "vmem"), (base, "vmem"), *((x, "vmem") for x in last)
    )


def solution(mesh):
    in_specs = (
        P(("sp", "tp"), None),
        P("sp", None, "tp"),
        P("sp", None, "tp"),
        P(None, None, "tp"),
        P(None, "tp", None, None),
        P(None, "tp", None, None),
        P(None, "tp"),
        P("sp", None, "tp"),
        P(None, "tp", None),
        P(),
        P(),
        P("sp", None),
        P("sp", None),
        P("sp", None, "tp"),
        P("sp", None, "tp"),
        P("sp", "tp", None),
        P(),
        P(),
        P(),
        P(),
        P(),
    )

    return jax.shard_map(shards, mesh=mesh, in_specs=in_specs, out_specs=P(("sp", "tp"), None), check_vma=False)
```

```python
import jax
import jax.numpy as jnp
from jax import lax
from jax.experimental import pallas as pl
from jax.experimental.pallas import tpu as pltpu
from jax.sharding import PartitionSpec as P

RESIDUAL_SCALE = 8.0**0.25
NORM_EPSILON = 1e-05
LANES = 128
SLOTS = 2
BF16, F32 = jnp.bfloat16, jnp.float32
VMEM = pl.BlockSpec(memory_space=pltpu.VMEM)
SMEM = pl.BlockSpec(memory_space=pltpu.SMEM)
ANY = pl.BlockSpec(memory_space=pl.ANY)


def kernel_call(body, out_shape, *operands, scratch=(), limit=16):
    several = isinstance(out_shape, (list, tuple))
    specs, arrays = [], []
    for operand in operands:
        array, place = operand if isinstance(operand, tuple) else (operand, None)
        specs.append({"smem": SMEM, "hbm": ANY}.get(place, VMEM))
        if place != "smem":
            array = pltpu.with_memory_space_constraint(array, pltpu.VMEM if place == "vmem" else pltpu.HBM)
        arrays.append(array)
    return pl.pallas_call(
        body,
        out_shape=out_shape,
        in_specs=specs,
        out_specs=[VMEM] * len(out_shape) if several else VMEM,
        scratch_shapes=scratch,
        compiler_params=pltpu.CompilerParams(vmem_limit_bytes=limit << 20),
    )(*arrays)


def fetched(pairs, sems):
    copies = [pltpu.make_async_copy(source, target, sems.at[k]) for k, (source, target) in enumerate(pairs)]
    for copy in copies:
        copy.start()
    return copies


def dot(a, b):
    return jnp.dot(a, b, preferred_element_type=F32)


def layer_norm(values, gain_vec, bias_vec):
    row_mean = jnp.mean(values, axis=-1, keepdims=True)
    spread = jnp.mean(jnp.square(values - row_mean), axis=-1, keepdims=True)
    return (values - row_mean) * lax.rsqrt(spread + NORM_EPSILON) * gain_vec + bias_vec


def softplus(x):
    u = jnp.exp(-jnp.abs(x))
    s = u / (2.0 + u)
    q = s * s
    series = 1.0 / 17.0
    for k in (15.0, 13.0, 11.0, 9.0, 7.0, 5.0, 3.0, 1.0):
        series = series * q + 1.0 / k
    return jnp.maximum(x, 0.0) + 2.0 * s * series


def expm1(z):
    series = 1.0 + z * (1.0 / 9.0)
    for k in (8.0, 7.0, 6.0, 5.0, 4.0, 3.0, 2.0):
        series = 1.0 + z * (1.0 / k) * series
    return jnp.where(jnp.abs(z) < 0.5, z * series, jnp.exp(z) - 1.0)


def shifted_rows(values, by, row, fill):
    if by < 8:
        return jnp.where(row >= by, pltpu.roll(values, by, 0), fill)
    head = jnp.full((by, values.shape[1]), fill, values.dtype)
    return jnp.concatenate([head, values[: values.shape[0] - by]], axis=0)


def chain_rows(decay, drive):
    row = lax.broadcasted_iota(jnp.int32, decay.shape, 0)
    by = 1
    while by < decay.shape[0]:
        drive = decay * shifted_rows(drive, by, row, 0.0) + drive
        decay = decay * shifted_rows(decay, by, row, 1.0)
        by *= 2
    return decay, drive


def flat(array):
    length, groups, half = array.shape
    return array.reshape(length, groups, half // LANES, LANES).transpose(0, 2, 1, 3).reshape(-1, LANES)


def local_kernel(rows, border, taps, small_maps, large_maps, decay_param, extra, decays, states, totals, padded, maps):
    groups, half = decay_param.shape
    per_half = half // LANES
    step = groups * per_half
    length = rows.shape[0] // step
    tap_count = taps.shape[0]
    tap_weights = taps[...].astype(F32)
    rate = -8.0 * softplus(-decay_param[...])
    margin = border.shape[0]
    padded[0:margin] = border[...].astype(F32)
    padded[margin:] = rows[...].astype(F32)
    logs, ends = [], []
    for g, blocks in enumerate((small_maps, large_maps)):
        conv_runs = []
        for c in range(per_half):
            at = slice(c * LANES, (c + 1) * LANES)
            summed = None
            for k in range(tap_count):
                start = margin - (tap_count - 1 - k) * step + c * groups + g
                term = tap_weights[k, g : g + 1, at] * padded[pl.ds(start, length, stride=step), :]
                summed = term if summed is None else summed + term
            conv_runs.append(summed.astype(BF16))
        conv_rows = jnp.concatenate(conv_runs, axis=1)
        maps[...] = jnp.zeros(maps.shape, BF16)
        head = blocks.shape[-1]
        for m in range(2):
            for h in range(blocks.shape[1]):
                maps[h * head : (h + 1) * head, m * half + h * head : m * half + (h + 1) * head] = blocks[m, h]
        gates = jax.nn.sigmoid(dot(conv_rows, maps[...]))
        for c in range(per_half):
            at = slice(c * LANES, (c + 1) * LANES)
            log_decay = gates[:, at] * rate[g : g + 1, at] + extra[pl.ds(c * groups + g, length, stride=step), :]
            gate = gates[:, half + c * LANES : half + (c + 1) * LANES]
            drive = jnp.sqrt(-expm1(2.0 * log_decay)) * gate * conv_runs[c].astype(F32)
            product, state = chain_rows(jnp.exp(log_decay), drive)
            to = slice((g * per_half + c) * LANES, (g * per_half + c + 1) * LANES)
            decays[:, to] = product
            states[:, to] = state
            logs.append(jnp.sum(log_decay, axis=0, keepdims=True))
            ends.append(state[length - 1 :])
    span = jnp.concatenate(logs + ends, axis=0).astype(BF16)
    for j in range(totals.shape[0]):
        totals[j] = span


def entering_state(spans, ahead):
    half = spans.shape[1] // 2
    passed = (ahead[...] > 0.0)[:, None, :]
    decays = jnp.where(passed, jnp.exp(spans[:, :half].astype(F32)), 1.0)
    ends = jnp.where(passed, spans[:, half:].astype(F32), 0.0)
    state = ends[0]
    for j in range(1, spans.shape[0] - 1):
        state = decays[j] * state + ends[j]
    return state


def project_kernel(spans, ahead, decays, states, weight, out):
    entering = entering_state(spans, ahead)
    runs = entering.shape[0]
    branches = []
    for run in range(runs):
        at = slice(run * LANES, (run + 1) * LANES)
        branches.append((states[:, at] + decays[:, at] * entering[run : run + 1]).astype(BF16))
    acc, per_half = None, runs // weight.shape[0]
    for g in range(weight.shape[0]):
        part = dot(jnp.concatenate(branches[g * per_half : (g + 1) * per_half], axis=1), weight[g])
        acc = part if acc is None else acc + part
    out[...] = acc.astype(BF16).reshape(out.shape)


def side_kernel(mine, ids, weights, decays, states, gate_rows, stream, gain, bias, projection, *rest):
    select, merge, gated_decays, gated_states, stream_kept, gain_kept, bias_kept, projection_kept, ahead, wide, sems = rest
    (copy,) = fetched([(projection, projection_kept)], sems)
    ahead[...] = jnp.where(lax.broadcasted_iota(jnp.int32, ahead.shape, 0) < mine[0], 1.0, 0.0)
    route(ids, weights, select, merge)
    wide[...] = gate_rows[...].astype(F32)
    length, runs = decays.shape[0], decays.shape[1] // LANES
    groups = 2
    for run in range(runs):
        g, c = divmod(run, runs // groups)
        values = jax.nn.gelu(wide[pl.ds(c * groups + g, length, stride=runs), :], approximate=True)
        at = slice(run * LANES, (run + 1) * LANES)
        gated_decays[:, at] = values * decays[:, at]
        gated_states[:, at] = values * states[:, at]
    stream_kept[...] = stream[...]
    gain_kept[...] = gain[...]
    bias_kept[...] = bias[...]
    copy.wait()


def route(ids, weights, select, merge):
    slot_count, rows = select.shape[0], ids.shape[1]
    slot = lax.broadcasted_iota(jnp.int32, (slot_count, rows), 0)
    names = jnp.zeros((slot_count, rows), F32)
    weight = jnp.zeros((slot_count, rows), F32)
    for k in range(ids.shape[0]):
        named = ids[k : k + 1] == slot // SLOTS
        names = jnp.where(named, 1.0, names)
        weight = jnp.where(named, weights[k : k + 1], weight)
    earlier = lax.broadcasted_iota(jnp.int32, (rows, rows), 0) < lax.broadcasted_iota(jnp.int32, (rows, rows), 1)
    rank = dot(names.astype(BF16), jnp.where(earlier, 1.0, 0.0).astype(BF16))
    taken = (names > 0.0) & (rank == (slot % SLOTS).astype(F32))
    select[...] = jnp.where(taken, 1.0, 0.0).astype(BF16)[:, : select.shape[1]]
    merge[...] = jnp.where(taken, weight, 0.0).T[: merge.shape[0]]


def mix_kernel(parts, stream, gain, bias, select, normed, outgoing):
    mixed = parts[0].astype(F32)
    for j in range(1, parts.shape[0]):
        mixed = mixed + parts[j].astype(F32)
    rows = layer_norm(RESIDUAL_SCALE * stream[...].astype(F32) + mixed, gain[...], bias[...]).astype(BF16)
    normed[...] = rows
    outgoing[...] = dot(select[...], rows).astype(BF16).reshape(outgoing.shape)


def pair_moves(pairs, weights):
    moves = []
    for j, (gate_w, up_w) in enumerate(weights):
        width = gate_w.shape[1]
        moves += [(gate_w, pairs.at[j, :, 0:width]), (up_w, pairs.at[j, :, width : 2 * width])]
    return moves


def shared_kernel(normed, gate_w, up_w, down_w, merge, gain, bias, g0, u0, g1, u1, base, *rest):
    *kept, near, sems = rest
    copies = fetched(pair_moves(near, ((g0, u0), (g1, u1))), sems)
    for target, source in zip(kept, (merge, gain, bias)):
        target[...] = source[...]
    rows = normed[...]
    gated, lifted = dot(rows, gate_w[...]), dot(rows, up_w[...])
    hidden = (jax.nn.silu(gated) * lifted).astype(BF16)
    base[...] = RESIDUAL_SCALE * rows.astype(F32) + dot(hidden, down_w[...])
    for copy in copies:
        copy.wait()


def expert_kernel(rows, near, g2, u2, g3, u3, d0, d1, d2, d3a, d3b, out, far, down, sems):
    moves = pair_moves(far, ((g2, u2), (g3, u3)))
    at = 0
    for piece in (d0, d1, d2, d3a, d3b):
        moves.append((piece, down.at[at : at + piece.shape[0]]))
        at += piece.shape[0]
    copies = fetched(moves, sems)
    picked = rows[...].reshape(-1, rows.shape[-1])

    def hidden_of(both):
        pair = dot(picked, both)
        width = pair.shape[1] // 2
        return (jax.nn.silu(pair[:, :width]) * pair[:, width:]).astype(BF16)

    hidden = [hidden_of(near[j]) for j in range(near.shape[0])]
    for j in range(far.shape[0]):
        copies[2 * j].wait()
        copies[2 * j + 1].wait()
        hidden.append(hidden_of(far[j]))
    for copy in copies[2 * far.shape[0] :]:
        copy.wait()
    acc = dot(jnp.concatenate(hidden, axis=1), down[...])
    out[...] = acc.astype(BF16).reshape(out.shape)


def merge_kernel(returned, base, merge, gain, bias, out):
    rest = merge[...]
    rows = returned[...].reshape(-1, returned.shape[-1])
    total = base[...]
    for _ in range(3):
        part = rest.astype(BF16)
        total = total + dot(part, rows)
        rest = rest - part.astype(F32)
    out[...] = layer_norm(total, gain[...], bias[...]).astype(BF16)


def turned(shard, by):
    count = lax.axis_size("tp")
    return lax.ppermute(shard, "tp", [(i, (i + by) % count) for i in range(count)])


def swapped(pieces, axis):
    return lax.all_to_all(pieces, axis, 0, 0, tiled=True)


def shards(
    stream,
    recurrence_input,
    output_gate_input,
    convolution_taps,
    first_group_gates,
    second_group_gates,
    channel_decay,
    position_log_extra,
    recurrence_output_weight,
    first_norm_gain,
    first_norm_bias,
    routed_expert_index,
    routed_expert_weight,
    routed_gate_weight,
    routed_up_weight,
    routed_down_weight,
    shared_gate_weight,
    shared_up_weight,
    shared_down_weight,
    second_norm_gain,
    second_norm_bias,
):
    length, groups, half = recurrence_input.shape
    width = stream.shape[1]
    tp_count, sp_count = lax.axis_size("tp"), lax.axis_size("sp")
    quarter = length // tp_count
    expert_count = routed_gate_weight.shape[0] * sp_count
    slot_count = expert_count * SLOTS
    channels = groups * half
    shape, kept = jax.ShapeDtypeStruct, pltpu.VMEM

    rows = flat(recurrence_input)
    margin = 16
    border = lax.ppermute(rows[rows.shape[0] - margin :], "sp", [(i, i + 1) for i in range(sp_count - 1)])

    gate_w, up_w, down_w = routed_gate_weight[0], routed_up_weight[0], routed_down_weight[0]
    gate_left, up_right = turned(gate_w, 1), turned(up_w, -1)
    up_left, gate_right = turned(up_w, 1), turned(gate_w, -1)
    down_left, down_right = turned(down_w, 1), turned(down_w, -1)

    runs = channels // LANES
    decays, states, totals = kernel_call(
        local_kernel,
        [kept((length, channels), F32), kept((length, channels), F32), shape((sp_count, 2 * runs, LANES), BF16)],
        rows,
        (border, "vmem"),
        convolution_taps,
        first_group_gates,
        second_group_gates,
        channel_decay,
        flat(position_log_extra),
        scratch=(pltpu.VMEM((margin + rows.shape[0], LANES), F32), pltpu.VMEM((half, 2 * half), BF16)),
    )
    spans = swapped(totals, "sp")

    own_index = lax.axis_index("tp")
    own_ids = lax.dynamic_slice_in_dim(routed_expert_index.T, own_index * quarter, quarter, 1)
    own_weights = lax.dynamic_slice_in_dim(routed_expert_weight.T, own_index * quarter, quarter, 1)
    fill = ((0, 0), (0, LANES - quarter))
    select, merge, decays, states, *norm_parts, projection, ahead = kernel_call(
        side_kernel,
        [
            kept((slot_count, quarter), BF16),
            shape((quarter, slot_count), F32),
            kept((length, channels), F32),
            kept((length, channels), F32),
            kept((quarter, width), BF16),
            kept((1, width), F32),
            kept((1, width), F32),
            kept(recurrence_output_weight.shape, BF16),
            kept((sp_count, LANES), F32),
        ],
        (lax.axis_index("sp").reshape(1), "smem"),
        (jnp.pad(own_ids, fill, constant_values=-1), "vmem"),
        (jnp.pad(own_weights, fill), "vmem"),
        (decays, "vmem"),
        (states, "vmem"),
        flat(output_gate_input),
        stream,
        first_norm_gain.reshape(1, width),
        first_norm_bias.reshape(1, width),
        (recurrence_output_weight, "hbm"),
        scratch=(pltpu.VMEM(rows.shape, F32), pltpu.SemaphoreType.DMA((1,))),
    )
    parts = kernel_call(
        project_kernel,
        shape((tp_count, quarter, width), BF16),
        *((x, "vmem") for x in (spans, ahead, decays, states, projection)),
    )
    parts = swapped(parts, "tp")

    gate_far, up_far = turned(gate_left, 1), turned(up_right, -1)

    normed, outgoing = kernel_call(
        mix_kernel,
        [kept((quarter, width), BF16), shape((expert_count, SLOTS, width), BF16)],
        (parts, "vmem"),
        *((x, "vmem") for x in norm_parts),
        (select, "vmem"),
    )
    arrived = swapped(outgoing, "sp")

    cut = down_w.shape[0] // 2
    down_far = turned(down_left[:cut], 1), turned(down_right[cut:], -1)

    last = (merge, second_norm_gain.reshape(1, width), second_norm_bias.reshape(1, width))
    near_weights = (gate_w, up_w, gate_left, up_left)
    unit = gate_w.shape[1]
    base, *last, near = kernel_call(
        shared_kernel,
        [
            kept((quarter, width), F32),
            *(kept(x.shape, F32) for x in last),
            kept((len(near_weights) // 2, width, 2 * unit), BF16),
        ],
        (normed, "vmem"),
        shared_gate_weight,
        shared_up_weight,
        shared_down_weight,
        *last,
        *((w, "hbm") for w in near_weights),
        scratch=(pltpu.SemaphoreType.DMA((len(near_weights),)),),
    )
    weights = (gate_right, up_right, gate_far, up_far, down_w, down_left, down_right, *down_far)
    leaving = kernel_call(
        expert_kernel,
        kept((expert_count, SLOTS, width), BF16),
        (arrived, "vmem"),
        (near, "vmem"),
        *((w, "hbm") for w in weights),
        scratch=(
            pltpu.VMEM((2, width, 2 * unit), BF16),
            pltpu.VMEM((tp_count * unit, width), BF16),
            pltpu.SemaphoreType.DMA((len(weights),)),
        ),
    )
    returned = swapped(leaving, "sp")
    return kernel_call(
        merge_kernel, shape((quarter, width), BF16), (returned, "vmem"), (base, "vmem"), *((x, "vmem") for x in last)
    )


def solution(mesh):
    in_specs = (
        P(("sp", "tp"), None),
        P("sp", None, "tp"),
        P("sp", None, "tp"),
        P(None, None, "tp"),
        P(None, "tp", None, None),
        P(None, "tp", None, None),
        P(None, "tp"),
        P("sp", None, "tp"),
        P(None, "tp", None),
        P(),
        P(),
        P("sp", None),
        P("sp", None),
        P("sp", None, "tp"),
        P("sp", None, "tp"),
        P("sp", "tp", None),
        P(),
        P(),
        P(),
        P(),
        P(),
    )

    return jax.shard_map(shards, mesh=mesh, in_specs=in_specs, out_specs=P(("sp", "tp"), None), check_vma=False)
```

```python
import jax
import jax.numpy as jnp
from jax import lax
from jax.experimental import pallas as pl
from jax.experimental.pallas import tpu as pltpu
from jax.sharding import PartitionSpec as P

RESIDUAL_SCALE = 8.0**0.25
NORM_EPSILON = 1e-05
LANES = 128
SLOTS = 2
BF16, F32 = jnp.bfloat16, jnp.float32
VMEM = pl.BlockSpec(memory_space=pltpu.VMEM)
SMEM = pl.BlockSpec(memory_space=pltpu.SMEM)
ANY = pl.BlockSpec(memory_space=pl.ANY)


def kernel_call(body, out_shape, *operands, scratch=(), limit=16):
    several = isinstance(out_shape, (list, tuple))
    specs, arrays = [], []
    for operand in operands:
        array, place = operand if isinstance(operand, tuple) else (operand, None)
        specs.append({"smem": SMEM, "hbm": ANY}.get(place, VMEM))
        if place != "smem":
            array = pltpu.with_memory_space_constraint(array, pltpu.VMEM if place == "vmem" else pltpu.HBM)
        arrays.append(array)
    return pl.pallas_call(
        body,
        out_shape=out_shape,
        in_specs=specs,
        out_specs=[VMEM] * len(out_shape) if several else VMEM,
        scratch_shapes=scratch,
        compiler_params=pltpu.CompilerParams(vmem_limit_bytes=limit << 20),
    )(*arrays)


def fetched(pairs, sems):
    copies = [pltpu.make_async_copy(source, target, sems.at[k]) for k, (source, target) in enumerate(pairs)]
    for copy in copies:
        copy.start()
    return copies


def dot(a, b):
    return jnp.dot(a, b, preferred_element_type=F32)


def layer_norm(values, gain_vec, bias_vec):
    row_mean = jnp.mean(values, axis=-1, keepdims=True)
    spread = jnp.mean(jnp.square(values - row_mean), axis=-1, keepdims=True)
    return (values - row_mean) * lax.rsqrt(spread + NORM_EPSILON) * gain_vec + bias_vec


def softplus(x):
    u = jnp.exp(-jnp.abs(x))
    s = u / (2.0 + u)
    q = s * s
    series = 1.0 / 17.0
    for k in (15.0, 13.0, 11.0, 9.0, 7.0, 5.0, 3.0, 1.0):
        series = series * q + 1.0 / k
    return jnp.maximum(x, 0.0) + 2.0 * s * series


def expm1(z):
    series = 1.0 + z * (1.0 / 9.0)
    for k in (8.0, 7.0, 6.0, 5.0, 4.0, 3.0, 2.0):
        series = 1.0 + z * (1.0 / k) * series
    return jnp.where(jnp.abs(z) < 0.5, z * series, jnp.exp(z) - 1.0)


def shifted_rows(values, by, row, fill):
    if by < 8:
        return jnp.where(row >= by, pltpu.roll(values, by, 0), fill)
    head = jnp.full((by, values.shape[1]), fill, values.dtype)
    return jnp.concatenate([head, values[: values.shape[0] - by]], axis=0)


def chain_rows(decay, drive):
    row = lax.broadcasted_iota(jnp.int32, decay.shape, 0)
    by = 1
    while by < decay.shape[0]:
        drive = decay * shifted_rows(drive, by, row, 0.0) + drive
        decay = decay * shifted_rows(decay, by, row, 1.0)
        by *= 2
    return decay, drive


def flat(array):
    length, groups, half = array.shape
    return array.reshape(length, groups, half // LANES, LANES).transpose(0, 2, 1, 3).reshape(-1, LANES)


def local_kernel(rows, border, taps, small_maps, large_maps, decay_param, extra, decays, states, totals, padded, maps):
    groups, half = decay_param.shape
    per_half = half // LANES
    step = groups * per_half
    length = rows.shape[0] // step
    tap_count = taps.shape[0]
    tap_weights = taps[...].astype(F32)
    rate = -8.0 * softplus(-decay_param[...])
    margin = border.shape[0]
    padded[0:margin] = border[...].astype(F32)
    padded[margin:] = rows[...].astype(F32)
    logs, ends = [], []
    for g, blocks in enumerate((small_maps, large_maps)):
        conv_runs = []
        for c in range(per_half):
            at = slice(c * LANES, (c + 1) * LANES)
            summed = None
            for k in range(tap_count):
                start = margin - (tap_count - 1 - k) * step + c * groups + g
                term = tap_weights[k, g : g + 1, at] * padded[pl.ds(start, length, stride=step), :]
                summed = term if summed is None else summed + term
            conv_runs.append(summed.astype(BF16))
        conv_rows = jnp.concatenate(conv_runs, axis=1)
        maps[...] = jnp.zeros(maps.shape, BF16)
        head = blocks.shape[-1]
        for m in range(2):
            for h in range(blocks.shape[1]):
                maps[h * head : (h + 1) * head, m * half + h * head : m * half + (h + 1) * head] = blocks[m, h]
        gates = jax.nn.sigmoid(dot(conv_rows, maps[...]))
        for c in range(per_half):
            at = slice(c * LANES, (c + 1) * LANES)
            log_decay = gates[:, at] * rate[g : g + 1, at] + extra[pl.ds(c * groups + g, length, stride=step), :]
            gate = gates[:, half + c * LANES : half + (c + 1) * LANES]
            drive = jnp.sqrt(-expm1(2.0 * log_decay)) * gate * conv_runs[c].astype(F32)
            product, state = chain_rows(jnp.exp(log_decay), drive)
            to = slice((g * per_half + c) * LANES, (g * per_half + c + 1) * LANES)
            decays[:, to] = product
            states[:, to] = state
            logs.append(jnp.sum(log_decay, axis=0, keepdims=True))
            ends.append(state[length - 1 :])
    span = jnp.concatenate(logs + ends, axis=0).astype(BF16)
    for j in range(totals.shape[0]):
        totals[j] = span


def entering_state(spans, ahead):
    half = spans.shape[1] // 2
    passed = (ahead[...] > 0.0)[:, None, :]
    decays = jnp.where(passed, jnp.exp(spans[:, :half].astype(F32)), 1.0)
    ends = jnp.where(passed, spans[:, half:].astype(F32), 0.0)
    state = ends[0]
    for j in range(1, spans.shape[0] - 1):
        state = decays[j] * state + ends[j]
    return state


def project_kernel(spans, ahead, decays, states, weight, out):
    entering = entering_state(spans, ahead)
    runs = entering.shape[0]
    branches = []
    for run in range(runs):
        at = slice(run * LANES, (run + 1) * LANES)
        branches.append((states[:, at] + decays[:, at] * entering[run : run + 1]).astype(BF16))
    acc, per_half = None, runs // weight.shape[0]
    for g in range(weight.shape[0]):
        part = dot(jnp.concatenate(branches[g * per_half : (g + 1) * per_half], axis=1), weight[g])
        acc = part if acc is None else acc + part
    out[...] = acc.astype(BF16).reshape(out.shape)


def side_kernel(mine, part, ids, weights, decays, states, gate_rows, stream, gain, bias, projection, *rest):
    select, merge, gated_decays, gated_states, stream_kept, gain_kept, bias_kept, projection_kept, ahead, wide, sems = rest
    (copy,) = fetched([(projection, projection_kept)], sems)
    ahead[...] = jnp.where(lax.broadcasted_iota(jnp.int32, ahead.shape, 0) < mine[0], 1.0, 0.0)
    route(ids, weights, select, merge, part[0])
    wide[...] = gate_rows[...].astype(F32)
    length, runs = decays.shape[0], decays.shape[1] // LANES
    groups = 2
    for run in range(runs):
        g, c = divmod(run, runs // groups)
        values = jax.nn.gelu(wide[pl.ds(c * groups + g, length, stride=runs), :], approximate=True)
        at = slice(run * LANES, (run + 1) * LANES)
        gated_decays[:, at] = values * decays[:, at]
        gated_states[:, at] = values * states[:, at]
    stream_kept[...] = stream[...]
    gain_kept[...] = gain[...]
    bias_kept[...] = bias[...]
    copy.wait()


def route(ids, weights, select, merge, part):
    slot_count, rows = select.shape[0], ids.shape[1]
    kept_rows = select.shape[1]
    turn = (rows - part * kept_rows) % rows
    own = lax.broadcasted_iota(jnp.int32, ids.shape, 1) < kept_rows
    ids = jnp.where(own, pltpu.roll(ids[...], turn, 1), -1)
    weights = pltpu.roll(weights[...], turn, 1)
    slot = lax.broadcasted_iota(jnp.int32, (slot_count, rows), 0)
    names = jnp.zeros((slot_count, rows), F32)
    weight = jnp.zeros((slot_count, rows), F32)
    for k in range(ids.shape[0]):
        named = ids[k : k + 1] == slot // SLOTS
        names = jnp.where(named, 1.0, names)
        weight = jnp.where(named, weights[k : k + 1], weight)
    earlier = lax.broadcasted_iota(jnp.int32, (rows, rows), 0) < lax.broadcasted_iota(jnp.int32, (rows, rows), 1)
    rank = dot(names.astype(BF16), jnp.where(earlier, 1.0, 0.0).astype(BF16))
    taken = (names > 0.0) & (rank == (slot % SLOTS).astype(F32))
    select[...] = jnp.where(taken, 1.0, 0.0).astype(BF16)[:, : select.shape[1]]
    merge[...] = jnp.where(taken, weight, 0.0).T[: merge.shape[0]]


def mix_kernel(parts, stream, gain, bias, select, normed, outgoing):
    mixed = parts[0].astype(F32)
    for j in range(1, parts.shape[0]):
        mixed = mixed + parts[j].astype(F32)
    rows = layer_norm(RESIDUAL_SCALE * stream[...].astype(F32) + mixed, gain[...], bias[...]).astype(BF16)
    normed[...] = rows
    outgoing[...] = dot(select[...], rows).astype(BF16).reshape(outgoing.shape)


def pair_moves(pairs, weights):
    moves = []
    for j, (gate_w, up_w) in enumerate(weights):
        width = gate_w.shape[1]
        moves += [(gate_w, pairs.at[j, :, 0:width]), (up_w, pairs.at[j, :, width : 2 * width])]
    return moves


def shared_kernel(normed, gate_w, up_w, down_w, merge, gain, bias, g0, u0, g1, u1, base, *rest):
    *kept, near, sems = rest
    copies = fetched(pair_moves(near, ((g0, u0), (g1, u1))), sems)
    for target, source in zip(kept, (merge, gain, bias)):
        target[...] = source[...]
    rows = normed[...]
    gated, lifted = dot(rows, gate_w[...]), dot(rows, up_w[...])
    hidden = (jax.nn.silu(gated) * lifted).astype(BF16)
    base[...] = RESIDUAL_SCALE * rows.astype(F32) + dot(hidden, down_w[...])
    for copy in copies:
        copy.wait()


def expert_kernel(rows, near, g2, u2, g3, u3, d0, d1, d2, acc, last, far, down, sems):
    moves = pair_moves(far, ((g2, u2), (g3, u3)))
    unit = d0.shape[0]
    moves += [(piece, down.at[j * unit : (j + 1) * unit]) for j, piece in enumerate((d0, d1, d2))]
    copies = fetched(moves, sems)
    picked = rows[...].reshape(-1, rows.shape[-1])

    def hidden_of(both):
        pair = dot(picked, both)
        return (jax.nn.silu(pair[:, :unit]) * pair[:, unit:]).astype(BF16)

    hidden = [hidden_of(near[j]) for j in range(near.shape[0])]
    for j in range(far.shape[0]):
        copies[2 * j].wait()
        copies[2 * j + 1].wait()
        hidden.append(hidden_of(far[j]))
    last[...] = hidden.pop()
    for copy in copies[2 * far.shape[0] :]:
        copy.wait()
    acc[...] = dot(jnp.concatenate(hidden, axis=1), down[...])


def last_kernel(acc, hidden, d3a, d3b, out):
    total = acc[...] + dot(hidden[...], jnp.concatenate([d3a[...], d3b[...]], axis=0))
    out[...] = total.astype(BF16).reshape(out.shape)


def merge_kernel(returned, base, merge, gain, bias, out):
    rest = merge[...]
    rows = returned[...].reshape(-1, returned.shape[-1])
    total = base[...]
    for _ in range(3):
        part = rest.astype(BF16)
        total = total + dot(part, rows)
        rest = rest - part.astype(F32)
    out[...] = layer_norm(total, gain[...], bias[...]).astype(BF16)


def turned(shard, by):
    count = lax.axis_size("tp")
    return lax.ppermute(shard, "tp", [(i, (i + by) % count) for i in range(count)])


def swapped(pieces, axis):
    return lax.all_to_all(pieces, axis, 0, 0, tiled=True)


def shards(
    stream,
    recurrence_input,
    output_gate_input,
    convolution_taps,
    first_group_gates,
    second_group_gates,
    channel_decay,
    position_log_extra,
    recurrence_output_weight,
    first_norm_gain,
    first_norm_bias,
    routed_expert_index,
    routed_expert_weight,
    routed_gate_weight,
    routed_up_weight,
    routed_down_weight,
    shared_gate_weight,
    shared_up_weight,
    shared_down_weight,
    second_norm_gain,
    second_norm_bias,
):
    length, groups, half = recurrence_input.shape
    width = stream.shape[1]
    tp_count, sp_count = lax.axis_size("tp"), lax.axis_size("sp")
    quarter = length // tp_count
    expert_count = routed_gate_weight.shape[0] * sp_count
    slot_count = expert_count * SLOTS
    channels = groups * half
    shape, kept = jax.ShapeDtypeStruct, pltpu.VMEM

    rows = flat(recurrence_input)
    margin = 16
    border = lax.ppermute(rows[rows.shape[0] - margin :], "sp", [(i, i + 1) for i in range(sp_count - 1)])

    gate_w, up_w, down_w = routed_gate_weight[0], routed_up_weight[0], routed_down_weight[0]
    gate_left, up_right = turned(gate_w, 1), turned(up_w, -1)
    up_left, gate_right = turned(up_w, 1), turned(gate_w, -1)
    down_left, down_right = turned(down_w, 1), turned(down_w, -1)

    runs = channels // LANES
    decays, states, totals = kernel_call(
        local_kernel,
        [kept((length, channels), F32), kept((length, channels), F32), shape((sp_count, 2 * runs, LANES), BF16)],
        rows,
        (border, "vmem"),
        convolution_taps,
        first_group_gates,
        second_group_gates,
        channel_decay,
        flat(position_log_extra),
        scratch=(pltpu.VMEM((margin + rows.shape[0], LANES), F32), pltpu.VMEM((half, 2 * half), BF16)),
    )
    spans = swapped(totals, "sp")

    select, merge, decays, states, *norm_parts, projection, ahead = kernel_call(
        side_kernel,
        [
            kept((slot_count, quarter), BF16),
            kept((quarter, slot_count), F32),
            kept((length, channels), F32),
            kept((length, channels), F32),
            kept((quarter, width), BF16),
            kept((1, width), F32),
            kept((1, width), F32),
            kept(recurrence_output_weight.shape, BF16),
            kept((sp_count, LANES), F32),
        ],
        (lax.axis_index("sp").reshape(1), "smem"),
        (lax.axis_index("tp").reshape(1), "smem"),
        routed_expert_index.T,
        routed_expert_weight.T,
        (decays, "vmem"),
        (states, "vmem"),
        flat(output_gate_input),
        stream,
        first_norm_gain.reshape(1, width),
        first_norm_bias.reshape(1, width),
        (recurrence_output_weight, "hbm"),
        scratch=(pltpu.VMEM(rows.shape, F32), pltpu.SemaphoreType.DMA((1,))),
    )
    parts = kernel_call(
        project_kernel,
        shape((tp_count, quarter, width), BF16),
        *((x, "vmem") for x in (spans, ahead, decays, states, projection)),
    )
    parts = swapped(parts, "tp")

    gate_far, up_far = turned(gate_left, 1), turned(up_right, -1)

    normed, outgoing = kernel_call(
        mix_kernel,
        [kept((quarter, width), BF16), shape((expert_count, SLOTS, width), BF16)],
        (parts, "vmem"),
        *((x, "vmem") for x in norm_parts),
        (select, "vmem"),
    )
    arrived = swapped(outgoing, "sp")

    cut = down_w.shape[0] // 2
    down_far = turned(down_left[:cut], 1), turned(down_right[cut:], -1)

    last = (merge, second_norm_gain.reshape(1, width), second_norm_bias.reshape(1, width))
    near_weights = (gate_w, up_w, gate_left, up_left)
    unit = gate_w.shape[1]
    base, *last, near = kernel_call(
        shared_kernel,
        [
            kept((quarter, width), F32),
            *(kept(x.shape, F32) for x in last),
            kept((len(near_weights) // 2, width, 2 * unit), BF16),
        ],
        (normed, "vmem"),
        shared_gate_weight,
        shared_up_weight,
        shared_down_weight,
        (last[0], "vmem"),
        *last[1:],
        *((w, "hbm") for w in near_weights),
        scratch=(pltpu.SemaphoreType.DMA((len(near_weights),)),),
    )
    weights = (gate_right, up_right, gate_far, up_far, down_w, down_left, down_right)
    acc, hidden = kernel_call(
        expert_kernel,
        [kept((slot_count, width), F32), kept((slot_count, unit), BF16)],
        (arrived, "vmem"),
        (near, "vmem"),
        *((w, "hbm") for w in weights),
        scratch=(
            pltpu.VMEM((2, width, 2 * unit), BF16),
            pltpu.VMEM((3 * unit, width), BF16),
            pltpu.SemaphoreType.DMA((len(weights),)),
        ),
    )
    leaving = kernel_call(
        last_kernel, kept((expert_count, SLOTS, width), BF16), (acc, "vmem"), (hidden, "vmem"), *down_far
    )
    returned = swapped(leaving, "sp")
    return kernel_call(
        merge_kernel, shape((quarter, width), BF16), (returned, "vmem"), (base, "vmem"), *((x, "vmem") for x in last)
    )


def solution(mesh):
    in_specs = (
        P(("sp", "tp"), None),
        P("sp", None, "tp"),
        P("sp", None, "tp"),
        P(None, None, "tp"),
        P(None, "tp", None, None),
        P(None, "tp", None, None),
        P(None, "tp"),
        P("sp", None, "tp"),
        P(None, "tp", None),
        P(),
        P(),
        P("sp", None),
        P("sp", None),
        P("sp", None, "tp"),
        P("sp", None, "tp"),
        P("sp", "tp", None),
        P(),
        P(),
        P(),
        P(),
        P(),
    )

    return jax.shard_map(shards, mesh=mesh, in_specs=in_specs, out_specs=P(("sp", "tp"), None), check_vma=False)
```

```python
import jax
import jax.numpy as jnp
from jax import lax
from jax.experimental import pallas as pl
from jax.experimental.pallas import tpu as pltpu
from jax.sharding import PartitionSpec as P

RESIDUAL_SCALE = 8.0**0.25
NORM_EPSILON = 1e-05
LANES = 128
SLOTS = 2
BF16, F32 = jnp.bfloat16, jnp.float32
VMEM = pl.BlockSpec(memory_space=pltpu.VMEM)
SMEM = pl.BlockSpec(memory_space=pltpu.SMEM)
ANY = pl.BlockSpec(memory_space=pl.ANY)


def kernel_call(body, out_shape, *operands, scratch=(), limit=16):
    several = isinstance(out_shape, (list, tuple))
    specs, arrays = [], []
    for operand in operands:
        array, place = operand if isinstance(operand, tuple) else (operand, None)
        specs.append({"smem": SMEM, "hbm": ANY}.get(place, VMEM))
        if place != "smem":
            array = pltpu.with_memory_space_constraint(array, pltpu.VMEM if place == "vmem" else pltpu.HBM)
        arrays.append(array)
    return pl.pallas_call(
        body,
        out_shape=out_shape,
        in_specs=specs,
        out_specs=[VMEM] * len(out_shape) if several else VMEM,
        scratch_shapes=scratch,
        compiler_params=pltpu.CompilerParams(vmem_limit_bytes=limit << 20),
    )(*arrays)


def fetched(pairs, sems):
    copies = [pltpu.make_async_copy(source, target, sems.at[k]) for k, (source, target) in enumerate(pairs)]
    for copy in copies:
        copy.start()
    return copies


def dot(a, b):
    return jnp.dot(a, b, preferred_element_type=F32)


def layer_norm(values, gain_vec, bias_vec):
    row_mean = jnp.mean(values, axis=-1, keepdims=True)
    spread = jnp.mean(jnp.square(values - row_mean), axis=-1, keepdims=True)
    return (values - row_mean) * lax.rsqrt(spread + NORM_EPSILON) * gain_vec + bias_vec


def softplus(x):
    u = jnp.exp(-jnp.abs(x))
    s = u / (2.0 + u)
    q = s * s
    series = 1.0 / 17.0
    for k in (15.0, 13.0, 11.0, 9.0, 7.0, 5.0, 3.0, 1.0):
        series = series * q + 1.0 / k
    return jnp.maximum(x, 0.0) + 2.0 * s * series


def expm1(z):
    series = 1.0 + z * (1.0 / 9.0)
    for k in (8.0, 7.0, 6.0, 5.0, 4.0, 3.0, 2.0):
        series = 1.0 + z * (1.0 / k) * series
    return jnp.where(jnp.abs(z) < 0.5, z * series, jnp.exp(z) - 1.0)


def shifted_rows(values, by, row, fill):
    if by < 8:
        return jnp.where(row >= by, pltpu.roll(values, by, 0), fill)
    head = jnp.full((by, values.shape[1]), fill, values.dtype)
    return jnp.concatenate([head, values[: values.shape[0] - by]], axis=0)


def chain_rows(decay, drive):
    row = lax.broadcasted_iota(jnp.int32, decay.shape, 0)
    by = 1
    while by < decay.shape[0]:
        drive = decay * shifted_rows(drive, by, row, 0.0) + drive
        decay = decay * shifted_rows(decay, by, row, 1.0)
        by *= 2
    return decay, drive


def flat(array):
    length, groups, half = array.shape
    return array.reshape(length, groups, half // LANES, LANES).transpose(0, 2, 1, 3).reshape(-1, LANES)


def local_kernel(rows, border, taps, small_maps, large_maps, decay_param, extra, decays, states, totals, padded, maps):
    groups, half = decay_param.shape
    per_half = half // LANES
    step = groups * per_half
    length = rows.shape[0] // step
    tap_count = taps.shape[0]
    tap_weights = taps[...].astype(F32)
    rate = -8.0 * softplus(-decay_param[...])
    margin = border.shape[0]
    padded[0:margin] = border[...].astype(F32)
    padded[margin:] = rows[...].astype(F32)
    logs, ends = [], []
    for g, blocks in enumerate((small_maps, large_maps)):
        conv_runs = []
        for c in range(per_half):
            at = slice(c * LANES, (c + 1) * LANES)
            summed = None
            for k in range(tap_count):
                start = margin - (tap_count - 1 - k) * step + c * groups + g
                term = tap_weights[k, g : g + 1, at] * padded[pl.ds(start, length, stride=step), :]
                summed = term if summed is None else summed + term
            conv_runs.append(summed.astype(BF16))
        conv_rows = jnp.concatenate(conv_runs, axis=1)
        maps[...] = jnp.zeros(maps.shape, BF16)
        head = blocks.shape[-1]
        for m in range(2):
            for h in range(blocks.shape[1]):
                maps[h * head : (h + 1) * head, m * half + h * head : m * half + (h + 1) * head] = blocks[m, h]
        gates = jax.nn.sigmoid(dot(conv_rows, maps[...]))
        for c in range(per_half):
            at = slice(c * LANES, (c + 1) * LANES)
            log_decay = gates[:, at] * rate[g : g + 1, at] + extra[pl.ds(c * groups + g, length, stride=step), :]
            gate = gates[:, half + c * LANES : half + (c + 1) * LANES]
            drive = jnp.sqrt(-expm1(2.0 * log_decay)) * gate * conv_runs[c].astype(F32)
            product, state = chain_rows(jnp.exp(log_decay), drive)
            to = slice((g * per_half + c) * LANES, (g * per_half + c + 1) * LANES)
            decays[:, to] = product
            states[:, to] = state
            logs.append(jnp.sum(log_decay, axis=0, keepdims=True))
            ends.append(state[length - 1 :])
    span = jnp.concatenate(logs + ends, axis=0).astype(BF16)
    for j in range(totals.shape[0]):
        totals[j] = span


def entering_state(spans, ahead):
    half = spans.shape[1] // 2
    passed = (ahead[...] > 0.0)[:, None, :]
    decays = jnp.where(passed, jnp.exp(spans[:, :half].astype(F32)), 1.0)
    ends = jnp.where(passed, spans[:, half:].astype(F32), 0.0)
    state = ends[0]
    for j in range(1, spans.shape[0] - 1):
        state = decays[j] * state + ends[j]
    return state


def project_kernel(spans, ahead, decays, states, weight, *outs):
    entering = entering_state(spans, ahead)
    runs = entering.shape[0]
    branches = []
    for run in range(runs):
        at = slice(run * LANES, (run + 1) * LANES)
        branches.append((states[:, at] + decays[:, at] * entering[run : run + 1]).astype(BF16))
    acc, per_half = None, runs // weight.shape[0]
    for g in range(weight.shape[0]):
        part = dot(jnp.concatenate(branches[g * per_half : (g + 1) * per_half], axis=1), weight[g])
        acc = part if acc is None else acc + part
    quarter = outs[0].shape[0]
    for k, out in enumerate(outs):
        out[...] = acc[k * quarter : (k + 1) * quarter].astype(BF16)


def route(ids, weights, select, merge, part):
    slot_count, rows = select.shape[0], ids.shape[1]
    kept_rows = select.shape[1]
    turn = (rows - part * kept_rows) % rows
    own = lax.broadcasted_iota(jnp.int32, ids.shape, 1) < kept_rows
    ids = jnp.where(own, pltpu.roll(ids[...], turn, 1), -1)
    weights = pltpu.roll(weights[...], turn, 1)
    slot = lax.broadcasted_iota(jnp.int32, (slot_count, rows), 0)
    names = jnp.zeros((slot_count, rows), F32)
    weight = jnp.zeros((slot_count, rows), F32)
    for k in range(ids.shape[0]):
        named = ids[k : k + 1] == slot // SLOTS
        names = jnp.where(named, 1.0, names)
        weight = jnp.where(named, weights[k : k + 1], weight)
    earlier = lax.broadcasted_iota(jnp.int32, (rows, rows), 0) < lax.broadcasted_iota(jnp.int32, (rows, rows), 1)
    rank = dot(names.astype(BF16), jnp.where(earlier, 1.0, 0.0).astype(BF16))
    taken = (names > 0.0) & (rank == (slot % SLOTS).astype(F32))
    select[...] = jnp.where(taken, 1.0, 0.0).astype(BF16)[:, : select.shape[1]]
    merge[...] = jnp.where(taken, weight, 0.0).T[: merge.shape[0]]


def mix_kernel(*refs):
    *parts, stream, gain, bias, select, normed, outgoing = refs
    mixed = parts[0][...].astype(F32)
    for part in parts[1:]:
        mixed = mixed + part[...].astype(F32)
    rows = layer_norm(RESIDUAL_SCALE * stream[...].astype(F32) + mixed, gain[...], bias[...]).astype(BF16)
    normed[...] = rows
    outgoing[...] = dot(select[...], rows).astype(BF16).reshape(outgoing.shape)


def side_kernel(places, decays, states, *rest):
    *far, select, merge, turned_decays, turned_states, stream, gain, bias, projection, ahead = rest[:16]
    ids, weights, gate_rows, wide, products, sums, sems = rest[16:]
    copies = fetched(list(zip(far, (gate_rows, ids, weights, stream, gain, bias, projection))), sems)
    part, mine = places[0], places[1]
    ahead[...] = jnp.where(lax.broadcasted_iota(jnp.int32, ahead.shape, 0) < mine, 1.0, 0.0)
    length, runs = decays.shape[0], decays.shape[1] // LANES
    copies[0].wait()
    wide[...] = gate_rows[...].astype(F32)
    groups = 2
    for run in range(runs):
        g, c = divmod(run, runs // groups)
        values = jax.nn.gelu(wide[pl.ds(c * groups + g, length, stride=runs), :], approximate=True)
        at = slice(run * LANES, (run + 1) * LANES)
        products[:, at] = values * decays[:, at]
        sums[:, at] = values * states[:, at]
    quarter = stream.shape[0]
    count = length // quarter
    for k in range(count):
        source = pl.ds(pl.multiple_of(lax.rem(part + k, count) * quarter, quarter), quarter)
        turned_decays[k * quarter : (k + 1) * quarter] = products[source]
        turned_states[k * quarter : (k + 1) * quarter] = sums[source]
    copies[1].wait()
    copies[2].wait()
    route(ids, weights, select, merge, part)
    for copy in copies[3:]:
        copy.wait()


def pair_moves(pairs, weights):
    moves = []
    for j, (gate_w, up_w) in enumerate(weights):
        width = gate_w.shape[1]
        moves += [(gate_w, pairs.at[j, :, 0:width]), (up_w, pairs.at[j, :, width : 2 * width])]
    return moves


def shared_kernel(normed, gate_w, up_w, down_w, merge, gain, bias, g0, u0, g1, u1, base, *rest):
    *kept, near, sems = rest
    copies = fetched(pair_moves(near, ((g0, u0), (g1, u1))), sems)
    for target, source in zip(kept, (merge, gain, bias)):
        target[...] = source[...]
    rows = normed[...]
    gated, lifted = dot(rows, gate_w[...]), dot(rows, up_w[...])
    hidden = (jax.nn.silu(gated) * lifted).astype(BF16)
    base[...] = RESIDUAL_SCALE * rows.astype(F32) + dot(hidden, down_w[...])
    for copy in copies:
        copy.wait()


def expert_kernel(rows, near, g2, u2, g3, u3, d0, d1, d2, acc, last, far, down, sems):
    moves = pair_moves(far, ((g2, u2), (g3, u3)))
    unit = d0.shape[0]
    moves += [(piece, down.at[j * unit : (j + 1) * unit]) for j, piece in enumerate((d0, d1, d2))]
    copies = fetched(moves, sems)
    picked = rows[...].reshape(-1, rows.shape[-1])

    def hidden_of(both):
        pair = dot(picked, both)
        return (jax.nn.silu(pair[:, :unit]) * pair[:, unit:]).astype(BF16)

    hidden = [hidden_of(near[j]) for j in range(near.shape[0])]
    for j in range(far.shape[0]):
        copies[2 * j].wait()
        copies[2 * j + 1].wait()
        hidden.append(hidden_of(far[j]))
    last[...] = hidden.pop()
    for copy in copies[2 * far.shape[0] :]:
        copy.wait()
    acc[...] = dot(jnp.concatenate(hidden, axis=1), down[...])


def last_kernel(acc, hidden, d3a, d3b, out):
    total = acc[...] + dot(hidden[...], jnp.concatenate([d3a[...], d3b[...]], axis=0))
    out[...] = total.astype(BF16).reshape(out.shape)


def merge_kernel(returned, base, merge, gain, bias, out):
    rest = merge[...]
    rows = returned[...].reshape(-1, returned.shape[-1])
    total = base[...]
    for _ in range(3):
        part = rest.astype(BF16)
        total = total + dot(part, rows)
        rest = rest - part.astype(F32)
    out[...] = layer_norm(total, gain[...], bias[...]).astype(BF16)


def turned(shard, by):
    count = lax.axis_size("tp")
    return lax.ppermute(shard, "tp", [(i, (i + by) % count) for i in range(count)])


def swapped(pieces, axis):
    return lax.all_to_all(pieces, axis, 0, 0, tiled=True)


def shards(
    stream,
    recurrence_input,
    output_gate_input,
    convolution_taps,
    first_group_gates,
    second_group_gates,
    channel_decay,
    position_log_extra,
    recurrence_output_weight,
    first_norm_gain,
    first_norm_bias,
    routed_expert_index,
    routed_expert_weight,
    routed_gate_weight,
    routed_up_weight,
    routed_down_weight,
    shared_gate_weight,
    shared_up_weight,
    shared_down_weight,
    second_norm_gain,
    second_norm_bias,
):
    length, groups, half = recurrence_input.shape
    width = stream.shape[1]
    tp_count, sp_count = lax.axis_size("tp"), lax.axis_size("sp")
    quarter = length // tp_count
    expert_count = routed_gate_weight.shape[0] * sp_count
    slot_count = expert_count * SLOTS
    channels = groups * half
    shape, kept = jax.ShapeDtypeStruct, pltpu.VMEM

    rows = flat(recurrence_input)
    margin = 16
    border = lax.ppermute(rows[rows.shape[0] - margin :], "sp", [(i, i + 1) for i in range(sp_count - 1)])

    gate_w, up_w, down_w = routed_gate_weight[0], routed_up_weight[0], routed_down_weight[0]
    gate_left, up_right = turned(gate_w, 1), turned(up_w, -1)
    up_left, gate_right = turned(up_w, 1), turned(gate_w, -1)
    down_left, down_right = turned(down_w, 1), turned(down_w, -1)

    runs = channels // LANES
    decays, states, totals = kernel_call(
        local_kernel,
        [kept((length, channels), F32), kept((length, channels), F32), shape((sp_count, 2 * runs, LANES), BF16)],
        rows,
        (border, "vmem"),
        convolution_taps,
        first_group_gates,
        second_group_gates,
        channel_decay,
        flat(position_log_extra),
        scratch=(pltpu.VMEM((margin + rows.shape[0], LANES), F32), pltpu.VMEM((half, 2 * half), BF16)),
    )
    spans = swapped(totals, "sp")

    side = (
        flat(output_gate_input),
        routed_expert_index.T,
        routed_expert_weight.T,
        stream,
        first_norm_gain.reshape(1, width),
        first_norm_bias.reshape(1, width),
        recurrence_output_weight,
    )
    select, merge, decays, states, *norm_parts, projection, ahead = kernel_call(
        side_kernel,
        [
            kept((slot_count, quarter), BF16),
            kept((quarter, slot_count), F32),
            kept((length, channels), F32),
            kept((length, channels), F32),
            kept((quarter, width), BF16),
            kept((1, width), F32),
            kept((1, width), F32),
            kept(recurrence_output_weight.shape, BF16),
            kept((sp_count, LANES), F32),
        ],
        (jnp.stack([lax.axis_index("tp"), lax.axis_index("sp")]), "smem"),
        (decays, "vmem"),
        (states, "vmem"),
        *((x, "hbm") for x in side),
        scratch=(
            pltpu.VMEM(routed_expert_index.T.shape, jnp.int32),
            pltpu.VMEM(routed_expert_weight.T.shape, F32),
            pltpu.VMEM(rows.shape, BF16),
            pltpu.VMEM(rows.shape, F32),
            pltpu.VMEM((length, channels), F32),
            pltpu.VMEM((length, channels), F32),
            pltpu.SemaphoreType.DMA((len(side),)),
        ),
    )
    own, *others = kernel_call(
        project_kernel,
        [kept((quarter, width), BF16) for _ in range(tp_count)],
        *((x, "vmem") for x in (spans, ahead, decays, states, projection)),
    )
    parts = {k: turned(others[k - 1], k) for k in (2, 1, 3)}
    parts = [own, *(parts[k] for k in (1, 3, 2))]

    gate_far, up_far = turned(gate_left, 1), turned(up_right, -1)

    normed, outgoing = kernel_call(
        mix_kernel,
        [kept((quarter, width), BF16), shape((expert_count, SLOTS, width), BF16)],
        *((x, "vmem") for x in parts),
        *((x, "vmem") for x in norm_parts),
        (select, "vmem"),
    )
    arrived = swapped(outgoing, "sp")

    cut = down_w.shape[0] // 4
    down_far = turned(down_left[:cut], 1), turned(down_right[cut:], -1)

    last = (merge, second_norm_gain.reshape(1, width), second_norm_bias.reshape(1, width))
    near_weights = (gate_w, up_w, gate_left, up_left)
    unit = gate_w.shape[1]
    base, *last, near = kernel_call(
        shared_kernel,
        [
            kept((quarter, width), F32),
            *(kept(x.shape, F32) for x in last),
            kept((len(near_weights) // 2, width, 2 * unit), BF16),
        ],
        (normed, "vmem"),
        shared_gate_weight,
        shared_up_weight,
        shared_down_weight,
        (last[0], "vmem"),
        *last[1:],
        *((w, "hbm") for w in near_weights),
        scratch=(pltpu.SemaphoreType.DMA((len(near_weights),)),),
    )
    weights = (gate_right, up_right, gate_far, up_far, down_w, down_left, down_right)
    acc, hidden = kernel_call(
        expert_kernel,
        [kept((slot_count, width), F32), kept((slot_count, unit), BF16)],
        (arrived, "vmem"),
        (near, "vmem"),
        *((w, "hbm") for w in weights),
        scratch=(
            pltpu.VMEM((2, width, 2 * unit), BF16),
            pltpu.VMEM((3 * unit, width), BF16),
            pltpu.SemaphoreType.DMA((len(weights),)),
        ),
    )
    leaving = kernel_call(
        last_kernel, kept((expert_count, SLOTS, width), BF16), (acc, "vmem"), (hidden, "vmem"), *down_far
    )
    returned = swapped(leaving, "sp")
    return kernel_call(
        merge_kernel, shape((quarter, width), BF16), (returned, "vmem"), (base, "vmem"), *((x, "vmem") for x in last)
    )


def solution(mesh):
    in_specs = (
        P(("sp", "tp"), None),
        P("sp", None, "tp"),
        P("sp", None, "tp"),
        P(None, None, "tp"),
        P(None, "tp", None, None),
        P(None, "tp", None, None),
        P(None, "tp"),
        P("sp", None, "tp"),
        P(None, "tp", None),
        P(),
        P(),
        P("sp", None),
        P("sp", None),
        P("sp", None, "tp"),
        P("sp", None, "tp"),
        P("sp", "tp", None),
        P(),
        P(),
        P(),
        P(),
        P(),
    )

    return jax.shard_map(shards, mesh=mesh, in_specs=in_specs, out_specs=P(("sp", "tp"), None), check_vma=False)
```

```python
import jax
import jax.numpy as jnp
from jax import lax
from jax.experimental import pallas as pl
from jax.experimental.pallas import tpu as pltpu
from jax.sharding import PartitionSpec as P

RESIDUAL_SCALE = 8.0**0.25
NORM_EPSILON = 1e-05
LANES = 128
SLOTS = 2
BF16, F32 = jnp.bfloat16, jnp.float32
VMEM = pl.BlockSpec(memory_space=pltpu.VMEM)
SMEM = pl.BlockSpec(memory_space=pltpu.SMEM)
ANY = pl.BlockSpec(memory_space=pl.ANY)


def kernel_call(body, out_shape, *operands, scratch=(), limit=16):
    several = isinstance(out_shape, (list, tuple))
    specs, arrays = [], []
    for operand in operands:
        array, place = operand if isinstance(operand, tuple) else (operand, None)
        specs.append({"smem": SMEM, "hbm": ANY}.get(place, VMEM))
        if place != "smem":
            array = pltpu.with_memory_space_constraint(array, pltpu.VMEM if place == "vmem" else pltpu.HBM)
        arrays.append(array)
    return pl.pallas_call(
        body,
        out_shape=out_shape,
        in_specs=specs,
        out_specs=[VMEM] * len(out_shape) if several else VMEM,
        scratch_shapes=scratch,
        compiler_params=pltpu.CompilerParams(vmem_limit_bytes=limit << 20),
    )(*arrays)


def fetched(pairs, sems):
    copies = [pltpu.make_async_copy(source, target, sems.at[k]) for k, (source, target) in enumerate(pairs)]
    for copy in copies:
        copy.start()
    return copies


def dot(a, b):
    return jnp.dot(a, b, preferred_element_type=F32)


def layer_norm(values, gain_vec, bias_vec):
    row_mean = jnp.mean(values, axis=-1, keepdims=True)
    spread = jnp.mean(jnp.square(values - row_mean), axis=-1, keepdims=True)
    return (values - row_mean) * lax.rsqrt(spread + NORM_EPSILON) * gain_vec + bias_vec


def softplus(x):
    u = jnp.exp(-jnp.abs(x))
    s = u / (2.0 + u)
    q = s * s
    series = 1.0 / 17.0
    for k in (15.0, 13.0, 11.0, 9.0, 7.0, 5.0, 3.0, 1.0):
        series = series * q + 1.0 / k
    return jnp.maximum(x, 0.0) + 2.0 * s * series


def expm1(z):
    series = 1.0 + z * (1.0 / 9.0)
    for k in (8.0, 7.0, 6.0, 5.0, 4.0, 3.0, 2.0):
        series = 1.0 + z * (1.0 / k) * series
    return jnp.where(jnp.abs(z) < 0.5, z * series, jnp.exp(z) - 1.0)


def shifted_rows(values, by, row, fill):
    if by < 8:
        return jnp.where(row >= by, pltpu.roll(values, by, 0), fill)
    head = jnp.full((by, values.shape[1]), fill, values.dtype)
    return jnp.concatenate([head, values[: values.shape[0] - by]], axis=0)


def chain_rows(decay, drive):
    row = lax.broadcasted_iota(jnp.int32, decay.shape, 0)
    by = 1
    while by < decay.shape[0]:
        drive = decay * shifted_rows(drive, by, row, 0.0) + drive
        decay = decay * shifted_rows(decay, by, row, 1.0)
        by *= 2
    return decay, drive


def flat(array):
    length, groups, half = array.shape
    return array.reshape(length, groups, half // LANES, LANES).transpose(0, 2, 1, 3).reshape(-1, LANES)


def load_kernel(*refs):
    count = (len(refs) - 2) // 2
    far, near, edge, sems = refs[:count], refs[count : 2 * count], refs[-2], refs[-1]
    copies = fetched(list(zip(far, near)), sems)
    copies[0].wait()
    edge[...] = near[0][near[0].shape[0] - edge.shape[0] :]
    for copy in copies[1:]:
        copy.wait()


def local_kernel(rows, taps, small_maps, large_maps, decay_param, extra, border, decays, states, totals, padded, maps):
    groups, half = decay_param.shape
    per_half = half // LANES
    step = groups * per_half
    length = rows.shape[0] // step
    tap_count = taps.shape[0]
    tap_weights = taps[...].astype(F32)
    rate = -8.0 * softplus(-decay_param[...])
    margin = border.shape[0]
    padded[0:margin] = border[...].astype(F32)
    padded[margin:] = rows[...].astype(F32)
    head = small_maps.shape[-1]
    per_run = LANES // head
    maps[...] = jnp.zeros(maps.shape, BF16)
    for c in range(per_half):
        for m in range(2):
            for h in range(per_run):
                at = h * head
                maps[c, at : at + head, m * LANES + at : m * LANES + at + head] = small_maps[m, c * per_run + h]
    logs, ends = [], []
    for g in range(groups):
        for c in range(per_half):
            at = slice(c * LANES, (c + 1) * LANES)
            summed = None
            for k in range(tap_count):
                start = margin - (tap_count - 1 - k) * step + c * groups + g
                term = tap_weights[k, g : g + 1, at] * padded[pl.ds(start, length, stride=step), :]
                summed = term if summed is None else summed + term
            conv_rows = summed.astype(BF16)
            both = maps[c] if g == 0 else jnp.concatenate([large_maps[0, c], large_maps[1, c]], axis=1)
            gates = jax.nn.sigmoid(dot(conv_rows, both))
            log_decay = gates[:, :LANES] * rate[g : g + 1, at] + extra[pl.ds(c * groups + g, length, stride=step), :]
            drive = jnp.sqrt(-expm1(2.0 * log_decay)) * gates[:, LANES:] * conv_rows.astype(F32)
            product, state = chain_rows(jnp.exp(log_decay), drive)
            to = slice((g * per_half + c) * LANES, (g * per_half + c + 1) * LANES)
            decays[:, to] = product
            states[:, to] = state
            logs.append(jnp.sum(log_decay, axis=0, keepdims=True))
            ends.append(state[length - 1 :])
    span = jnp.concatenate(logs + ends, axis=0).astype(BF16)
    for j in range(totals.shape[0]):
        totals[j] = span


def entering_state(spans, ahead):
    half = spans.shape[1] // 2
    passed = (ahead[...] > 0.0)[:, None, :]
    decays = jnp.where(passed, jnp.exp(spans[:, :half].astype(F32)), 1.0)
    ends = jnp.where(passed, spans[:, half:].astype(F32), 0.0)
    state = ends[0]
    for j in range(1, spans.shape[0] - 1):
        state = decays[j] * state + ends[j]
    return state


def project_kernel(spans, ahead, decays, states, weight, *outs):
    entering = entering_state(spans, ahead)
    runs = entering.shape[0]
    branches = []
    for run in range(runs):
        at = slice(run * LANES, (run + 1) * LANES)
        branches.append((states[:, at] + decays[:, at] * entering[run : run + 1]).astype(BF16))
    acc, per_half = None, runs // weight.shape[0]
    for g in range(weight.shape[0]):
        part = dot(jnp.concatenate(branches[g * per_half : (g + 1) * per_half], axis=1), weight[g])
        acc = part if acc is None else acc + part
    quarter = outs[0].shape[0]
    for k, out in enumerate(outs):
        out[...] = acc[k * quarter : (k + 1) * quarter].astype(BF16)


def route(ids, weights, select, merge, part):
    slot_count, rows = select.shape[0], ids.shape[1]
    kept_rows = select.shape[1]
    turn = (rows - part * kept_rows) % rows
    own = lax.broadcasted_iota(jnp.int32, ids.shape, 1) < kept_rows
    ids = jnp.where(own, pltpu.roll(ids[...], turn, 1), -1)
    weights = pltpu.roll(weights[...], turn, 1)
    slot = lax.broadcasted_iota(jnp.int32, (slot_count, rows), 0)
    names = jnp.zeros((slot_count, rows), F32)
    weight = jnp.zeros((slot_count, rows), F32)
    for k in range(ids.shape[0]):
        named = ids[k : k + 1] == slot // SLOTS
        names = jnp.where(named, 1.0, names)
        weight = jnp.where(named, weights[k : k + 1], weight)
    earlier = lax.broadcasted_iota(jnp.int32, (rows, rows), 0) < lax.broadcasted_iota(jnp.int32, (rows, rows), 1)
    rank = dot(names.astype(BF16), jnp.where(earlier, 1.0, 0.0).astype(BF16))
    taken = (names > 0.0) & (rank == (slot % SLOTS).astype(F32))
    select[...] = jnp.where(taken, 1.0, 0.0).astype(BF16)[:, : select.shape[1]]
    merge[...] = jnp.where(taken, weight, 0.0).T[: merge.shape[0]]


def mix_kernel(*refs):
    *parts, stream, gain, bias, select, normed, outgoing = refs
    mixed = parts[0][...].astype(F32)
    for part in parts[1:]:
        mixed = mixed + part[...].astype(F32)
    rows = layer_norm(RESIDUAL_SCALE * stream[...].astype(F32) + mixed, gain[...], bias[...]).astype(BF16)
    normed[...] = rows
    outgoing[...] = dot(select[...], rows).astype(BF16).reshape(outgoing.shape)


def side_kernel(places, decays, states, *rest):
    *far, select, merge, turned_decays, turned_states, stream, gain, bias, projection, ahead = rest[:16]
    ids, weights, gate_rows, wide, products, sums, sems = rest[16:]
    copies = fetched(list(zip(far, (gate_rows, ids, weights, stream, gain, bias, projection))), sems)
    part, mine = places[0], places[1]
    ahead[...] = jnp.where(lax.broadcasted_iota(jnp.int32, ahead.shape, 0) < mine, 1.0, 0.0)
    length, runs = decays.shape[0], decays.shape[1] // LANES
    copies[0].wait()
    wide[...] = gate_rows[...].astype(F32)
    groups = 2
    for run in range(runs):
        g, c = divmod(run, runs // groups)
        values = jax.nn.gelu(wide[pl.ds(c * groups + g, length, stride=runs), :], approximate=True)
        at = slice(run * LANES, (run + 1) * LANES)
        products[:, at] = values * decays[:, at]
        sums[:, at] = values * states[:, at]
    quarter = stream.shape[0]
    count = length // quarter
    for k in range(count):
        source = pl.ds(pl.multiple_of(lax.rem(part + k, count) * quarter, quarter), quarter)
        turned_decays[k * quarter : (k + 1) * quarter] = products[source]
        turned_states[k * quarter : (k + 1) * quarter] = sums[source]
    copies[1].wait()
    copies[2].wait()
    route(ids, weights, select, merge, part)
    for copy in copies[3:]:
        copy.wait()


def pair_moves(pairs, weights):
    moves = []
    for j, (gate_w, up_w) in enumerate(weights):
        width = gate_w.shape[1]
        moves += [(gate_w, pairs.at[j, :, 0:width]), (up_w, pairs.at[j, :, width : 2 * width])]
    return moves


def shared_kernel(normed, gate_w, up_w, down_w, merge, gain, bias, g0, u0, g1, u1, base, *rest):
    *kept, near, sems = rest
    copies = fetched(pair_moves(near, ((g0, u0), (g1, u1))), sems)
    for target, source in zip(kept, (merge, gain, bias)):
        target[...] = source[...]
    rows = normed[...]
    gated, lifted = dot(rows, gate_w[...]), dot(rows, up_w[...])
    hidden = (jax.nn.silu(gated) * lifted).astype(BF16)
    base[...] = RESIDUAL_SCALE * rows.astype(F32) + dot(hidden, down_w[...])
    for copy in copies:
        copy.wait()


def expert_kernel(rows, near, g2, u2, g3, u3, d0, d1, d2, acc, last, far, down, sems):
    moves = pair_moves(far, ((g2, u2), (g3, u3)))
    unit = d0.shape[0]
    moves += [(piece, down.at[j * unit : (j + 1) * unit]) for j, piece in enumerate((d0, d1, d2))]
    copies = fetched(moves, sems)
    picked = rows[...].reshape(-1, rows.shape[-1])

    def hidden_of(both):
        pair = dot(picked, both)
        return (jax.nn.silu(pair[:, :unit]) * pair[:, unit:]).astype(BF16)

    hidden = [hidden_of(near[j]) for j in range(near.shape[0])]
    for j in range(far.shape[0]):
        copies[2 * j].wait()
        copies[2 * j + 1].wait()
        hidden.append(hidden_of(far[j]))
    last[...] = hidden.pop()
    for copy in copies[2 * far.shape[0] :]:
        copy.wait()
    acc[...] = dot(jnp.concatenate(hidden, axis=1), down[...])


def last_kernel(acc, hidden, d3a, d3b, out):
    total = acc[...] + dot(hidden[...], jnp.concatenate([d3a[...], d3b[...]], axis=0))
    out[...] = total.astype(BF16).reshape(out.shape)


def merge_kernel(returned, base, merge, gain, bias, out):
    rest = merge[...]
    rows = returned[...].reshape(-1, returned.shape[-1])
    total = base[...]
    for _ in range(3):
        part = rest.astype(BF16)
        total = total + dot(part, rows)
        rest = rest - part.astype(F32)
    out[...] = layer_norm(total, gain[...], bias[...]).astype(BF16)


def turned(shard, by):
    count = lax.axis_size("tp")
    return lax.ppermute(shard, "tp", [(i, (i + by) % count) for i in range(count)])


def swapped(pieces, axis):
    return lax.all_to_all(pieces, axis, 0, 0, tiled=True)


def shards(
    stream,
    recurrence_input,
    output_gate_input,
    convolution_taps,
    first_group_gates,
    second_group_gates,
    channel_decay,
    position_log_extra,
    recurrence_output_weight,
    first_norm_gain,
    first_norm_bias,
    routed_expert_index,
    routed_expert_weight,
    routed_gate_weight,
    routed_up_weight,
    routed_down_weight,
    shared_gate_weight,
    shared_up_weight,
    shared_down_weight,
    second_norm_gain,
    second_norm_bias,
):
    length, groups, half = recurrence_input.shape
    width = stream.shape[1]
    tp_count, sp_count = lax.axis_size("tp"), lax.axis_size("sp")
    quarter = length // tp_count
    expert_count = routed_gate_weight.shape[0] * sp_count
    slot_count = expert_count * SLOTS
    channels = groups * half
    shape, kept = jax.ShapeDtypeStruct, pltpu.VMEM

    rows = flat(recurrence_input)
    margin = 16
    operands = (
        rows,
        convolution_taps,
        first_group_gates,
        second_group_gates,
        channel_decay,
        flat(position_log_extra),
    )
    *operands, edge = kernel_call(
        load_kernel,
        [*(kept(x.shape, x.dtype) for x in operands), kept((margin, LANES), BF16)],
        *((x, "hbm") for x in operands),
        scratch=(pltpu.SemaphoreType.DMA((len(operands),)),),
    )
    border = lax.ppermute(edge, "sp", [(i, i + 1) for i in range(sp_count - 1)])

    gate_w, up_w, down_w = routed_gate_weight[0], routed_up_weight[0], routed_down_weight[0]
    gate_left, up_right = turned(gate_w, 1), turned(up_w, -1)
    up_left, gate_right = turned(up_w, 1), turned(gate_w, -1)
    down_left, down_right = turned(down_w, 1), turned(down_w, -1)

    runs = channels // LANES
    decays, states, totals = kernel_call(
        local_kernel,
        [kept((length, channels), F32), kept((length, channels), F32), shape((sp_count, 2 * runs, LANES), BF16)],
        *((x, "vmem") for x in (*operands, border)),
        scratch=(
            pltpu.VMEM((margin + rows.shape[0], LANES), F32),
            pltpu.VMEM((half // LANES, LANES, 2 * LANES), BF16),
        ),
    )
    spans = swapped(totals, "sp")

    side = (
        flat(output_gate_input),
        routed_expert_index.T,
        routed_expert_weight.T,
        stream,
        first_norm_gain.reshape(1, width),
        first_norm_bias.reshape(1, width),
        recurrence_output_weight,
    )
    select, merge, decays, states, *norm_parts, projection, ahead = kernel_call(
        side_kernel,
        [
            kept((slot_count, quarter), BF16),
            kept((quarter, slot_count), F32),
            kept((length, channels), F32),
            kept((length, channels), F32),
            kept((quarter, width), BF16),
            kept((1, width), F32),
            kept((1, width), F32),
            kept(recurrence_output_weight.shape, BF16),
            kept((sp_count, LANES), F32),
        ],
        (jnp.stack([lax.axis_index("tp"), lax.axis_index("sp")]), "smem"),
        (decays, "vmem"),
        (states, "vmem"),
        *((x, "hbm") for x in side),
        scratch=(
            pltpu.VMEM(routed_expert_index.T.shape, jnp.int32),
            pltpu.VMEM(routed_expert_weight.T.shape, F32),
            pltpu.VMEM(rows.shape, BF16),
            pltpu.VMEM(rows.shape, F32),
            pltpu.VMEM((length, channels), F32),
            pltpu.VMEM((length, channels), F32),
            pltpu.SemaphoreType.DMA((len(side),)),
        ),
    )
    own, *others = kernel_call(
        project_kernel,
        [kept((quarter, width), BF16) for _ in range(tp_count)],
        *((x, "vmem") for x in (spans, ahead, decays, states, projection)),
    )
    parts = {k: turned(others[k - 1], k) for k in (2, 1, 3)}
    parts = [own, *(parts[k] for k in (1, 3, 2))]

    gate_far, up_far = turned(gate_left, 1), turned(up_right, -1)

    normed, outgoing = kernel_call(
        mix_kernel,
        [kept((quarter, width), BF16), shape((expert_count, SLOTS, width), BF16)],
        *((x, "vmem") for x in parts),
        *((x, "vmem") for x in norm_parts),
        (select, "vmem"),
    )
    arrived = swapped(outgoing, "sp")

    cut = down_w.shape[0] // 2
    down_far = turned(down_left[:cut], 1), turned(down_right[cut:], -1)

    last = (merge, second_norm_gain.reshape(1, width), second_norm_bias.reshape(1, width))
    near_weights = (gate_w, up_w, gate_left, up_left)
    unit = gate_w.shape[1]
    base, *last, near = kernel_call(
        shared_kernel,
        [
            kept((quarter, width), F32),
            *(kept(x.shape, F32) for x in last),
            kept((len(near_weights) // 2, width, 2 * unit), BF16),
        ],
        (normed, "vmem"),
        shared_gate_weight,
        shared_up_weight,
        shared_down_weight,
        (last[0], "vmem"),
        *last[1:],
        *((w, "hbm") for w in near_weights),
        scratch=(pltpu.SemaphoreType.DMA((len(near_weights),)),),
    )
    weights = (gate_right, up_right, gate_far, up_far, down_w, down_left, down_right)
    acc, hidden = kernel_call(
        expert_kernel,
        [kept((slot_count, width), F32), kept((slot_count, unit), BF16)],
        (arrived, "vmem"),
        (near, "vmem"),
        *((w, "hbm") for w in weights),
        scratch=(
            pltpu.VMEM((2, width, 2 * unit), BF16),
            pltpu.VMEM((3 * unit, width), BF16),
            pltpu.SemaphoreType.DMA((len(weights),)),
        ),
    )
    leaving = kernel_call(
        last_kernel, kept((expert_count, SLOTS, width), BF16), (acc, "vmem"), (hidden, "vmem"), *down_far
    )
    returned = swapped(leaving, "sp")
    return kernel_call(
        merge_kernel, shape((quarter, width), BF16), (returned, "vmem"), (base, "vmem"), *((x, "vmem") for x in last)
    )


def solution(mesh):
    in_specs = (
        P(("sp", "tp"), None),
        P("sp", None, "tp"),
        P("sp", None, "tp"),
        P(None, None, "tp"),
        P(None, "tp", None, None),
        P(None, "tp", None, None),
        P(None, "tp"),
        P("sp", None, "tp"),
        P(None, "tp", None),
        P(),
        P(),
        P("sp", None),
        P("sp", None),
        P("sp", None, "tp"),
        P("sp", None, "tp"),
        P("sp", "tp", None),
        P(),
        P(),
        P(),
        P(),
        P(),
    )

    return jax.shard_map(shards, mesh=mesh, in_specs=in_specs, out_specs=P(("sp", "tp"), None), check_vma=False)
```

```python
import jax
import jax.numpy as jnp
from jax import lax
from jax.experimental import pallas as pl
from jax.experimental.pallas import tpu as pltpu
from jax.sharding import PartitionSpec as P

RESIDUAL_SCALE = 8.0**0.25
NORM_EPSILON = 1e-05
LANES = 128
SLOTS = 2
BF16, F32 = jnp.bfloat16, jnp.float32
VMEM = pl.BlockSpec(memory_space=pltpu.VMEM)
SMEM = pl.BlockSpec(memory_space=pltpu.SMEM)
ANY = pl.BlockSpec(memory_space=pl.ANY)


def kernel_call(body, out_shape, *operands, scratch=(), limit=16):
    several = isinstance(out_shape, (list, tuple))
    specs, arrays = [], []
    for operand in operands:
        array, place = operand if isinstance(operand, tuple) else (operand, None)
        specs.append({"smem": SMEM, "hbm": ANY}.get(place, VMEM))
        if place != "smem":
            array = pltpu.with_memory_space_constraint(array, pltpu.VMEM if place == "vmem" else pltpu.HBM)
        arrays.append(array)
    return pl.pallas_call(
        body,
        out_shape=out_shape,
        in_specs=specs,
        out_specs=[VMEM] * len(out_shape) if several else VMEM,
        scratch_shapes=scratch,
        compiler_params=pltpu.CompilerParams(vmem_limit_bytes=limit << 20),
    )(*arrays)


def fetched(pairs, sems):
    copies = [pltpu.make_async_copy(source, target, sems.at[k]) for k, (source, target) in enumerate(pairs)]
    for copy in copies:
        copy.start()
    return copies


def dot(a, b):
    return jnp.dot(a, b, preferred_element_type=F32)


def layer_norm(values, gain_vec, bias_vec):
    row_mean = jnp.mean(values, axis=-1, keepdims=True)
    spread = jnp.mean(jnp.square(values - row_mean), axis=-1, keepdims=True)
    return (values - row_mean) * lax.rsqrt(spread + NORM_EPSILON) * gain_vec + bias_vec


def softplus(x):
    u = jnp.exp(-jnp.abs(x))
    s = u / (2.0 + u)
    q = s * s
    series = 1.0 / 17.0
    for k in (15.0, 13.0, 11.0, 9.0, 7.0, 5.0, 3.0, 1.0):
        series = series * q + 1.0 / k
    return jnp.maximum(x, 0.0) + 2.0 * s * series


def expm1(z):
    series = 1.0 + z * (1.0 / 9.0)
    for k in (8.0, 7.0, 6.0, 5.0, 4.0, 3.0, 2.0):
        series = 1.0 + z * (1.0 / k) * series
    return jnp.where(jnp.abs(z) < 0.5, z * series, jnp.exp(z) - 1.0)


def shifted_rows(values, by, row, fill):
    if by < 8:
        return jnp.where(row >= by, pltpu.roll(values, by, 0), fill)
    head = jnp.full((by, values.shape[1]), fill, values.dtype)
    return jnp.concatenate([head, values[: values.shape[0] - by]], axis=0)


def chain_rows(decay, drive):
    row = lax.broadcasted_iota(jnp.int32, decay.shape, 0)
    by = 1
    while by < decay.shape[0]:
        drive = decay * shifted_rows(drive, by, row, 0.0) + drive
        decay = decay * shifted_rows(decay, by, row, 1.0)
        by *= 2
    return decay, drive


def flat(array):
    length, groups, half = array.shape
    return array.reshape(length, groups, half // LANES, LANES).transpose(0, 2, 1, 3).reshape(-1, LANES)


def load_kernel(*refs):
    *far, extra, conv, small_pairs, large_pairs, rate, taps_wide, rows, taps, small_maps, large_maps, decay_param, wide, sems = refs
    copies = fetched(list(zip(far, (rows, taps, small_maps, large_maps, decay_param, extra))), sems)
    for copy in copies[:5]:
        copy.wait()
    groups, half = decay_param.shape
    per_half = half // LANES
    step = groups * per_half
    length = rows.shape[0] // step
    margin = wide.shape[0] - rows.shape[0]
    tap_count = taps.shape[0]
    tap_weights = taps[...].astype(F32)
    taps_wide[...] = tap_weights
    rate[...] = -8.0 * softplus(-decay_param[...])
    head = small_maps.shape[-1]
    per_run = LANES // head
    small_pairs[...] = jnp.zeros(small_pairs.shape, BF16)
    for c in range(per_half):
        for m in range(2):
            for h in range(per_run):
                at = h * head
                small_pairs[c, at : at + head, m * LANES + at : m * LANES + at + head] = small_maps[m, c * per_run + h]
            large_pairs[c, :, m * LANES : (m + 1) * LANES] = large_maps[m, c]
    wide[0:margin] = jnp.zeros((margin, LANES), F32)
    wide[margin:] = rows[...].astype(F32)
    for run in range(step):
        g, c = divmod(run, per_half)
        at = slice(c * LANES, (c + 1) * LANES)
        summed = None
        for k in range(tap_count):
            start = margin - (tap_count - 1 - k) * step + c * groups + g
            term = tap_weights[k, g : g + 1, at] * wide[pl.ds(start, length, stride=step), :]
            summed = term if summed is None else summed + term
        conv[:, run * LANES : (run + 1) * LANES] = summed
    copies[5].wait()


def local_kernel(border, extra, conv, small_pairs, large_pairs, rate, taps, decays, states, totals, edge):
    groups = rate.shape[0]
    per_half = small_pairs.shape[0]
    step = groups * per_half
    length = conv.shape[0]
    tap_count = taps.shape[0]
    tap_weights = taps[...]
    margin = border.shape[0]
    edge[0:margin] = border[...].astype(F32)
    edge[margin:] = jnp.zeros((edge.shape[0] - margin, LANES), F32)
    top = (edge.shape[0] - margin) // step
    logs, ends = [], []
    for run in range(step):
        g, c = divmod(run, per_half)
        at = slice(c * LANES, (c + 1) * LANES)
        to = slice(run * LANES, (run + 1) * LANES)
        first = conv[0:top, to]
        for k in range(tap_count - 1):
            start = margin - (tap_count - 1 - k) * step + c * groups + g
            first = first + tap_weights[k, g : g + 1, at] * edge[pl.ds(start, top, stride=step), :]
        conv_rows = jnp.concatenate([first, conv[top:, to]], axis=0).astype(BF16)
        gates = jax.nn.sigmoid(dot(conv_rows, (small_pairs, large_pairs)[g][c]))
        log_decay = gates[:, :LANES] * rate[g : g + 1, at] + extra[pl.ds(c * groups + g, length, stride=step), :]
        drive = jnp.sqrt(-expm1(2.0 * log_decay)) * gates[:, LANES:] * conv_rows.astype(F32)
        product, state = chain_rows(jnp.exp(log_decay), drive)
        decays[:, to] = product
        states[:, to] = state
        logs.append(jnp.sum(log_decay, axis=0, keepdims=True))
        ends.append(state[length - 1 :])
    span = jnp.concatenate(logs + ends, axis=0).astype(BF16)
    for j in range(totals.shape[0]):
        totals[j] = span


def entering_state(spans, ahead):
    half = spans.shape[1] // 2
    passed = (ahead[...] > 0.0)[:, None, :]
    decays = jnp.where(passed, jnp.exp(spans[:, :half].astype(F32)), 1.0)
    ends = jnp.where(passed, spans[:, half:].astype(F32), 0.0)
    state = ends[0]
    for j in range(1, spans.shape[0] - 1):
        state = decays[j] * state + ends[j]
    return state


def project_kernel(spans, ahead, decays, states, weight, *outs):
    entering = entering_state(spans, ahead)
    runs = entering.shape[0]
    branches = []
    for run in range(runs):
        at = slice(run * LANES, (run + 1) * LANES)
        branches.append((states[:, at] + decays[:, at] * entering[run : run + 1]).astype(BF16))
    acc, per_half = None, runs // weight.shape[0]
    for g in range(weight.shape[0]):
        part = dot(jnp.concatenate(branches[g * per_half : (g + 1) * per_half], axis=1), weight[g])
        acc = part if acc is None else acc + part
    quarter = outs[0].shape[0]
    for k, out in enumerate(outs):
        out[...] = acc[k * quarter : (k + 1) * quarter].astype(BF16)


def route(ids, weights, select, merge, part):
    slot_count, rows = select.shape[0], ids.shape[1]
    kept_rows = select.shape[1]
    turn = (rows - part * kept_rows) % rows
    own = lax.broadcasted_iota(jnp.int32, ids.shape, 1) < kept_rows
    ids = jnp.where(own, pltpu.roll(ids[...], turn, 1), -1)
    weights = pltpu.roll(weights[...], turn, 1)
    slot = lax.broadcasted_iota(jnp.int32, (slot_count, rows), 0)
    names = jnp.zeros((slot_count, rows), F32)
    weight = jnp.zeros((slot_count, rows), F32)
    for k in range(ids.shape[0]):
        named = ids[k : k + 1] == slot // SLOTS
        names = jnp.where(named, 1.0, names)
        weight = jnp.where(named, weights[k : k + 1], weight)
    earlier = lax.broadcasted_iota(jnp.int32, (rows, rows), 0) < lax.broadcasted_iota(jnp.int32, (rows, rows), 1)
    rank = dot(names.astype(BF16), jnp.where(earlier, 1.0, 0.0).astype(BF16))
    taken = (names > 0.0) & (rank == (slot % SLOTS).astype(F32))
    select[...] = jnp.where(taken, 1.0, 0.0).astype(BF16)[:, : select.shape[1]]
    merge[...] = jnp.where(taken, weight, 0.0).T[: merge.shape[0]]


def mix_kernel(*refs):
    *parts, stream, gain, bias, select, normed, outgoing = refs
    mixed = parts[0][...].astype(F32)
    for part in parts[1:]:
        mixed = mixed + part[...].astype(F32)
    rows = layer_norm(RESIDUAL_SCALE * stream[...].astype(F32) + mixed, gain[...], bias[...]).astype(BF16)
    normed[...] = rows
    outgoing[...] = dot(select[...], rows).astype(BF16).reshape(outgoing.shape)


def side_kernel(places, decays, states, *rest):
    *far, select, merge, turned_decays, turned_states, stream, gain, bias, projection, ahead = rest[:16]
    ids, weights, gate_rows, wide, products, sums, sems = rest[16:]
    copies = fetched(list(zip(far, (gate_rows, ids, weights, stream, gain, bias, projection))), sems)
    part, mine = places[0], places[1]
    ahead[...] = jnp.where(lax.broadcasted_iota(jnp.int32, ahead.shape, 0) < mine, 1.0, 0.0)
    length, runs = decays.shape[0], decays.shape[1] // LANES
    copies[0].wait()
    wide[...] = gate_rows[...].astype(F32)
    groups = 2
    for run in range(runs):
        g, c = divmod(run, runs // groups)
        values = jax.nn.gelu(wide[pl.ds(c * groups + g, length, stride=runs), :], approximate=True)
        at = slice(run * LANES, (run + 1) * LANES)
        products[:, at] = values * decays[:, at]
        sums[:, at] = values * states[:, at]
    quarter = stream.shape[0]
    count = length // quarter
    for k in range(count):
        source = pl.ds(pl.multiple_of(lax.rem(part + k, count) * quarter, quarter), quarter)
        turned_decays[k * quarter : (k + 1) * quarter] = products[source]
        turned_states[k * quarter : (k + 1) * quarter] = sums[source]
    copies[1].wait()
    copies[2].wait()
    route(ids, weights, select, merge, part)
    for copy in copies[3:]:
        copy.wait()


def pair_moves(pairs, weights):
    moves = []
    for j, (gate_w, up_w) in enumerate(weights):
        width = gate_w.shape[1]
        moves += [(gate_w, pairs.at[j, :, 0:width]), (up_w, pairs.at[j, :, width : 2 * width])]
    return moves


def shared_kernel(normed, gate_w, up_w, down_w, merge, gain, bias, g0, u0, g1, u1, base, *rest):
    *kept, near, sems = rest
    copies = fetched(pair_moves(near, ((g0, u0), (g1, u1))), sems)
    for target, source in zip(kept, (merge, gain, bias)):
        target[...] = source[...]
    rows = normed[...]
    gated, lifted = dot(rows, gate_w[...]), dot(rows, up_w[...])
    hidden = (jax.nn.silu(gated) * lifted).astype(BF16)
    base[...] = RESIDUAL_SCALE * rows.astype(F32) + dot(hidden, down_w[...])
    for copy in copies:
        copy.wait()


def expert_kernel(rows, near, g2, u2, g3, u3, d0, d1, d2, acc, last, far, down, sems):
    moves = pair_moves(far, ((g2, u2), (g3, u3)))
    unit = d0.shape[0]
    moves += [(piece, down.at[j * unit : (j + 1) * unit]) for j, piece in enumerate((d0, d1, d2))]
    copies = fetched(moves, sems)
    picked = rows[...].reshape(-1, rows.shape[-1])

    def hidden_of(both):
        pair = dot(picked, both)
        return (jax.nn.silu(pair[:, :unit]) * pair[:, unit:]).astype(BF16)

    hidden = [hidden_of(near[j]) for j in range(near.shape[0])]
    for j in range(far.shape[0]):
        copies[2 * j].wait()
        copies[2 * j + 1].wait()
        hidden.append(hidden_of(far[j]))
    last[...] = hidden.pop()
    for copy in copies[2 * far.shape[0] :]:
        copy.wait()
    acc[...] = dot(jnp.concatenate(hidden, axis=1), down[...])


def last_kernel(acc, hidden, d3a, d3b, out):
    total = acc[...] + dot(hidden[...], jnp.concatenate([d3a[...], d3b[...]], axis=0))
    out[...] = total.astype(BF16).reshape(out.shape)


def merge_kernel(returned, base, merge, gain, bias, out):
    rest = merge[...]
    rows = returned[...].reshape(-1, returned.shape[-1])
    total = base[...]
    for _ in range(3):
        part = rest.astype(BF16)
        total = total + dot(part, rows)
        rest = rest - part.astype(F32)
    out[...] = layer_norm(total, gain[...], bias[...]).astype(BF16)


def turned(shard, by):
    count = lax.axis_size("tp")
    return lax.ppermute(shard, "tp", [(i, (i + by) % count) for i in range(count)])


def swapped(pieces, axis):
    return lax.all_to_all(pieces, axis, 0, 0, tiled=True)


def shards(
    stream,
    recurrence_input,
    output_gate_input,
    convolution_taps,
    first_group_gates,
    second_group_gates,
    channel_decay,
    position_log_extra,
    recurrence_output_weight,
    first_norm_gain,
    first_norm_bias,
    routed_expert_index,
    routed_expert_weight,
    routed_gate_weight,
    routed_up_weight,
    routed_down_weight,
    shared_gate_weight,
    shared_up_weight,
    shared_down_weight,
    second_norm_gain,
    second_norm_bias,
):
    length, groups, half = recurrence_input.shape
    width = stream.shape[1]
    tp_count, sp_count = lax.axis_size("tp"), lax.axis_size("sp")
    quarter = length // tp_count
    expert_count = routed_gate_weight.shape[0] * sp_count
    slot_count = expert_count * SLOTS
    channels = groups * half
    shape, kept = jax.ShapeDtypeStruct, pltpu.VMEM

    rows = flat(recurrence_input)
    margin = 16
    border = lax.ppermute(rows[rows.shape[0] - margin :], "sp", [(i, i + 1) for i in range(sp_count - 1)])
    operands = (
        rows,
        convolution_taps,
        first_group_gates,
        second_group_gates,
        channel_decay,
        flat(position_log_extra),
    )
    per_half = half // LANES
    prepared = kernel_call(
        load_kernel,
        [
            kept((rows.shape[0], LANES), F32),
            kept((length, channels), F32),
            kept((per_half, LANES, 2 * LANES), BF16),
            kept((per_half, LANES, 2 * LANES), BF16),
            kept((groups, half), F32),
            kept(convolution_taps.shape, F32),
        ],
        *((x, "hbm") for x in operands),
        scratch=(
            *(pltpu.VMEM(x.shape, x.dtype) for x in operands[:5]),
            pltpu.VMEM((margin + rows.shape[0], LANES), F32),
            pltpu.SemaphoreType.DMA((len(operands),)),
        ),
    )

    gate_w, up_w, down_w = routed_gate_weight[0], routed_up_weight[0], routed_down_weight[0]
    gate_left, up_right = turned(gate_w, 1), turned(up_w, -1)
    up_left, gate_right = turned(up_w, 1), turned(gate_w, -1)
    down_left, down_right = turned(down_w, 1), turned(down_w, -1)

    runs = channels // LANES
    decays, states, totals = kernel_call(
        local_kernel,
        [kept((length, channels), F32), kept((length, channels), F32), shape((sp_count, 2 * runs, LANES), BF16)],
        *((x, "vmem") for x in (border, *prepared)),
        scratch=(pltpu.VMEM((margin + 8 * groups * per_half, LANES), F32),),
    )
    spans = swapped(totals, "sp")

    side = (
        flat(output_gate_input),
        routed_expert_index.T,
        routed_expert_weight.T,
        stream,
        first_norm_gain.reshape(1, width),
        first_norm_bias.reshape(1, width),
        recurrence_output_weight,
    )
    select, merge, decays, states, *norm_parts, projection, ahead = kernel_call(
        side_kernel,
        [
            kept((slot_count, quarter), BF16),
            kept((quarter, slot_count), F32),
            kept((length, channels), F32),
            kept((length, channels), F32),
            kept((quarter, width), BF16),
            kept((1, width), F32),
            kept((1, width), F32),
            kept(recurrence_output_weight.shape, BF16),
            kept((sp_count, LANES), F32),
        ],
        (jnp.stack([lax.axis_index("tp"), lax.axis_index("sp")]), "smem"),
        (decays, "vmem"),
        (states, "vmem"),
        *((x, "hbm") for x in side),
        scratch=(
            pltpu.VMEM(routed_expert_index.T.shape, jnp.int32),
            pltpu.VMEM(routed_expert_weight.T.shape, F32),
            pltpu.VMEM(rows.shape, BF16),
            pltpu.VMEM(rows.shape, F32),
            pltpu.VMEM((length, channels), F32),
            pltpu.VMEM((length, channels), F32),
            pltpu.SemaphoreType.DMA((len(side),)),
        ),
    )
    own, *others = kernel_call(
        project_kernel,
        [kept((quarter, width), BF16) for _ in range(tp_count)],
        *((x, "vmem") for x in (spans, ahead, decays, states, projection)),
    )
    parts = {k: turned(others[k - 1], k) for k in (2, 1, 3)}
    parts = [own, *(parts[k] for k in (1, 3, 2))]

    gate_far, up_far = turned(gate_left, 1), turned(up_right, -1)

    normed, outgoing = kernel_call(
        mix_kernel,
        [kept((quarter, width), BF16), shape((expert_count, SLOTS, width), BF16)],
        *((x, "vmem") for x in parts),
        *((x, "vmem") for x in norm_parts),
        (select, "vmem"),
    )
    arrived = swapped(outgoing, "sp")

    cut = down_w.shape[0] // 2
    down_far = turned(down_left[:cut], 1), turned(down_right[cut:], -1)

    last = (merge, second_norm_gain.reshape(1, width), second_norm_bias.reshape(1, width))
    near_weights = (gate_w, up_w, gate_left, up_left)
    unit = gate_w.shape[1]
    base, *last, near = kernel_call(
        shared_kernel,
        [
            kept((quarter, width), F32),
            *(kept(x.shape, F32) for x in last),
            kept((len(near_weights) // 2, width, 2 * unit), BF16),
        ],
        (normed, "vmem"),
        shared_gate_weight,
        shared_up_weight,
        shared_down_weight,
        (last[0], "vmem"),
        *last[1:],
        *((w, "hbm") for w in near_weights),
        scratch=(pltpu.SemaphoreType.DMA((len(near_weights),)),),
    )
    weights = (gate_right, up_right, gate_far, up_far, down_w, down_left, down_right)
    acc, hidden = kernel_call(
        expert_kernel,
        [kept((slot_count, width), F32), kept((slot_count, unit), BF16)],
        (arrived, "vmem"),
        (near, "vmem"),
        *((w, "hbm") for w in weights),
        scratch=(
            pltpu.VMEM((2, width, 2 * unit), BF16),
            pltpu.VMEM((3 * unit, width), BF16),
            pltpu.SemaphoreType.DMA((len(weights),)),
        ),
    )
    leaving = kernel_call(
        last_kernel, kept((expert_count, SLOTS, width), BF16), (acc, "vmem"), (hidden, "vmem"), *down_far
    )
    returned = swapped(leaving, "sp")
    return kernel_call(
        merge_kernel, shape((quarter, width), BF16), (returned, "vmem"), (base, "vmem"), *((x, "vmem") for x in last)
    )


def solution(mesh):
    in_specs = (
        P(("sp", "tp"), None),
        P("sp", None, "tp"),
        P("sp", None, "tp"),
        P(None, None, "tp"),
        P(None, "tp", None, None),
        P(None, "tp", None, None),
        P(None, "tp"),
        P("sp", None, "tp"),
        P(None, "tp", None),
        P(),
        P(),
        P("sp", None),
        P("sp", None),
        P("sp", None, "tp"),
        P("sp", None, "tp"),
        P("sp", "tp", None),
        P(),
        P(),
        P(),
        P(),
        P(),
    )

    return jax.shard_map(shards, mesh=mesh, in_specs=in_specs, out_specs=P(("sp", "tp"), None), check_vma=False)
```

```python
import jax
import jax.numpy as jnp
from jax import lax
from jax.experimental import pallas as pl
from jax.experimental.pallas import tpu as pltpu
from jax.sharding import PartitionSpec as P

RESIDUAL_SCALE = 8.0**0.25
NORM_EPSILON = 1e-05
LANES = 128
SLOTS = 2
BF16, F32 = jnp.bfloat16, jnp.float32
VMEM = pl.BlockSpec(memory_space=pltpu.VMEM)
SMEM = pl.BlockSpec(memory_space=pltpu.SMEM)
ANY = pl.BlockSpec(memory_space=pl.ANY)


def kernel_call(body, out_shape, *operands, scratch=(), limit=16):
    several = isinstance(out_shape, (list, tuple))
    specs, arrays = [], []
    for operand in operands:
        array, place = operand if isinstance(operand, tuple) else (operand, None)
        specs.append({"smem": SMEM, "hbm": ANY}.get(place, VMEM))
        if place != "smem":
            array = pltpu.with_memory_space_constraint(array, pltpu.VMEM if place == "vmem" else pltpu.HBM)
        arrays.append(array)
    return pl.pallas_call(
        body,
        out_shape=out_shape,
        in_specs=specs,
        out_specs=[VMEM] * len(out_shape) if several else VMEM,
        scratch_shapes=scratch,
        compiler_params=pltpu.CompilerParams(vmem_limit_bytes=limit << 20),
    )(*arrays)


def fetched(pairs, sems):
    copies = [pltpu.make_async_copy(source, target, sems.at[k]) for k, (source, target) in enumerate(pairs)]
    for copy in copies:
        copy.start()
    return copies


def dot(a, b):
    return jnp.dot(a, b, preferred_element_type=F32)


def layer_norm(values, gain_vec, bias_vec):
    row_mean = jnp.mean(values, axis=-1, keepdims=True)
    spread = jnp.mean(jnp.square(values - row_mean), axis=-1, keepdims=True)
    return (values - row_mean) * lax.rsqrt(spread + NORM_EPSILON) * gain_vec + bias_vec


def softplus(x):
    u = jnp.exp(-jnp.abs(x))
    s = u / (2.0 + u)
    q = s * s
    series = 1.0 / 17.0
    for k in (15.0, 13.0, 11.0, 9.0, 7.0, 5.0, 3.0, 1.0):
        series = series * q + 1.0 / k
    return jnp.maximum(x, 0.0) + 2.0 * s * series


def expm1(z):
    series = 1.0 + z * (1.0 / 9.0)
    for k in (8.0, 7.0, 6.0, 5.0, 4.0, 3.0, 2.0):
        series = 1.0 + z * (1.0 / k) * series
    return jnp.where(jnp.abs(z) < 0.5, z * series, jnp.exp(z) - 1.0)


def shifted_rows(values, by, row, fill):
    if by < 8:
        return jnp.where(row >= by, pltpu.roll(values, by, 0), fill)
    head = jnp.full((by, values.shape[1]), fill, values.dtype)
    return jnp.concatenate([head, values[: values.shape[0] - by]], axis=0)


def chain_rows(decay, drive):
    row = lax.broadcasted_iota(jnp.int32, decay.shape, 0)
    by = 1
    while by < decay.shape[0]:
        drive = decay * shifted_rows(drive, by, row, 0.0) + drive
        decay = decay * shifted_rows(decay, by, row, 1.0)
        by *= 2
    return decay, drive


def flat(array):
    length, groups, half = array.shape
    return array.reshape(length, groups, half // LANES, LANES).transpose(0, 2, 1, 3).reshape(-1, LANES)


def load_kernel(*refs):
    count = (len(refs) - 2) // 2
    far, near, edge, sems = refs[:count], refs[count : 2 * count], refs[-2], refs[-1]
    copies = fetched(list(zip(far, near)), sems)
    copies[0].wait()
    edge[...] = near[0][near[0].shape[0] - edge.shape[0] :]
    for copy in copies[1:]:
        copy.wait()


def local_kernel(rows, taps, small_maps, large_maps, decay_param, extra, border, decays, states, totals, padded, maps):
    groups, half = decay_param.shape
    per_half = half // LANES
    step = groups * per_half
    length = rows.shape[0] // step
    tap_count = taps.shape[0]
    tap_weights = taps[...].astype(F32)
    rate = -8.0 * softplus(-decay_param[...])
    margin = border.shape[0]
    padded[0:margin] = border[...].astype(F32)
    padded[margin:] = rows[...].astype(F32)
    head = small_maps.shape[-1]
    per_run = LANES // head
    maps[...] = jnp.zeros(maps.shape, BF16)
    for c in range(per_half):
        for m in range(2):
            for h in range(per_run):
                at = h * head
                maps[c, at : at + head, m * LANES + at : m * LANES + at + head] = small_maps[m, c * per_run + h]
    logs, ends = [], []
    for g in range(groups):
        for c in range(per_half):
            at = slice(c * LANES, (c + 1) * LANES)
            summed = None
            for k in range(tap_count):
                start = margin - (tap_count - 1 - k) * step + c * groups + g
                term = tap_weights[k, g : g + 1, at] * padded[pl.ds(start, length, stride=step), :]
                summed = term if summed is None else summed + term
            conv_rows = summed.astype(BF16)
            both = maps[c] if g == 0 else jnp.concatenate([large_maps[0, c], large_maps[1, c]], axis=1)
            gates = jax.nn.sigmoid(dot(conv_rows, both))
            log_decay = gates[:, :LANES] * rate[g : g + 1, at] + extra[pl.ds(c * groups + g, length, stride=step), :]
            drive = jnp.sqrt(-expm1(2.0 * log_decay)) * gates[:, LANES:] * conv_rows.astype(F32)
            product, state = chain_rows(jnp.exp(log_decay), drive)
            to = slice((g * per_half + c) * LANES, (g * per_half + c + 1) * LANES)
            decays[:, to] = product
            states[:, to] = state
            logs.append(jnp.sum(log_decay, axis=0, keepdims=True))
            ends.append(state[length - 1 :])
    span = jnp.concatenate(logs + ends, axis=0).astype(BF16)
    for j in range(totals.shape[0]):
        totals[j] = span


def entering_state(spans, ahead):
    half = spans.shape[1] // 2
    passed = (ahead[...] > 0.0)[:, None, :]
    decays = jnp.where(passed, jnp.exp(spans[:, :half].astype(F32)), 1.0)
    ends = jnp.where(passed, spans[:, half:].astype(F32), 0.0)
    state = ends[0]
    for j in range(1, spans.shape[0] - 1):
        state = decays[j] * state + ends[j]
    return state


def project_kernel(spans, ahead, decays, states, weight, *outs):
    entering = entering_state(spans, ahead)
    runs = entering.shape[0]
    branches = []
    for run in range(runs):
        at = slice(run * LANES, (run + 1) * LANES)
        branches.append((states[:, at] + decays[:, at] * entering[run : run + 1]).astype(BF16))
    acc, per_half = None, runs // weight.shape[0]
    for g in range(weight.shape[0]):
        part = dot(jnp.concatenate(branches[g * per_half : (g + 1) * per_half], axis=1), weight[g])
        acc = part if acc is None else acc + part
    quarter = outs[0].shape[0]
    for k, out in enumerate(outs):
        out[...] = acc[k * quarter : (k + 1) * quarter].astype(BF16)


def route(ids, weights, select, merge, part):
    slot_count, rows = select.shape[0], ids.shape[1]
    kept_rows = select.shape[1]
    turn = (rows - part * kept_rows) % rows
    own = lax.broadcasted_iota(jnp.int32, ids.shape, 1) < kept_rows
    ids = jnp.where(own, pltpu.roll(ids[...], turn, 1), -1)
    weights = pltpu.roll(weights[...], turn, 1)
    slot = lax.broadcasted_iota(jnp.int32, (slot_count, rows), 0)
    names = jnp.zeros((slot_count, rows), F32)
    weight = jnp.zeros((slot_count, rows), F32)
    for k in range(ids.shape[0]):
        named = ids[k : k + 1] == slot // SLOTS
        names = jnp.where(named, 1.0, names)
        weight = jnp.where(named, weights[k : k + 1], weight)
    earlier = lax.broadcasted_iota(jnp.int32, (rows, rows), 0) < lax.broadcasted_iota(jnp.int32, (rows, rows), 1)
    rank = dot(names.astype(BF16), jnp.where(earlier, 1.0, 0.0).astype(BF16))
    taken = (names > 0.0) & (rank == (slot % SLOTS).astype(F32))
    select[...] = jnp.where(taken, 1.0, 0.0).astype(BF16)[:, : select.shape[1]]
    merge[...] = jnp.where(taken, weight, 0.0).T[: merge.shape[0]]


def mix_kernel(*refs):
    *parts, stream, gain, bias, select, normed, outgoing = refs
    mixed = parts[0][...].astype(F32)
    for part in parts[1:]:
        mixed = mixed + part[...].astype(F32)
    rows = layer_norm(RESIDUAL_SCALE * stream[...].astype(F32) + mixed, gain[...], bias[...]).astype(BF16)
    normed[...] = rows
    outgoing[...] = dot(select[...], rows).astype(BF16).reshape(outgoing.shape)


def side_kernel(places, decays, states, *rest):
    *far, select, merge, turned_decays, turned_states, stream, gain, bias, projection, ahead = rest[:16]
    ids, weights, gate_rows, wide, products, sums, sems = rest[16:]
    copies = fetched(list(zip(far, (gate_rows, ids, weights, stream, gain, bias, projection))), sems)
    part, mine = places[0], places[1]
    ahead[...] = jnp.where(lax.broadcasted_iota(jnp.int32, ahead.shape, 0) < mine, 1.0, 0.0)
    length, runs = decays.shape[0], decays.shape[1] // LANES
    copies[0].wait()
    wide[...] = gate_rows[...].astype(F32)
    groups = 2
    for run in range(runs):
        g, c = divmod(run, runs // groups)
        values = jax.nn.gelu(wide[pl.ds(c * groups + g, length, stride=runs), :], approximate=True)
        at = slice(run * LANES, (run + 1) * LANES)
        products[:, at] = values * decays[:, at]
        sums[:, at] = values * states[:, at]
    quarter = stream.shape[0]
    count = length // quarter
    for k in range(count):
        source = pl.ds(pl.multiple_of(lax.rem(part + k, count) * quarter, quarter), quarter)
        turned_decays[k * quarter : (k + 1) * quarter] = products[source]
        turned_states[k * quarter : (k + 1) * quarter] = sums[source]
    copies[1].wait()
    copies[2].wait()
    route(ids, weights, select, merge, part)
    for copy in copies[3:]:
        copy.wait()


def pair_moves(pairs, weights):
    moves = []
    for j, (gate_w, up_w) in enumerate(weights):
        width = gate_w.shape[1]
        moves += [(gate_w, pairs.at[j, :, 0:width]), (up_w, pairs.at[j, :, width : 2 * width])]
    return moves


def shared_kernel(normed, gate_w, up_w, down_w, merge, gain, bias, g0, u0, base, *rest):
    *kept, near, sems = rest
    copies = fetched(pair_moves(near, ((g0, u0),)), sems)
    for target, source in zip(kept, (merge, gain, bias)):
        target[...] = source[...]
    rows = normed[...]
    gated, lifted = dot(rows, gate_w[...]), dot(rows, up_w[...])
    hidden = (jax.nn.silu(gated) * lifted).astype(BF16)
    base[...] = RESIDUAL_SCALE * rows.astype(F32) + dot(hidden, down_w[...])
    for copy in copies:
        copy.wait()


def expert_kernel(rows, near, g1, u1, g2, u2, g3, u3, d0, d1, d2, acc, last, far, down, sems):
    moves = pair_moves(far, ((g1, u1), (g2, u2), (g3, u3)))
    unit = d0.shape[0]
    moves += [(piece, down.at[j * unit : (j + 1) * unit]) for j, piece in enumerate((d0, d1, d2))]
    copies = fetched(moves, sems)
    picked = rows[...].reshape(-1, rows.shape[-1])

    def hidden_of(both):
        pair = dot(picked, both)
        return (jax.nn.silu(pair[:, :unit]) * pair[:, unit:]).astype(BF16)

    hidden = [hidden_of(near[j]) for j in range(near.shape[0])]
    for j in range(far.shape[0]):
        copies[2 * j].wait()
        copies[2 * j + 1].wait()
        hidden.append(hidden_of(far[j]))
    last[...] = hidden.pop()
    for copy in copies[2 * far.shape[0] :]:
        copy.wait()
    acc[...] = dot(jnp.concatenate(hidden, axis=1), down[...])


def last_kernel(acc, hidden, d3a, d3b, out):
    total = acc[...] + dot(hidden[...], jnp.concatenate([d3a[...], d3b[...]], axis=0))
    out[...] = total.astype(BF16).reshape(out.shape)


def merge_kernel(returned, base, merge, gain, bias, out):
    rest = merge[...]
    rows = returned[...].reshape(-1, returned.shape[-1])
    total = base[...]
    for _ in range(3):
        part = rest.astype(BF16)
        total = total + dot(part, rows)
        rest = rest - part.astype(F32)
    out[...] = layer_norm(total, gain[...], bias[...]).astype(BF16)


def turned(shard, by):
    count = lax.axis_size("tp")
    return lax.ppermute(shard, "tp", [(i, (i + by) % count) for i in range(count)])


def swapped(pieces, axis):
    return lax.all_to_all(pieces, axis, 0, 0, tiled=True)


def shards(
    stream,
    recurrence_input,
    output_gate_input,
    convolution_taps,
    first_group_gates,
    second_group_gates,
    channel_decay,
    position_log_extra,
    recurrence_output_weight,
    first_norm_gain,
    first_norm_bias,
    routed_expert_index,
    routed_expert_weight,
    routed_gate_weight,
    routed_up_weight,
    routed_down_weight,
    shared_gate_weight,
    shared_up_weight,
    shared_down_weight,
    second_norm_gain,
    second_norm_bias,
):
    length, groups, half = recurrence_input.shape
    width = stream.shape[1]
    tp_count, sp_count = lax.axis_size("tp"), lax.axis_size("sp")
    quarter = length // tp_count
    expert_count = routed_gate_weight.shape[0] * sp_count
    slot_count = expert_count * SLOTS
    channels = groups * half
    shape, kept = jax.ShapeDtypeStruct, pltpu.VMEM

    rows = flat(recurrence_input)
    margin = 16
    operands = (
        rows,
        convolution_taps,
        first_group_gates,
        second_group_gates,
        channel_decay,
        flat(position_log_extra),
    )
    *operands, edge = kernel_call(
        load_kernel,
        [*(kept(x.shape, x.dtype) for x in operands), kept((margin, LANES), BF16)],
        *((x, "hbm") for x in operands),
        scratch=(pltpu.SemaphoreType.DMA((len(operands),)),),
    )
    border = lax.ppermute(edge, "sp", [(i, i + 1) for i in range(sp_count - 1)])

    gate_w, up_w, down_w = routed_gate_weight[0], routed_up_weight[0], routed_down_weight[0]
    gate_left, up_right = turned(gate_w, 1), turned(up_w, -1)
    up_left, gate_right = turned(up_w, 1), turned(gate_w, -1)
    down_left, down_right = turned(down_w, 1), turned(down_w, -1)

    runs = channels // LANES
    decays, states, totals = kernel_call(
        local_kernel,
        [kept((length, channels), F32), kept((length, channels), F32), shape((sp_count, 2 * runs, LANES), BF16)],
        *((x, "vmem") for x in (*operands, border)),
        scratch=(
            pltpu.VMEM((margin + rows.shape[0], LANES), F32),
            pltpu.VMEM((half // LANES, LANES, 2 * LANES), BF16),
        ),
    )
    spans = swapped(totals, "sp")

    side = (
        flat(output_gate_input),
        routed_expert_index.T,
        routed_expert_weight.T,
        stream,
        first_norm_gain.reshape(1, width),
        first_norm_bias.reshape(1, width),
        recurrence_output_weight,
    )
    select, merge, decays, states, *norm_parts, projection, ahead = kernel_call(
        side_kernel,
        [
            kept((slot_count, quarter), BF16),
            kept((quarter, slot_count), F32),
            kept((length, channels), F32),
            kept((length, channels), F32),
            kept((quarter, width), BF16),
            kept((1, width), F32),
            kept((1, width), F32),
            kept(recurrence_output_weight.shape, BF16),
            kept((sp_count, LANES), F32),
        ],
        (jnp.stack([lax.axis_index("tp"), lax.axis_index("sp")]), "smem"),
        (decays, "vmem"),
        (states, "vmem"),
        *((x, "hbm") for x in side),
        scratch=(
            pltpu.VMEM(routed_expert_index.T.shape, jnp.int32),
            pltpu.VMEM(routed_expert_weight.T.shape, F32),
            pltpu.VMEM(rows.shape, BF16),
            pltpu.VMEM(rows.shape, F32),
            pltpu.VMEM((length, channels), F32),
            pltpu.VMEM((length, channels), F32),
            pltpu.SemaphoreType.DMA((len(side),)),
        ),
    )
    own, *others = kernel_call(
        project_kernel,
        [kept((quarter, width), BF16) for _ in range(tp_count)],
        *((x, "vmem") for x in (spans, ahead, decays, states, projection)),
    )
    parts = {k: turned(others[k - 1], k) for k in (2, 1, 3)}
    parts = [own, *(parts[k] for k in (1, 3, 2))]

    gate_far, up_far = turned(gate_left, 1), turned(up_right, -1)

    normed, outgoing = kernel_call(
        mix_kernel,
        [kept((quarter, width), BF16), shape((expert_count, SLOTS, width), BF16)],
        *((x, "vmem") for x in parts),
        *((x, "vmem") for x in norm_parts),
        (select, "vmem"),
    )
    arrived = swapped(outgoing, "sp")

    cut = down_w.shape[0] // 2
    down_far = turned(down_left[:cut], 1), turned(down_right[cut:], -1)

    last = (merge, second_norm_gain.reshape(1, width), second_norm_bias.reshape(1, width))
    near_weights = (gate_w, up_w)
    unit = gate_w.shape[1]
    base, *last, near = kernel_call(
        shared_kernel,
        [
            kept((quarter, width), F32),
            *(kept(x.shape, F32) for x in last),
            kept((len(near_weights) // 2, width, 2 * unit), BF16),
        ],
        (normed, "vmem"),
        shared_gate_weight,
        shared_up_weight,
        shared_down_weight,
        (last[0], "vmem"),
        *last[1:],
        *((w, "hbm") for w in near_weights),
        scratch=(pltpu.SemaphoreType.DMA((len(near_weights),)),),
    )
    weights = (gate_left, up_left, gate_right, up_right, gate_far, up_far, down_w, down_left, down_right)
    acc, hidden = kernel_call(
        expert_kernel,
        [kept((slot_count, width), F32), kept((slot_count, unit), BF16)],
        (arrived, "vmem"),
        (near, "vmem"),
        *((w, "hbm") for w in weights),
        scratch=(
            pltpu.VMEM((tp_count - 1, width, 2 * unit), BF16),
            pltpu.VMEM((3 * unit, width), BF16),
            pltpu.SemaphoreType.DMA((len(weights),)),
        ),
    )
    leaving = kernel_call(
        last_kernel,
        kept((expert_count, SLOTS, width), BF16),
        (acc, "vmem"),
        (hidden, "vmem"),
        *((w, "vmem") for w in down_far),
    )
    returned = swapped(leaving, "sp")
    return kernel_call(
        merge_kernel, shape((quarter, width), BF16), (returned, "vmem"), (base, "vmem"), *((x, "vmem") for x in last)
    )


def solution(mesh):
    in_specs = (
        P(("sp", "tp"), None),
        P("sp", None, "tp"),
        P("sp", None, "tp"),
        P(None, None, "tp"),
        P(None, "tp", None, None),
        P(None, "tp", None, None),
        P(None, "tp"),
        P("sp", None, "tp"),
        P(None, "tp", None),
        P(),
        P(),
        P("sp", None),
        P("sp", None),
        P("sp", None, "tp"),
        P("sp", None, "tp"),
        P("sp", "tp", None),
        P(),
        P(),
        P(),
        P(),
        P(),
    )

    return jax.shard_map(shards, mesh=mesh, in_specs=in_specs, out_specs=P(("sp", "tp"), None), check_vma=False)
```

```python
import jax
import jax.numpy as jnp
from jax import lax
from jax.experimental import pallas as pl
from jax.experimental.pallas import tpu as pltpu
from jax.sharding import PartitionSpec as P

RESIDUAL_SCALE = 8.0**0.25
NORM_EPSILON = 1e-05
LANES = 128
SLOTS = 2
BF16, F32 = jnp.bfloat16, jnp.float32
VMEM = pl.BlockSpec(memory_space=pltpu.VMEM)
SMEM = pl.BlockSpec(memory_space=pltpu.SMEM)
ANY = pl.BlockSpec(memory_space=pl.ANY)


def kernel_call(body, out_shape, *operands, scratch=(), limit=16):
    several = isinstance(out_shape, (list, tuple))
    specs, arrays = [], []
    for operand in operands:
        array, place = operand if isinstance(operand, tuple) else (operand, None)
        specs.append({"smem": SMEM, "hbm": ANY}.get(place, VMEM))
        if place != "smem":
            array = pltpu.with_memory_space_constraint(array, pltpu.VMEM if place == "vmem" else pltpu.HBM)
        arrays.append(array)
    return pl.pallas_call(
        body,
        out_shape=out_shape,
        in_specs=specs,
        out_specs=[VMEM] * len(out_shape) if several else VMEM,
        scratch_shapes=scratch,
        compiler_params=pltpu.CompilerParams(vmem_limit_bytes=limit << 20),
    )(*arrays)


def fetched(pairs, sems):
    copies = [pltpu.make_async_copy(source, target, sems.at[k]) for k, (source, target) in enumerate(pairs)]
    for copy in copies:
        copy.start()
    return copies


def dot(a, b):
    return jnp.dot(a, b, preferred_element_type=F32)


def layer_norm(values, gain_vec, bias_vec):
    row_mean = jnp.mean(values, axis=-1, keepdims=True)
    spread = jnp.mean(jnp.square(values - row_mean), axis=-1, keepdims=True)
    return (values - row_mean) * lax.rsqrt(spread + NORM_EPSILON) * gain_vec + bias_vec


def softplus(x):
    u = jnp.exp(-jnp.abs(x))
    s = u / (2.0 + u)
    q = s * s
    series = 1.0 / 17.0
    for k in (15.0, 13.0, 11.0, 9.0, 7.0, 5.0, 3.0, 1.0):
        series = series * q + 1.0 / k
    return jnp.maximum(x, 0.0) + 2.0 * s * series


def expm1(z):
    series = 1.0 + z * (1.0 / 9.0)
    for k in (8.0, 7.0, 6.0, 5.0, 4.0, 3.0, 2.0):
        series = 1.0 + z * (1.0 / k) * series
    return jnp.where(jnp.abs(z) < 0.5, z * series, jnp.exp(z) - 1.0)


def shifted_rows(values, by, row, fill):
    if by < 8:
        return jnp.where(row >= by, pltpu.roll(values, by, 0), fill)
    head = jnp.full((by, values.shape[1]), fill, values.dtype)
    return jnp.concatenate([head, values[: values.shape[0] - by]], axis=0)


def chain_rows(decay, drive):
    row = lax.broadcasted_iota(jnp.int32, decay.shape, 0)
    by = 1
    while by < decay.shape[0]:
        drive = decay * shifted_rows(drive, by, row, 0.0) + drive
        decay = decay * shifted_rows(decay, by, row, 1.0)
        by *= 2
    return decay, drive


def flat(array):
    length, groups, half = array.shape
    return array.reshape(length, groups, half // LANES, LANES).transpose(0, 2, 1, 3).reshape(-1, LANES)


def load_kernel(*refs):
    count = (len(refs) - 2) // 2
    far, near, edge, sems = refs[:count], refs[count : 2 * count], refs[-2], refs[-1]
    copies = fetched(list(zip(far, near)), sems)
    copies[0].wait()
    edge[...] = near[0][near[0].shape[0] - edge.shape[0] :]
    for copy in copies[1:]:
        copy.wait()


def local_kernel(rows, taps, small_maps, large_maps, decay_param, extra, border, decays, states, totals, padded, maps):
    groups, half = decay_param.shape
    per_half = half // LANES
    step = groups * per_half
    length = rows.shape[0] // step
    tap_count = taps.shape[0]
    tap_weights = taps[...].astype(F32)
    rate = -8.0 * softplus(-decay_param[...])
    margin = border.shape[0]
    padded[0:margin] = border[...].astype(F32)
    padded[margin:] = rows[...].astype(F32)
    head = small_maps.shape[-1]
    per_run = LANES // head
    maps[...] = jnp.zeros(maps.shape, BF16)
    for c in range(per_half):
        for m in range(2):
            for h in range(per_run):
                at = h * head
                maps[c, at : at + head, m * LANES + at : m * LANES + at + head] = small_maps[m, c * per_run + h]
    logs, ends = [], []
    for g in range(groups):
        for c in range(per_half):
            at = slice(c * LANES, (c + 1) * LANES)
            summed = None
            for k in range(tap_count):
                start = margin - (tap_count - 1 - k) * step + c * groups + g
                term = tap_weights[k, g : g + 1, at] * padded[pl.ds(start, length, stride=step), :]
                summed = term if summed is None else summed + term
            conv_rows = summed.astype(BF16)
            both = maps[c] if g == 0 else jnp.concatenate([large_maps[0, c], large_maps[1, c]], axis=1)
            gates = jax.nn.sigmoid(dot(conv_rows, both))
            log_decay = gates[:, :LANES] * rate[g : g + 1, at] + extra[pl.ds(c * groups + g, length, stride=step), :]
            drive = jnp.sqrt(-expm1(2.0 * log_decay)) * gates[:, LANES:] * conv_rows.astype(F32)
            product, state = chain_rows(jnp.exp(log_decay), drive)
            to = slice((g * per_half + c) * LANES, (g * per_half + c + 1) * LANES)
            decays[:, to] = product
            states[:, to] = state
            logs.append(jnp.sum(log_decay, axis=0, keepdims=True))
            ends.append(state[length - 1 :])
    span = jnp.concatenate(logs + ends, axis=0).astype(BF16)
    for j in range(totals.shape[0]):
        totals[j] = span


def entering_state(spans, ahead):
    half = spans.shape[1] // 2
    passed = (ahead[...] > 0.0)[:, None, :]
    decays = jnp.where(passed, jnp.exp(spans[:, :half].astype(F32)), 1.0)
    ends = jnp.where(passed, spans[:, half:].astype(F32), 0.0)
    state = ends[0]
    for j in range(1, spans.shape[0] - 1):
        state = decays[j] * state + ends[j]
    return state


def project_kernel(spans, ahead, decays, states, weight, *outs):
    entering = entering_state(spans, ahead)
    runs = entering.shape[0]
    branches = []
    for run in range(runs):
        at = slice(run * LANES, (run + 1) * LANES)
        branches.append((states[:, at] + decays[:, at] * entering[run : run + 1]).astype(BF16))
    acc, per_half = None, runs // weight.shape[0]
    for g in range(weight.shape[0]):
        part = dot(jnp.concatenate(branches[g * per_half : (g + 1) * per_half], axis=1), weight[g])
        acc = part if acc is None else acc + part
    quarter = outs[0].shape[0]
    for k, out in enumerate(outs):
        out[...] = acc[k * quarter : (k + 1) * quarter].astype(BF16)


def route(ids, weights, select, merge, part):
    slot_count, rows = select.shape[0], ids.shape[1]
    kept_rows = select.shape[1]
    turn = (rows - part * kept_rows) % rows
    own = lax.broadcasted_iota(jnp.int32, ids.shape, 1) < kept_rows
    ids = jnp.where(own, pltpu.roll(ids[...], turn, 1), -1)
    weights = pltpu.roll(weights[...], turn, 1)
    slot = lax.broadcasted_iota(jnp.int32, (slot_count, rows), 0)
    names = jnp.zeros((slot_count, rows), F32)
    weight = jnp.zeros((slot_count, rows), F32)
    for k in range(ids.shape[0]):
        named = ids[k : k + 1] == slot // SLOTS
        names = jnp.where(named, 1.0, names)
        weight = jnp.where(named, weights[k : k + 1], weight)
    earlier = lax.broadcasted_iota(jnp.int32, (rows, rows), 0) < lax.broadcasted_iota(jnp.int32, (rows, rows), 1)
    rank = dot(names.astype(BF16), jnp.where(earlier, 1.0, 0.0).astype(BF16))
    taken = (names > 0.0) & (rank == (slot % SLOTS).astype(F32))
    select[...] = jnp.where(taken, 1.0, 0.0).astype(BF16)[:, : select.shape[1]]
    merge[...] = jnp.where(taken, weight, 0.0).T[: merge.shape[0]]


def mix_kernel(*refs):
    *parts, stream, gain, bias, select, normed, outgoing = refs
    mixed = parts[0][...].astype(F32)
    for part in parts[1:]:
        mixed = mixed + part[...].astype(F32)
    rows = layer_norm(RESIDUAL_SCALE * stream[...].astype(F32) + mixed, gain[...], bias[...]).astype(BF16)
    normed[...] = rows
    outgoing[...] = dot(select[...], rows).astype(BF16).reshape(outgoing.shape)


def side_kernel(places, decays, states, *rest):
    *far, select, merge, turned_decays, turned_states, stream, gain, bias, projection, ahead = rest[:16]
    ids, weights, gate_rows, wide, products, sums, sems = rest[16:]
    copies = fetched(list(zip(far, (gate_rows, ids, weights, stream, gain, bias, projection))), sems)
    part, mine = places[0], places[1]
    ahead[...] = jnp.where(lax.broadcasted_iota(jnp.int32, ahead.shape, 0) < mine, 1.0, 0.0)
    length, runs = decays.shape[0], decays.shape[1] // LANES
    copies[0].wait()
    wide[...] = gate_rows[...].astype(F32)
    groups = 2
    for run in range(runs):
        g, c = divmod(run, runs // groups)
        values = jax.nn.gelu(wide[pl.ds(c * groups + g, length, stride=runs), :], approximate=True)
        at = slice(run * LANES, (run + 1) * LANES)
        products[:, at] = values * decays[:, at]
        sums[:, at] = values * states[:, at]
    quarter = stream.shape[0]
    count = length // quarter
    for k in range(count):
        source = pl.ds(pl.multiple_of(lax.rem(part + k, count) * quarter, quarter), quarter)
        turned_decays[k * quarter : (k + 1) * quarter] = products[source]
        turned_states[k * quarter : (k + 1) * quarter] = sums[source]
    copies[1].wait()
    copies[2].wait()
    route(ids, weights, select, merge, part)
    for copy in copies[3:]:
        copy.wait()


def pair_moves(pairs, weights):
    moves = []
    for j, (gate_w, up_w) in enumerate(weights):
        width = gate_w.shape[1]
        moves += [(gate_w, pairs.at[j, :, 0:width]), (up_w, pairs.at[j, :, width : 2 * width])]
    return moves


def shared_kernel(normed, gate_w, up_w, down_w, merge, gain, bias, g0, u0, d0, base, *rest):
    *kept, near, near_down, sems = rest
    copies = fetched(pair_moves(near, ((g0, u0),)) + [(d0, near_down)], sems)
    for target, source in zip(kept, (merge, gain, bias)):
        target[...] = source[...]
    rows = normed[...]
    gated, lifted = dot(rows, gate_w[...]), dot(rows, up_w[...])
    hidden = (jax.nn.silu(gated) * lifted).astype(BF16)
    base[...] = RESIDUAL_SCALE * rows.astype(F32) + dot(hidden, down_w[...])
    for copy in copies:
        copy.wait()


def expert_kernel(rows, near, near_down, g1, u1, g2, u2, g3, u3, d1, d2, acc, last, far, down, sems):
    moves = pair_moves(far, ((g1, u1), (g2, u2), (g3, u3)))
    unit = d2.shape[0]
    moves += [(piece, down.at[j * unit : (j + 1) * unit]) for j, piece in enumerate((d1, d2))]
    copies = fetched(moves, sems)
    picked = rows[...].reshape(-1, rows.shape[-1])

    def hidden_of(both):
        pair = dot(picked, both)
        return (jax.nn.silu(pair[:, :unit]) * pair[:, unit:]).astype(BF16)

    hidden = [hidden_of(near[j]) for j in range(near.shape[0])]
    for j in range(far.shape[0]):
        copies[2 * j].wait()
        copies[2 * j + 1].wait()
        hidden.append(hidden_of(far[j]))
    last[...] = hidden.pop()
    for copy in copies[2 * far.shape[0] :]:
        copy.wait()
    acc[...] = dot(hidden[0], near_down[...]) + dot(jnp.concatenate(hidden[1:], axis=1), down[...])


def last_kernel(acc, hidden, d3a, d3b, out):
    total = acc[...] + dot(hidden[...], jnp.concatenate([d3a[...], d3b[...]], axis=0))
    out[...] = total.astype(BF16).reshape(out.shape)


def merge_kernel(returned, base, merge, gain, bias, out):
    rest = merge[...]
    rows = returned[...].reshape(-1, returned.shape[-1])
    total = base[...]
    for _ in range(3):
        part = rest.astype(BF16)
        total = total + dot(part, rows)
        rest = rest - part.astype(F32)
    out[...] = layer_norm(total, gain[...], bias[...]).astype(BF16)


def turned(shard, by):
    count = lax.axis_size("tp")
    return lax.ppermute(shard, "tp", [(i, (i + by) % count) for i in range(count)])


def swapped(pieces, axis):
    return lax.all_to_all(pieces, axis, 0, 0, tiled=True)


def shards(
    stream,
    recurrence_input,
    output_gate_input,
    convolution_taps,
    first_group_gates,
    second_group_gates,
    channel_decay,
    position_log_extra,
    recurrence_output_weight,
    first_norm_gain,
    first_norm_bias,
    routed_expert_index,
    routed_expert_weight,
    routed_gate_weight,
    routed_up_weight,
    routed_down_weight,
    shared_gate_weight,
    shared_up_weight,
    shared_down_weight,
    second_norm_gain,
    second_norm_bias,
):
    length, groups, half = recurrence_input.shape
    width = stream.shape[1]
    tp_count, sp_count = lax.axis_size("tp"), lax.axis_size("sp")
    quarter = length // tp_count
    expert_count = routed_gate_weight.shape[0] * sp_count
    slot_count = expert_count * SLOTS
    channels = groups * half
    shape, kept = jax.ShapeDtypeStruct, pltpu.VMEM

    rows = flat(recurrence_input)
    margin = 16
    operands = (
        rows,
        convolution_taps,
        first_group_gates,
        second_group_gates,
        channel_decay,
        flat(position_log_extra),
    )
    *operands, edge = kernel_call(
        load_kernel,
        [*(kept(x.shape, x.dtype) for x in operands), kept((margin, LANES), BF16)],
        *((x, "hbm") for x in operands),
        scratch=(pltpu.SemaphoreType.DMA((len(operands),)),),
    )
    border = lax.ppermute(edge, "sp", [(i, i + 1) for i in range(sp_count - 1)])

    gate_w, up_w, down_w = routed_gate_weight[0], routed_up_weight[0], routed_down_weight[0]
    gate_left, up_right = turned(gate_w, 1), turned(up_w, -1)
    up_left, gate_right = turned(up_w, 1), turned(gate_w, -1)
    down_left, down_right = turned(down_w, 1), turned(down_w, -1)

    runs = channels // LANES
    decays, states, totals = kernel_call(
        local_kernel,
        [kept((length, channels), F32), kept((length, channels), F32), shape((sp_count, 2 * runs, LANES), BF16)],
        *((x, "vmem") for x in (*operands, border)),
        scratch=(
            pltpu.VMEM((margin + rows.shape[0], LANES), F32),
            pltpu.VMEM((half // LANES, LANES, 2 * LANES), BF16),
        ),
    )
    spans = swapped(totals, "sp")

    side = (
        flat(output_gate_input),
        routed_expert_index.T,
        routed_expert_weight.T,
        stream,
        first_norm_gain.reshape(1, width),
        first_norm_bias.reshape(1, width),
        recurrence_output_weight,
    )
    select, merge, decays, states, *norm_parts, projection, ahead = kernel_call(
        side_kernel,
        [
            kept((slot_count, quarter), BF16),
            kept((quarter, slot_count), F32),
            kept((length, channels), F32),
            kept((length, channels), F32),
            kept((quarter, width), BF16),
            kept((1, width), F32),
            kept((1, width), F32),
            kept(recurrence_output_weight.shape, BF16),
            kept((sp_count, LANES), F32),
        ],
        (jnp.stack([lax.axis_index("tp"), lax.axis_index("sp")]), "smem"),
        (decays, "vmem"),
        (states, "vmem"),
        *((x, "hbm") for x in side),
        scratch=(
            pltpu.VMEM(routed_expert_index.T.shape, jnp.int32),
            pltpu.VMEM(routed_expert_weight.T.shape, F32),
            pltpu.VMEM(rows.shape, BF16),
            pltpu.VMEM(rows.shape, F32),
            pltpu.VMEM((length, channels), F32),
            pltpu.VMEM((length, channels), F32),
            pltpu.SemaphoreType.DMA((len(side),)),
        ),
    )
    own, *others = kernel_call(
        project_kernel,
        [kept((quarter, width), BF16) for _ in range(tp_count)],
        *((x, "vmem") for x in (spans, ahead, decays, states, projection)),
    )
    parts = {k: turned(others[k - 1], k) for k in (2, 1, 3)}
    parts = [own, *(parts[k] for k in (1, 3, 2))]

    gate_far, up_far = turned(gate_left, 1), turned(up_right, -1)

    normed, outgoing = kernel_call(
        mix_kernel,
        [kept((quarter, width), BF16), shape((expert_count, SLOTS, width), BF16)],
        *((x, "vmem") for x in parts),
        *((x, "vmem") for x in norm_parts),
        (select, "vmem"),
    )
    arrived = swapped(outgoing, "sp")

    cut = down_w.shape[0] // 2
    down_far = turned(down_left[:cut], 1), turned(down_right[cut:], -1)

    last = (merge, second_norm_gain.reshape(1, width), second_norm_bias.reshape(1, width))
    near_weights = (gate_w, up_w, down_w)
    unit = gate_w.shape[1]
    base, *last, near, near_down = kernel_call(
        shared_kernel,
        [
            kept((quarter, width), F32),
            *(kept(x.shape, F32) for x in last),
            kept((1, width, 2 * unit), BF16),
            kept((unit, width), BF16),
        ],
        (normed, "vmem"),
        shared_gate_weight,
        shared_up_weight,
        shared_down_weight,
        (last[0], "vmem"),
        *last[1:],
        *((w, "hbm") for w in near_weights),
        scratch=(pltpu.SemaphoreType.DMA((len(near_weights),)),),
    )
    weights = (gate_left, up_left, gate_right, up_right, gate_far, up_far, down_left, down_right)
    acc, hidden = kernel_call(
        expert_kernel,
        [kept((slot_count, width), F32), kept((slot_count, unit), BF16)],
        (arrived, "vmem"),
        (near, "vmem"),
        (near_down, "vmem"),
        *((w, "hbm") for w in weights),
        scratch=(
            pltpu.VMEM((tp_count - 1, width, 2 * unit), BF16),
            pltpu.VMEM((2 * unit, width), BF16),
            pltpu.SemaphoreType.DMA((len(weights),)),
        ),
    )
    leaving = kernel_call(
        last_kernel,
        kept((expert_count, SLOTS, width), BF16),
        (acc, "vmem"),
        (hidden, "vmem"),
        *((w, "vmem") for w in down_far),
    )
    returned = swapped(leaving, "sp")
    return kernel_call(
        merge_kernel, shape((quarter, width), BF16), (returned, "vmem"), (base, "vmem"), *((x, "vmem") for x in last)
    )


def solution(mesh):
    in_specs = (
        P(("sp", "tp"), None),
        P("sp", None, "tp"),
        P("sp", None, "tp"),
        P(None, None, "tp"),
        P(None, "tp", None, None),
        P(None, "tp", None, None),
        P(None, "tp"),
        P("sp", None, "tp"),
        P(None, "tp", None),
        P(),
        P(),
        P("sp", None),
        P("sp", None),
        P("sp", None, "tp"),
        P("sp", None, "tp"),
        P("sp", "tp", None),
        P(),
        P(),
        P(),
        P(),
        P(),
    )

    return jax.shard_map(shards, mesh=mesh, in_specs=in_specs, out_specs=P(("sp", "tp"), None), check_vma=False)
```
